32 devices in a mesh: ep: 8 (over z, x), tp: 4 (over y, core).
Axes of the slice: x: 2, y: 2, z: 4, core: 2. Of those that a mesh axis runs over, the one named last changes fastest.
Arguments:
- conv_value: bfloat16 [8192, 1024], P('ep', 'tp'), may hold values from -600 to 600
- conv_gate: bfloat16 [8192, 1024], P('ep', 'tp'), may hold values from -8 to 8
- depth_weight: float32 [31, 1024], replicated, may hold values from -1 to 1
- norm_gain: float32 [1024], replicated, may hold values from 0.1 to 1.9
- norm_shift: float32 [1024], replicated, may hold values from -3 to 3
- conv_out_weight: bfloat16 [1024, 2048], P('tp'), may hold values from -0.1875 to 0.1875
- moe_input: bfloat16 [12288, 2048], P(('ep', 'tp')), may hold values from -6 to 6
- moe_gain: float32 [2048], replicated, may hold values from 0.1 to 1.9
- route_experts: int32 [12288, 2], P(('ep', 'tp')), may hold values from 0 to 7, as said below
- route_scores: float32 [12288, 2], P(('ep', 'tp')), may hold values from -8 to 8
- expert_gate: bfloat16 [8, 2048, 512], P('ep'), may hold values from -0.125 to 0.125
- expert_up: bfloat16 [8, 2048, 512], P('ep'), may hold values from -0.125 to 0.125
- expert_down: bfloat16 [8, 512, 2048], P('ep'), may hold values from -1 to 1
Outputs:
- conv_out: bfloat16 [8192, 2048], P(('ep', 'tp'))
- moe_out: bfloat16 [12288, 2048], P(('ep', 'tp'))
The draws below stay inside these ranges and needn't reach their ends.
Inputs may be any that keep to these rules, and one draw needn't show every extreme that they name: `route_experts`: each row names two different experts that lie in one group of 2 consecutive experts.
All inputs are finite; a program needn't handle non-finite values.
Results may differ from the reference program's by a relative error of at most 0.009.
Values may be sent and summed in bfloat16 or wider, within the bound.
A program may use at most 128 MiB of HBM per device.

```python
import jax
import jax.numpy as jnp
from jax import lax

D = 2048
CONV = 1024
FF = 512
KERNEL = 31
GROUPS = 4
TOP = 2
TOK_B = 384
EXPERTS = 8
GROUP_EXP = 2
CAP = 144
TOKENS_A = 8192
TOKENS_B = 12288
N_EP = 8
N_TP = 4


def draw_conv_value(key, part):
    keys = jax.random.split(jax.random.fold_in(key, 31), 2)
    column_scale = 10.0 ** (jnp.arange(CONV, dtype=jnp.float32) / CONV)
    base = jnp.clip(jax.random.normal(keys[0], (TOKENS_A, CONV), jnp.float32), -4.0, 4.0)
    row_scale = 10.0 ** jax.random.uniform(keys[1], (TOKENS_A, 1), jnp.float32)
    return (base * row_scale * column_scale[None, :]).astype(jnp.bfloat16)


def group_order(key):
    return jax.random.permutation(key, GROUP_EXP)


def draw_route_experts(key, part):
    keys = jax.random.split(jax.random.fold_in(key, 17), 7)
    order_groups = jax.random.permutation(keys[0], GROUPS)
    group_pick = jnp.minimum(jax.random.randint(keys[1], (TOKENS_B,), 0, GROUPS), jax.random.randint(keys[2], (TOKENS_B,), 0, GROUPS))
    group_id = order_groups[group_pick]
    orders = jax.vmap(group_order)(jax.random.split(keys[3], GROUPS))
    first_pick = jnp.minimum(jax.random.randint(keys[4], (TOKENS_B,), 0, GROUP_EXP), jax.random.randint(keys[5], (TOKENS_B,), 0, GROUP_EXP))
    second_pick = (first_pick + 1 + jax.random.randint(keys[6], (TOKENS_B,), 0, GROUP_EXP - 1)) % GROUP_EXP
    first = group_id * GROUP_EXP + orders[group_id, first_pick]
    second = group_id * GROUP_EXP + orders[group_id, second_pick]
    return jnp.stack([first, second], axis=1).astype(jnp.int32)


def shard_levels(rng, dims, shards, smallest, top_value):
    def one(position, shards_of):
        steps = jax.random.uniform(jax.random.fold_in(jax.random.fold_in(rng, 6), position), (shards_of,), jnp.float32, smallest / len(shards), top_value / len(shards))
        return jnp.repeat(jnp.exp(steps), dims[position] // shards_of).reshape((-1,) + (1,) * (len(dims) - position - 1))

    gain = one(*shards[0])
    for cut in shards[1:]:
        gain = gain * one(*cut)
    return gain


def normal_values(key, dims, deviation, reach, cuts=(), kind=jnp.bfloat16):
    result = jax.random.normal(key, dims, jnp.float32) * deviation
    if len(cuts) > 0:
        result = shard_levels(key, dims, cuts, -0.22, 0.18) * result
    return jnp.clip(result, min=-reach, max=reach).astype(kind)


def setup_inputs(seed: int = 0) -> dict:
    arg_keys = jax.random.split(jax.random.key(seed), 14)
    conv_value = draw_conv_value(jax.random.fold_in(arg_keys[13], 71), 0)
    conv_gate = normal_values(arg_keys[1], (TOKENS_A, CONV), 1.5, 8.0, ((0, 8), (1, 4)))
    depth_weight = normal_values(arg_keys[2], (KERNEL, CONV), KERNEL ** -0.5, 1.0, (), jnp.float32)
    norm_gain = jnp.clip(1.0 + 0.18 * jax.random.normal(arg_keys[3], (CONV,), jnp.float32), 0.1, 1.9)
    norm_shift = normal_values(arg_keys[4], (CONV,), 0.5, 3.0, (), jnp.float32)
    conv_out_weight = normal_values(arg_keys[5], (CONV, D), CONV ** -0.5, 0.1875, ((0, 4),))
    moe_input = normal_values(arg_keys[6], (TOKENS_B, D), 1.0, 6.0, ((0, 32),))
    moe_gain = jnp.clip(1.0 + 0.18 * jax.random.normal(arg_keys[7], (D,), jnp.float32), 0.1, 1.9)
    route_experts = draw_route_experts(jax.random.fold_in(arg_keys[13], 71), 0)
    route_scores = normal_values(arg_keys[9], (TOKENS_B, TOP), 1.5, 8.0, ((0, 32),), jnp.float32)
    expert_gate = normal_values(arg_keys[10], (EXPERTS, D, FF), D ** -0.5, 0.125, ((0, 8),))
    expert_up = normal_values(arg_keys[11], (EXPERTS, D, FF), D ** -0.5, 0.125, ((0, 8),))
    expert_down = normal_values(arg_keys[12], (EXPERTS, FF, D), (FF // 16) ** -0.5, 1.0, ((0, 8),))
    return dict(conv_value=conv_value, conv_gate=conv_gate, depth_weight=depth_weight, norm_gain=norm_gain, norm_shift=norm_shift, conv_out_weight=conv_out_weight, moe_input=moe_input, moe_gain=moe_gain, route_experts=route_experts, route_scores=route_scores, expert_gate=expert_gate, expert_up=expert_up, expert_down=expert_down)


def conv_part(conv_value, conv_gate, depth_weight, norm_gain, norm_shift, conv_out_weight):
    gated = (conv_value.astype(jnp.float32) * jax.nn.sigmoid(conv_gate.astype(jnp.float32))).astype(jnp.bfloat16)
    padded = jnp.concatenate([jnp.zeros((KERNEL - 1, CONV), jnp.bfloat16), gated], 0).astype(jnp.float32)
    filtered = jnp.zeros((TOKENS_A, CONV), jnp.float32)
    for offset in range(KERNEL):
        filtered = filtered + depth_weight[offset] * padded[offset:offset + TOKENS_A]
    center = lax.optimization_barrier(jnp.mean(filtered, axis=-1, keepdims=True))
    spread = lax.optimization_barrier(jnp.mean(filtered * filtered, axis=-1, keepdims=True)) - center * center
    normed = (filtered - center) * lax.rsqrt(spread + 1e-05) * norm_gain + norm_shift
    activated = jax.nn.silu(normed).astype(jnp.bfloat16)
    block_width = CONV // N_TP
    summed = jnp.zeros((TOKENS_A, D), jnp.float32)
    for column_block in range(N_TP):
        low = column_block * block_width
        partial_value = jnp.dot(activated[:, low:low + block_width], conv_out_weight[low:low + block_width], preferred_element_type=jnp.float32).astype(jnp.bfloat16)
        summed = summed + partial_value.astype(jnp.float32)
    return summed.astype(jnp.bfloat16)

def moe_part(moe_input, moe_gain, route_experts, route_scores, expert_gate, expert_up, expert_down):
    widened = moe_input.astype(jnp.float32)
    normal_in = (widened * lax.rsqrt(lax.optimization_barrier(jnp.mean(widened * widened, axis=-1, keepdims=True)) + 1e-06) * moe_gain).astype(jnp.bfloat16)
    sources = N_EP * N_TP
    chosen = route_experts.reshape(sources, TOK_B * TOP)
    onehot = (chosen[:, :, None] == jnp.arange(EXPERTS, dtype=jnp.int32)[None, None, :]).astype(jnp.int32)
    slot_rank = lax.optimization_barrier(jnp.sum(jnp.cumsum(onehot, axis=1) * onehot, axis=-1)) - 1
    within_cap = slot_rank < CAP
    source_ids = jnp.arange(sources, dtype=jnp.int32)[:, None]
    token_index = source_ids * TOK_B + jnp.arange(TOK_B * TOP, dtype=jnp.int32)[None, :] // TOP
    per_expert = sources * CAP
    slot_index = jnp.where(within_cap, chosen * per_expert + source_ids * CAP + slot_rank, EXPERTS * per_expert).astype(jnp.int32)
    slot_token = jnp.full((EXPERTS * per_expert,), TOKENS_B, jnp.int32).at[slot_index.reshape(-1)].set(token_index.reshape(-1), mode='drop')
    group_gate = jax.nn.sigmoid(route_scores[:, 0])
    weights = jnp.stack([group_gate * jax.nn.sigmoid(route_scores[:, 1]), group_gate * jax.nn.sigmoid(-route_scores[:, 1])], axis=-1)
    slot_weight = jnp.zeros((EXPERTS * per_expert,), jnp.float32).at[slot_index.reshape(-1)].set(weights.reshape(-1), mode='drop')
    padded_in = jnp.concatenate([normal_in, jnp.zeros((1, D), jnp.bfloat16)], 0)

    def apply_expert(summed, inputs):
        gate_matrix, up_matrix, down_matrix, tokens_here, weight_here = inputs
        picked_rows = padded_in[tokens_here]
        gate_act = jnp.dot(picked_rows, gate_matrix, preferred_element_type=jnp.float32)
        up_act = jnp.dot(picked_rows, up_matrix, preferred_element_type=jnp.float32)
        inner = (jax.nn.silu(gate_act) * up_act).astype(jnp.bfloat16)
        expert_rows = jnp.dot(inner, down_matrix, preferred_element_type=jnp.float32).astype(jnp.bfloat16)
        summed = summed.at[tokens_here].add(weight_here[:, None] * expert_rows.astype(jnp.float32), mode='drop')
        return (summed, None)
    summed, _ = lax.scan(apply_expert, jnp.zeros((TOKENS_B, D), jnp.float32), (expert_gate, expert_up, expert_down, slot_token.reshape(EXPERTS, per_expert), slot_weight.reshape(EXPERTS, per_expert)))
    return summed.astype(jnp.bfloat16)

def reference(conv_value, conv_gate, depth_weight, norm_gain, norm_shift, conv_out_weight, moe_input, moe_gain, route_experts, route_scores, expert_gate, expert_up, expert_down):
    conv_out = conv_part(conv_value, conv_gate, depth_weight, norm_gain, norm_shift, conv_out_weight)
    moe_out = moe_part(moe_input, moe_gain, route_experts, route_scores, expert_gate, expert_up, expert_down)
    return (conv_out, moe_out)
```

```python
import functools

import jax
import jax.numpy as jnp
from jax import lax
from jax.experimental import pallas as pl
from jax.experimental.pallas import tpu as pltpu
from jax.sharding import PartitionSpec as P

GROUPS = 4
TOP = 2
LANES = 128
HALO = 32
MESH = pl.DeviceIdType.MESH
F32 = jnp.float32
BF16 = jnp.bfloat16


def passed_along(x, axis, by):
    peers = lax.axis_size(axis)
    pairs = [(i, i + by) for i in range(peers) if 0 <= i + by < peers]
    return lax.ppermute(x, axis, pairs)


def gated_rows(value, gate):
    return (value.astype(jnp.float32) * jax.nn.sigmoid(gate.astype(jnp.float32))).astype(
        jnp.bfloat16
    )


def conv_half(conv_value, conv_gate, earlier, depth_weight, norm_gain, norm_shift, conv_out_weight):
    channels = conv_value.shape[1]
    length = conv_value.shape[0]
    first_col = lax.axis_index("tp") * channels
    taps = lax.dynamic_slice_in_dim(depth_weight, first_col, channels, 1)
    gains = lax.dynamic_slice_in_dim(norm_gain, first_col, channels, 0)
    shifts = lax.dynamic_slice_in_dim(norm_shift, first_col, channels, 0)
    reach = taps.shape[0] - 1
    gated = gated_rows(conv_value, conv_gate)
    padded = jnp.concatenate([earlier, gated], 0).astype(jnp.float32)
    filtered = taps[0] * padded[0:length]
    for offset in range(1, reach + 1):
        filtered = filtered + taps[offset] * padded[offset : offset + length]
    sums, squares = lax.psum(
        (jnp.sum(filtered, axis=1), jnp.sum(filtered * filtered, axis=1)), "tp"
    )
    all_channels = channels * lax.axis_size("tp")
    center = (sums / all_channels)[:, None]
    spread = (squares / all_channels)[:, None] - center * center
    normed = (filtered - center) * lax.rsqrt(spread + 1e-05) * gains + shifts
    activated = jax.nn.silu(normed).astype(jnp.bfloat16)
    partial_value = jnp.dot(activated, conv_out_weight, preferred_element_type=jnp.float32)
    return partial_value.astype(jnp.bfloat16)


def swapped(x, axis, mask):
    peers = lax.axis_size(axis)
    return lax.ppermute(x, axis, [(i, i ^ mask) for i in range(peers)])


def scattered_sum(partial):
    peers = lax.axis_size("tp")
    me = lax.axis_index("tp")
    size = partial.shape[0] // peers
    total = lax.dynamic_slice_in_dim(partial, me * size, size, 0).astype(jnp.float32)
    for mask in range(peers - 1, 0, -1):
        block = lax.dynamic_slice_in_dim(partial, (me ^ mask) * size, size, 0)
        total = total + swapped(block, "tp", mask).astype(jnp.float32)
    return total.astype(jnp.bfloat16)


def moe_half(moe_input, moe_gain, route_experts, route_scores, expert_gate, expert_up, expert_down):
    rows = moe_input.shape[0]
    model_width = moe_input.shape[1]
    experts_all = lax.axis_size("ep")
    capacity = 2 * (3 * TOP * rows // (4 * experts_all))
    widened = moe_input.astype(jnp.float32)
    normal_in = (
        widened * lax.rsqrt(jnp.mean(widened * widened, axis=-1, keepdims=True) + 1e-06) * moe_gain
    ).astype(jnp.bfloat16)
    chosen = route_experts.reshape(-1)
    onehot = (chosen[:, None] == jnp.arange(experts_all, dtype=jnp.int32)[None, :]).astype(
        jnp.int32
    )
    slot_rank = jnp.sum(jnp.cumsum(onehot, axis=0) * onehot, axis=-1) - 1
    slot_index = jnp.where(
        slot_rank < capacity, chosen * capacity + slot_rank, experts_all * capacity
    )
    source_row = jnp.arange(rows * TOP, dtype=jnp.int32) // TOP
    slot_token = (
        jnp.full((experts_all * capacity,), rows, jnp.int32)
        .at[slot_index]
        .set(source_row, mode="drop")
    )
    padded_in = jnp.concatenate([normal_in, jnp.zeros((1, model_width), jnp.bfloat16)], 0)
    send_buffer = padded_in[slot_token].reshape(experts_all, capacity, model_width)
    arrived = lax.all_to_all(send_buffer, "ep", split_axis=0, concat_axis=0, tiled=True)
    flat_rows = arrived.reshape(-1, model_width)
    gate_act = jnp.dot(flat_rows, expert_gate[0], preferred_element_type=jnp.float32)
    up_act = jnp.dot(flat_rows, expert_up[0], preferred_element_type=jnp.float32)
    inner = (jax.nn.silu(gate_act) * up_act).astype(jnp.bfloat16)
    result = jnp.dot(inner, expert_down[0], preferred_element_type=jnp.float32).astype(jnp.bfloat16)
    returned = lax.all_to_all(
        result.reshape(arrived.shape), "ep", split_axis=0, concat_axis=0, tiled=True
    )
    returned_flat = jnp.concatenate(
        [
            returned.reshape(experts_all * capacity, model_width),
            jnp.zeros((1, model_width), jnp.bfloat16),
        ],
        0,
    )
    picked = returned_flat[slot_index].reshape(rows, TOP, model_width)
    group_gate = jax.nn.sigmoid(route_scores[:, 0])
    first_weight = (group_gate * jax.nn.sigmoid(route_scores[:, 1]))[:, None]
    second_weight = (group_gate * jax.nn.sigmoid(-route_scores[:, 1]))[:, None]
    combined = first_weight * picked[:, 0].astype(jnp.float32) + second_weight * picked[
        :, 1
    ].astype(jnp.float32)
    return combined.astype(jnp.bfloat16)


def sigmoid(v):
    return 1.0 / (1.0 + jnp.exp(-v))


def fused(
    cap,
    value_hbm,
    gate_hbm,
    taps_ref,
    gain_ref,
    shift_ref,
    wout_hbm,
    moe_hbm,
    mgain_ref,
    experts_ref,
    scores_ref,
    egate_hbm,
    eup_hbm,
    edown_hbm,
    conv_ref,
    moe_ref,
    value,
    gate,
    gpad,
    gin,
    halo,
    wide,
    filt,
    act,
    wout,
    tokens,
    normal,
    slots,
    wpieces,
    send,
    recv,
    wsend,
    wrecv,
    ogate,
    oup,
    odown,
    pgu,
    pdown,
    inner,
    result,
    ret,
    local_sem,
    zs,
    zr,
    us,
    ur,
    rs,
    rr,
    xs,
    xr,
    ys,
    yr,
    ds,
    dr,
    es,
    er,
    gs,
    gr,
    hs,
    hr,
    cs,
    cr,
):
    ep = lax.axis_index("ep")
    tp = lax.axis_index("tp")
    last_ep = lax.axis_size("ep") - 1
    z = ep // TOP
    x = lax.rem(ep, TOP)
    core = lax.rem(tp, 2)
    y = tp // 2
    core_peer = y * 2 + (1 - core)
    y_peer = (1 - y) * 2 + core
    diag = (1 - y) * 2 + (1 - core)
    lo = z < 2
    rows, width = tokens.shape
    length, chans = value.shape
    tile = gin.shape[0] - HALO
    share = pgu.shape[1] // 8
    wpad = wsend.shape[2]

    def at(e, t):
        return {"ep": e, "tp": t}

    def remote(src, dst, ssem, rsem, e, t):
        return pltpu.make_async_remote_copy(
            src_ref=src, dst_ref=dst, send_sem=ssem, recv_sem=rsem,
            device_id=at(e, t), device_id_type=MESH,
        )

    loads = [
        pltpu.make_async_copy(moe_hbm, tokens, local_sem.at[0]),
        pltpu.make_async_copy(value_hbm, value, local_sem.at[1]),
        pltpu.make_async_copy(gate_hbm, gate, local_sem.at[2]),
        pltpu.make_async_copy(egate_hbm, ogate, local_sem.at[3]),
        pltpu.make_async_copy(eup_hbm, oup, local_sem.at[4]),
        pltpu.make_async_copy(edown_hbm, odown, local_sem.at[5]),
        pltpu.make_async_copy(wout_hbm, wout.at[tp], local_sem.at[6]),
    ]
    for load in loads:
        load.start()

    barrier = pltpu.get_barrier_semaphore()

    def greet(e, t):
        pl.semaphore_signal(barrier, inc=1, device_id=at(e, t), device_id_type=MESH)

    for step in range(1, GROUPS):
        greet(lax.rem(z + step, GROUPS) * TOP + x, tp)
    greet(z * TOP + 1 - x, tp)
    greet(ep, core_peer)
    greet(ep, y_peer)
    greet(ep, diag)

    @pl.when(ep < last_ep)
    def _():
        greet(ep + 1, 0)

    first_tp = jnp.logical_and(ep > 0, tp == 0)

    @pl.when(first_tp)
    def _():
        for t in range(4):
            greet(ep - 1, t)

    expected = (
        GROUPS + 3
        + jnp.where(ep < last_ep, 1, 0)
        + jnp.where(first_tp, 4, 0)
    )
    pl.semaphore_wait(barrier, expected)

    depth = width // 2
    half = share // 2

    def piece(j, q, gates, ups, downs, wide_cols):
        c = j % 2
        kind = j // 2
        if kind == 2:
            return downs.at[pl.ds(pl.multiple_of(q * share + c * half, half), half), :]
        span = pl.ds(c * depth, depth)
        ref = gates if kind == 0 else ups
        if wide_cols:
            col = pl.multiple_of(q * (2 * share) + kind * share, share)
        else:
            col = pl.multiple_of(q * share, share)
        return ref.at[span, pl.ds(col, share)]

    def held(j, q):
        return piece(j, q, pgu, pgu, pdown, True)

    pieces = 6
    hop_x = [
        remote(
            piece(j, tp, egate_hbm, eup_hbm, edown_hbm, False),
            held(j, tp), xs.at[j], xr.at[j], z * TOP + 1 - x, tp,
        )
        for j in range(pieces)
    ]
    hop_y = [remote(held(j, tp), held(j, tp), ys.at[j], yr.at[j], ep, y_peer) for j in range(pieces)]
    hop_d = [remote(held(j, tp), held(j, tp), ds.at[j], dr.at[j], ep, core_peer) for j in range(pieces)]
    hop_e = [
        remote(held(j, y_peer), held(j, y_peer), es.at[j], er.at[j], ep, core_peer)
        for j in range(pieces)
    ]
    for hop in hop_x:
        hop.start()

    first = jnp.broadcast_to(experts_ref[0:1, :], (8, rows))
    group_id = lax.broadcasted_iota(jnp.int32, (8, rows), 0)
    member = jnp.logical_and(first >= group_id * TOP, first < (group_id + 1) * TOP)
    before = (
        lax.broadcasted_iota(jnp.int32, (rows, rows), 0)
        < lax.broadcasted_iota(jnp.int32, (rows, rows), 1)
    ).astype(F32).astype(BF16)
    rank = jnp.dot(member.astype(F32).astype(BF16), before, preferred_element_type=F32)
    keep = jnp.logical_and(member, rank < cap)
    slots[...] = jnp.where(keep, rank, -1.0)
    group_gate = sigmoid(scores_ref[0:1, :])
    first_weight = group_gate * sigmoid(scores_ref[1:2, :])
    second_weight = group_gate * sigmoid(-scores_ref[1:2, :])
    in_order = experts_ref[0:1, :] < experts_ref[1:2, :]
    low = jnp.where(in_order, first_weight, second_weight)
    high = jnp.where(in_order, second_weight, first_weight)
    parts = []
    for weight in (low, high):
        for _ in range(3):
            rounded = weight.astype(BF16).astype(F32)
            parts.append(rounded)
            weight = weight - rounded
    nothing = jnp.zeros((2, rows), F32)
    wpieces[...] = jnp.concatenate(parts + [nothing], 0).astype(BF16)

    loads[0].wait()
    strip = 32

    def norm_rows(i, carry):
        span = pl.ds(pl.multiple_of(i * strip, strip), strip)
        wide_rows = tokens[span, :].astype(F32)
        scale = lax.rsqrt(
            jnp.sum(wide_rows * wide_rows, axis=1, keepdims=True) * (1.0 / width) + 1e-06
        )
        normal[span, :] = (wide_rows * scale * mgain_ref[...]).astype(BF16)
        return carry

    lax.fori_loop(0, rows // strip, norm_rows, 0)

    zx = z + 1 - 2 * lax.rem(z, 2)
    block = 512

    def dispatch(k, carry):
        d = jnp.where(
            k == 0, jnp.where(lo, 3, 0),
            jnp.where(k == 1, zx, jnp.where(k == 2, jnp.where(lo, 2, 1), z)),
        )
        slot = slots[pl.ds(d, 1), :]
        pick = (
            lax.broadcasted_iota(jnp.int32, (wpad, rows), 0).astype(F32)
            == jnp.broadcast_to(slot, (wpad, rows))
        ).astype(F32).astype(BF16)
        weights = lax.dot_general(
            wpieces[...], pick, (((1,), (1,)), ((), ())), preferred_element_type=F32
        )
        for n in range(width // block):
            cols = pl.ds(n * block, block)
            chosen = jnp.dot(pick[:cap], normal[:, cols], preferred_element_type=F32)
            send[d, :, cols] = chosen.astype(BF16)
        wsend[d] = weights

        @pl.when(k < 3)
        def _():
            remote(
                send.at[d], recv.at[z], zs.at[d], zr.at[z], d * TOP + x, tp
            ).start()
            remote(
                wsend.at[d], wrecv.at[z], us.at[d], ur.at[z], d * TOP + x, tp
            ).start()

        return carry

    lax.fori_loop(0, 4, dispatch, 0)
    recv[z] = send[z]
    wrecv[z] = wsend[z]

    loads[1].wait()
    loads[2].wait()
    gpad[0:HALO, :] = jnp.zeros((HALO, chans), BF16)
    gstrip = 64

    def gate_rows(i, carry):
        span = pl.ds(pl.multiple_of(i * gstrip, gstrip), gstrip)
        out = pl.ds(pl.multiple_of(i * gstrip + HALO, HALO), gstrip)
        gpad[out, :] = (value[span, :].astype(F32) * sigmoid(gate[span, :].astype(F32))).astype(BF16)
        return carry

    lax.fori_loop(0, length // gstrip, gate_rows, 0)
    my_cols = pl.ds(pl.multiple_of(tp * chans, LANES), chans)

    def window(t):
        return pl.ds(pl.multiple_of(t * tile, HALO), tile + HALO)

    gated_copies = [
        remote(gpad.at[window(t)], gin.at[:, my_cols], gs.at[i], gr.at[i], ep, t)
        for i, t in enumerate((core_peer, y_peer, diag))
    ]
    for copy in gated_copies:
        copy.start()

    def halo_copy(t, e, c):
        cols = pl.ds(pl.multiple_of(c * chans, LANES), chans)
        return remote(
            gpad.at[pl.ds(length, HALO)], halo.at[:, cols], hs, hr.at[c], e, t
        )

    @pl.when(ep < last_ep)
    def _():
        halo_copy(0, ep + 1, tp).start()

    gin[:, my_cols] = gpad[window(tp), :]

    for g in range(GROUPS):
        ret[g, cap:, :] = jnp.zeros((ret.shape[1] - cap, width), BF16)

    own_wout = wout.at[tp]
    out_y = remote(own_wout, own_wout, cs.at[0], cr.at[0], ep, y_peer)
    out_d = remote(own_wout, own_wout, cs.at[1], cr.at[1], ep, core_peer)
    out_e = remote(wout.at[y_peer], wout.at[y_peer], cs.at[2], cr.at[2], ep, core_peer)

    taps_count = taps_ref.shape[0]
    lane_blocks = gin.shape[1] // LANES
    frows = 64

    def widen():
        for copy in gated_copies:
            copy.wait_recv()

        @pl.when(first_tp)
        def _():
            for c in range(4):
                halo_copy(0, ep, c).wait_recv()
            gin[0:HALO, :] = halo[...]

        for b in range(lane_blocks):
            wide[b] = gin[:, b * LANES : (b + 1) * LANES].astype(F32)

    def filter_block(b, carry):
        for r in range(tile // frows):
            total = jnp.zeros((frows, LANES), F32)
            for k in range(taps_count):
                start = r * frows + HALO - taps_count + 1 + k
                tap = taps_ref[pl.ds(k, 1), pl.ds(pl.multiple_of(b * LANES, LANES), LANES)]
                total = total + tap * wide[b, pl.ds(start, frows), :]
            filt[b, pl.ds(r * frows, frows), :] = total
        return carry

    def activate(i, carry):
        span = pl.ds(pl.multiple_of(i * strip, strip), strip)
        total = filt[0, span, :]
        squares = total * total
        for b in range(1, lane_blocks):
            part = filt[b, span, :]
            total = total + part
            squares = squares + part * part
        count = 1.0 / (lane_blocks * LANES)
        center = jnp.sum(total, axis=1, keepdims=True) * count
        spread = jnp.sum(squares, axis=1, keepdims=True) * count - center * center
        scale = lax.rsqrt(spread + 1e-05)
        for b in range(lane_blocks):
            cols = slice(b * LANES, (b + 1) * LANES)
            normed = (filt[b, span, :] - center) * scale * gain_ref[:, cols] + shift_ref[:, cols]
            act[span, cols] = (normed * sigmoid(normed)).astype(BF16)
        return carry

    for j in range(pieces):
        hop_x[j].wait_recv()
        hop_y[j].start()
        hop_d[j].start()
        if j > 0:
            hop_y[j - 1].wait_recv()
            hop_e[j - 1].start()
        if j == 1:
            widen()
            lax.fori_loop(0, 2, filter_block, 0)
        if 2 <= j < 5:
            lax.fori_loop(2 * j - 2, 2 * j, filter_block, 0)
        if j == 5:
            lax.fori_loop(0, tile // strip, activate, 0)
    loads[6].wait()
    out_y.start()
    out_d.start()
    hop_y[pieces - 1].wait_recv()
    hop_e[pieces - 1].start()
    for load in loads[3:6]:
        load.wait()
    for j in range(pieces):
        hop_d[j].wait_recv()
        hop_e[j].wait_recv()

    ff = ogate.shape[1]
    even = x == 0
    nb = 256

    def expert(i, carry):
        even_z = lax.rem(z, 2) == 0
        s = jnp.where(
            i == 0, jnp.where(even_z, 3, 0),
            jnp.where(
                i == 1, lax.rem(z + 2, GROUPS),
                jnp.where(i == 2, jnp.where(even_z, 1, 2), z),
            ),
        )

        @pl.when(i < 3)
        def _():
            remote(send.at[s], recv.at[s], zs.at[s], zr.at[s], s * TOP + x, tp).wait_recv()
            remote(wsend.at[s], wrecv.at[s], us.at[s], ur.at[s], s * TOP + x, tp).wait_recv()

        w8 = wrecv[s]
        w_low = w8[0:1] + w8[1:2] + w8[2:3]
        w_high = w8[3:4] + w8[4:5] + w8[5:6]
        mine = jnp.where(even, w_low, w_high)
        theirs = jnp.where(even, w_high, w_low)
        mine = jnp.transpose(jnp.broadcast_to(mine, (LANES, wpad)))[:cap]
        theirs = jnp.transpose(jnp.broadcast_to(theirs, (LANES, wpad)))[:cap]
        mine2 = jnp.concatenate([mine] * (nb // LANES), 1)
        theirs1 = jnp.concatenate([theirs] * (share // LANES), 1)
        here = recv[s]
        for n in range(ff // nb):
            cols = pl.ds(n * nb, nb)
            g = jnp.dot(here, ogate[:, cols], preferred_element_type=F32)
            u = jnp.dot(here, oup[:, cols], preferred_element_type=F32)
            inner[:, cols] = (g * sigmoid(g) * u * mine2).astype(BF16)
        for q in range(4):
            gu = jnp.dot(
                here, pgu[:, pl.ds(q * 2 * share, 2 * share)], preferred_element_type=F32
            )
            g = gu[:, :share]
            u = gu[:, share:]
            inner[:, pl.ds(ff + q * share, share)] = (g * sigmoid(g) * u * theirs1).astype(BF16)
        for n in range(width // nb):
            cols = pl.ds(n * nb, nb)
            total = jnp.dot(inner[:, :ff], odown[:, cols], preferred_element_type=F32) + jnp.dot(
                inner[:, ff:], pdown[:, cols], preferred_element_type=F32
            )
            result[s, :, cols] = total.astype(BF16)

        @pl.when(i < 3)
        def _():
            remote(
                result.at[s], ret.at[z, pl.ds(0, cap)], rs.at[s], rr.at[z], s * TOP + x, tp
            ).start()

        return carry

    lax.fori_loop(0, 4, expert, 0)
    ret[z, pl.ds(0, cap), :] = result[z]

    out_y.wait_recv()
    out_e.start()
    out_d.wait_recv()
    out_e.wait_recv()

    def project(n, carry):
        cols = pl.ds(pl.multiple_of(n * nb, nb), nb)
        total = jnp.dot(act[:, 0:chans], wout[0, :, cols], preferred_element_type=F32)
        for t in range(1, 4):
            total = total + jnp.dot(
                act[:, t * chans : (t + 1) * chans], wout[t, :, cols], preferred_element_type=F32
            )
        conv_ref[:, cols] = total.astype(BF16)
        return carry

    lax.fori_loop(0, width // nb, project, 0)

    def put(g):
        slot = jnp.transpose(jnp.broadcast_to(slots[pl.ds(g, 1), :], (LANES, rows)))
        lane = lax.broadcasted_iota(jnp.int32, (rows, LANES), 1).astype(F32)
        return jnp.concatenate(
            [(slot == lane + float(b * LANES)).astype(F32).astype(BF16) for b in range(wpad // LANES)],
            1,
        )

    def returned(g):
        return remote(
            result.at[g], ret.at[g, pl.ds(0, cap)], rs.at[g], rr.at[g], g * TOP + x, tp
        )

    third = jnp.where(lo, 3, 0)
    last = jnp.where(lo, 2, 1)

    def add_back(g, fresh):
        chosen = put(g)
        for n in range(width // nb):
            cols = pl.ds(n * nb, nb)
            rows_back = jnp.dot(chosen, ret[g, :, cols], preferred_element_type=F32)
            if fresh:
                moe_ref[:, cols] = rows_back.astype(BF16)
            else:
                moe_ref[:, cols] = (moe_ref[:, cols].astype(F32) + rows_back).astype(BF16)

    add_back(z, True)

    def rest(i, carry):
        g = jnp.where(i == 0, zx, jnp.where(i == 1, third, last))
        returned(g).wait_recv()
        add_back(g, False)
        return carry

    lax.fori_loop(0, 3, rest, 0)

    for step in range(1, GROUPS):
        s = lax.rem(z + step, GROUPS)
        remote(send.at[s], recv.at[s], zs.at[s], zr.at[s], s * TOP + x, tp).wait_send()
        remote(wsend.at[s], wrecv.at[s], us.at[s], ur.at[s], s * TOP + x, tp).wait_send()
        returned(s).wait_send()
    for j in range(pieces):
        hop_x[j].wait_send()
        hop_y[j].wait_send()
        hop_d[j].wait_send()
        hop_e[j].wait_send()
    for copy in gated_copies:
        copy.wait_send()

    @pl.when(ep < last_ep)
    def _():
        halo_copy(0, ep + 1, tp).wait_send()

    out_y.wait_send()
    out_d.wait_send()
    out_e.wait_send()


def one_kernel(
    conv_value, conv_gate, depth_weight, norm_gain, norm_shift, conv_out_weight,
    moe_input, moe_gain, route_experts, route_scores, expert_gate, expert_up, expert_down,
):
    length, chans = conv_value.shape
    peers = lax.axis_size("tp")
    tile = length // peers
    all_chans = chans * peers
    rows, width = moe_input.shape
    ff = expert_gate.shape[2]
    cap = 2 * (3 * TOP * rows // (4 * lax.axis_size("ep")))
    wpad = -(-cap // LANES) * LANES
    vmem = pl.BlockSpec(memory_space=pltpu.VMEM)
    hbm = pl.BlockSpec(memory_space=pl.ANY)
    dma = pltpu.SemaphoreType.DMA
    blocks = all_chans // LANES
    return pl.pallas_call(
        functools.partial(fused, cap),
        out_shape=(
            jax.ShapeDtypeStruct((tile, width), BF16),
            jax.ShapeDtypeStruct((rows, width), BF16),
        ),
        in_specs=[hbm, hbm, vmem, vmem, vmem, hbm, hbm, vmem, vmem, vmem, hbm, hbm, hbm],
        out_specs=(vmem, vmem),
        scratch_shapes=[
            pltpu.VMEM((length, chans), BF16),
            pltpu.VMEM((length, chans), BF16),
            pltpu.VMEM((length + HALO, chans), BF16),
            pltpu.VMEM((tile + HALO, all_chans), BF16),
            pltpu.VMEM((HALO, all_chans), BF16),
            pltpu.VMEM((blocks, tile + HALO, LANES), F32),
            pltpu.VMEM((blocks, tile, LANES), F32),
            pltpu.VMEM((tile, all_chans), BF16),
            pltpu.VMEM((peers, chans, width), BF16),
            pltpu.VMEM((rows, width), BF16),
            pltpu.VMEM((rows, width), BF16),
            pltpu.VMEM((8, rows), F32),
            pltpu.VMEM((8, rows), BF16),
            pltpu.VMEM((GROUPS, cap, width), BF16),
            pltpu.VMEM((GROUPS, cap, width), BF16),
            pltpu.VMEM((GROUPS, 8, wpad), F32),
            pltpu.VMEM((GROUPS, 8, wpad), F32),
            pltpu.VMEM((width, ff), BF16),
            pltpu.VMEM((width, ff), BF16),
            pltpu.VMEM((ff, width), BF16),
            pltpu.VMEM((width, 2 * ff), BF16),
            pltpu.VMEM((ff, width), BF16),
            pltpu.VMEM((cap, 2 * ff), BF16),
            pltpu.VMEM((GROUPS, cap, width), BF16),
            pltpu.VMEM((GROUPS, wpad, width), BF16),
            dma((7,)),
            dma((GROUPS,)), dma((GROUPS,)),
            dma((GROUPS,)), dma((GROUPS,)),
            dma((GROUPS,)), dma((GROUPS,)),
            dma((6,)), dma((6,)),
            dma((6,)), dma((6,)),
            dma((6,)), dma((6,)),
            dma((6,)), dma((6,)),
            dma((3,)), dma((3,)),
            dma(()), dma((4,)),
            dma((3,)), dma((3,)),
        ],
        compiler_params=pltpu.CompilerParams(
            collective_id=0, has_side_effects=True, vmem_limit_bytes=63 * 1024 * 1024
        ),
        name="fused",
    )(
        conv_value, conv_gate, depth_weight, norm_gain[None, :], norm_shift[None, :],
        conv_out_weight, moe_input, moe_gain[None, :], route_experts.T, route_scores.T,
        expert_gate[0], expert_up[0], expert_down[0],
    )


def on_device(
    conv_value,
    conv_gate,
    depth_weight,
    norm_gain,
    norm_shift,
    conv_out_weight,
    moe_input,
    moe_gain,
    route_experts,
    route_scores,
    expert_gate,
    expert_up,
    expert_down,
):
    conv_args = (conv_value, conv_gate, depth_weight, norm_gain, norm_shift, conv_out_weight)
    moe_args = (
        moe_input, moe_gain, route_experts, route_scores, expert_gate, expert_up, expert_down
    )
    if lax.axis_size("ep") == GROUPS * TOP and lax.axis_size("tp") == 4:
        return one_kernel(*conv_args, *moe_args)
    last = conv_value.shape[0] - depth_weight.shape[0] + 1
    earlier = passed_along(gated_rows(conv_value[last:], conv_gate[last:]), "ep", 1)
    partial = conv_half(conv_value, conv_gate, earlier, *conv_args[2:])
    return (scattered_sum(partial), moe_half(*moe_args))


def solution(mesh):
    in_specs = (
        P("ep", "tp"),
        P("ep", "tp"),
        P(),
        P(),
        P(),
        P("tp", None),
        P(("ep", "tp"), None),
        P(),
        P(("ep", "tp"), None),
        P(("ep", "tp"), None),
        P("ep", None, None),
        P("ep", None, None),
        P("ep", None, None),
    )
    out_specs = (P(("ep", "tp"), None), P(("ep", "tp"), None))
    return jax.shard_map(
        on_device, mesh=mesh, in_specs=in_specs, out_specs=out_specs, check_vma=False
    )
```

```python
import functools

import jax
import jax.numpy as jnp
from jax import lax
from jax.experimental import pallas as pl
from jax.experimental.pallas import tpu as pltpu
from jax.sharding import PartitionSpec as P

GROUPS = 4
TOP = 2
LANES = 128
HALO = 32
MESH = pl.DeviceIdType.MESH
F32 = jnp.float32
BF16 = jnp.bfloat16


def passed_along(x, axis, by):
    peers = lax.axis_size(axis)
    pairs = [(i, i + by) for i in range(peers) if 0 <= i + by < peers]
    return lax.ppermute(x, axis, pairs)


def gated_rows(value, gate):
    return (value.astype(jnp.float32) * jax.nn.sigmoid(gate.astype(jnp.float32))).astype(
        jnp.bfloat16
    )


def conv_half(conv_value, conv_gate, earlier, depth_weight, norm_gain, norm_shift, conv_out_weight):
    channels = conv_value.shape[1]
    length = conv_value.shape[0]
    first_col = lax.axis_index("tp") * channels
    taps = lax.dynamic_slice_in_dim(depth_weight, first_col, channels, 1)
    gains = lax.dynamic_slice_in_dim(norm_gain, first_col, channels, 0)
    shifts = lax.dynamic_slice_in_dim(norm_shift, first_col, channels, 0)
    reach = taps.shape[0] - 1
    gated = gated_rows(conv_value, conv_gate)
    padded = jnp.concatenate([earlier, gated], 0).astype(jnp.float32)
    filtered = taps[0] * padded[0:length]
    for offset in range(1, reach + 1):
        filtered = filtered + taps[offset] * padded[offset : offset + length]
    sums, squares = lax.psum(
        (jnp.sum(filtered, axis=1), jnp.sum(filtered * filtered, axis=1)), "tp"
    )
    all_channels = channels * lax.axis_size("tp")
    center = (sums / all_channels)[:, None]
    spread = (squares / all_channels)[:, None] - center * center
    normed = (filtered - center) * lax.rsqrt(spread + 1e-05) * gains + shifts
    activated = jax.nn.silu(normed).astype(jnp.bfloat16)
    partial_value = jnp.dot(activated, conv_out_weight, preferred_element_type=jnp.float32)
    return partial_value.astype(jnp.bfloat16)


def swapped(x, axis, mask):
    peers = lax.axis_size(axis)
    return lax.ppermute(x, axis, [(i, i ^ mask) for i in range(peers)])


def scattered_sum(partial):
    peers = lax.axis_size("tp")
    me = lax.axis_index("tp")
    size = partial.shape[0] // peers
    total = lax.dynamic_slice_in_dim(partial, me * size, size, 0).astype(jnp.float32)
    for mask in range(peers - 1, 0, -1):
        block = lax.dynamic_slice_in_dim(partial, (me ^ mask) * size, size, 0)
        total = total + swapped(block, "tp", mask).astype(jnp.float32)
    return total.astype(jnp.bfloat16)


def moe_half(moe_input, moe_gain, route_experts, route_scores, expert_gate, expert_up, expert_down):
    rows = moe_input.shape[0]
    model_width = moe_input.shape[1]
    experts_all = lax.axis_size("ep")
    capacity = 2 * (3 * TOP * rows // (4 * experts_all))
    widened = moe_input.astype(jnp.float32)
    normal_in = (
        widened * lax.rsqrt(jnp.mean(widened * widened, axis=-1, keepdims=True) + 1e-06) * moe_gain
    ).astype(jnp.bfloat16)
    chosen = route_experts.reshape(-1)
    onehot = (chosen[:, None] == jnp.arange(experts_all, dtype=jnp.int32)[None, :]).astype(
        jnp.int32
    )
    slot_rank = jnp.sum(jnp.cumsum(onehot, axis=0) * onehot, axis=-1) - 1
    slot_index = jnp.where(
        slot_rank < capacity, chosen * capacity + slot_rank, experts_all * capacity
    )
    source_row = jnp.arange(rows * TOP, dtype=jnp.int32) // TOP
    slot_token = (
        jnp.full((experts_all * capacity,), rows, jnp.int32)
        .at[slot_index]
        .set(source_row, mode="drop")
    )
    padded_in = jnp.concatenate([normal_in, jnp.zeros((1, model_width), jnp.bfloat16)], 0)
    send_buffer = padded_in[slot_token].reshape(experts_all, capacity, model_width)
    arrived = lax.all_to_all(send_buffer, "ep", split_axis=0, concat_axis=0, tiled=True)
    flat_rows = arrived.reshape(-1, model_width)
    gate_act = jnp.dot(flat_rows, expert_gate[0], preferred_element_type=jnp.float32)
    up_act = jnp.dot(flat_rows, expert_up[0], preferred_element_type=jnp.float32)
    inner = (jax.nn.silu(gate_act) * up_act).astype(jnp.bfloat16)
    result = jnp.dot(inner, expert_down[0], preferred_element_type=jnp.float32).astype(jnp.bfloat16)
    returned = lax.all_to_all(
        result.reshape(arrived.shape), "ep", split_axis=0, concat_axis=0, tiled=True
    )
    returned_flat = jnp.concatenate(
        [
            returned.reshape(experts_all * capacity, model_width),
            jnp.zeros((1, model_width), jnp.bfloat16),
        ],
        0,
    )
    picked = returned_flat[slot_index].reshape(rows, TOP, model_width)
    group_gate = jax.nn.sigmoid(route_scores[:, 0])
    first_weight = (group_gate * jax.nn.sigmoid(route_scores[:, 1]))[:, None]
    second_weight = (group_gate * jax.nn.sigmoid(-route_scores[:, 1]))[:, None]
    combined = first_weight * picked[:, 0].astype(jnp.float32) + second_weight * picked[
        :, 1
    ].astype(jnp.float32)
    return combined.astype(jnp.bfloat16)


def sigmoid(v):
    return 1.0 / (1.0 + jnp.exp(-v))


def fused(
    cap,
    value_hbm,
    gate_hbm,
    taps_hbm,
    gain_hbm,
    shift_hbm,
    wout_hbm,
    moe_hbm,
    mgain_hbm,
    experts_hbm,
    scores_hbm,
    egate_hbm,
    eup_hbm,
    edown_hbm,
    conv_ref,
    moe_ref,
    taps_ref,
    gain_ref,
    shift_ref,
    mgain_ref,
    experts_ref,
    scores_ref,
    value,
    gate,
    gpad,
    gin,
    halo,
    edge,
    wide,
    filt,
    act,
    wout,
    tokens,
    normal,
    slots,
    wpieces,
    send,
    recv,
    wsend,
    wrecv,
    ogate,
    oup,
    odown,
    pgu,
    pdown,
    inner,
    result,
    ret,
    local_sem,
    zs,
    zr,
    us,
    ur,
    rs,
    rr,
    xs,
    xr,
    ys,
    yr,
    ds,
    dr,
    es,
    er,
    gs,
    gr,
    hs,
    hr,
    cs,
    cr,
):
    ep = lax.axis_index("ep")
    tp = lax.axis_index("tp")
    last_ep = lax.axis_size("ep") - 1
    z = ep // TOP
    x = lax.rem(ep, TOP)
    core = lax.rem(tp, 2)
    y = tp // 2
    core_peer = y * 2 + (1 - core)
    y_peer = (1 - y) * 2 + core
    diag = (1 - y) * 2 + (1 - core)
    lo = z < 2
    rows, width = tokens.shape
    length, chans = value.shape
    tile = gin.shape[0] - HALO
    share = pgu.shape[1] // 8
    wpad = wsend.shape[2]

    def at(e, t):
        return {"ep": e, "tp": t}

    def remote(src, dst, ssem, rsem, e, t):
        return pltpu.make_async_remote_copy(
            src_ref=src, dst_ref=dst, send_sem=ssem, recv_sem=rsem,
            device_id=at(e, t), device_id_type=MESH,
        )

    small = [
        pltpu.make_async_copy(experts_hbm, experts_ref, local_sem.at[9]),
        pltpu.make_async_copy(scores_hbm, scores_ref, local_sem.at[10]),
        pltpu.make_async_copy(mgain_hbm, mgain_ref, local_sem.at[11]),
        pltpu.make_async_copy(taps_hbm, taps_ref, local_sem.at[12]),
        pltpu.make_async_copy(gain_hbm, gain_ref, local_sem.at[13]),
        pltpu.make_async_copy(shift_hbm, shift_ref, local_sem.at[14]),
    ]
    for load in small[:3]:
        load.start()
    loads = [
        pltpu.make_async_copy(moe_hbm, tokens, local_sem.at[0]),
        pltpu.make_async_copy(value_hbm, value, local_sem.at[1]),
        pltpu.make_async_copy(gate_hbm, gate, local_sem.at[2]),
        pltpu.make_async_copy(egate_hbm, ogate, local_sem.at[3]),
        pltpu.make_async_copy(eup_hbm, oup, local_sem.at[4]),
        pltpu.make_async_copy(edown_hbm, odown, local_sem.at[5]),
        pltpu.make_async_copy(wout_hbm, wout.at[tp], local_sem.at[6]),
        pltpu.make_async_copy(value_hbm.at[pl.ds(length - HALO, HALO)], edge.at[0], local_sem.at[7]),
        pltpu.make_async_copy(gate_hbm.at[pl.ds(length - HALO, HALO)], edge.at[1], local_sem.at[8]),
    ]
    for load in loads[:1] + loads[7:] + loads[1:7] + small[3:]:
        load.start()

    barrier = pltpu.get_barrier_semaphore()

    def greet(e, t):
        pl.semaphore_signal(barrier, inc=1, device_id=at(e, t), device_id_type=MESH)

    for step in range(1, GROUPS):
        greet(lax.rem(z + step, GROUPS) * TOP + x, tp)
    greet(z * TOP + 1 - x, tp)
    greet(ep, core_peer)
    greet(ep, y_peer)
    greet(ep, diag)

    @pl.when(ep < last_ep)
    def _():
        greet(ep + 1, 0)

    first_tp = jnp.logical_and(ep > 0, tp == 0)

    @pl.when(first_tp)
    def _():
        for t in range(4):
            greet(ep - 1, t)

    expected = (
        GROUPS + 3
        + jnp.where(ep < last_ep, 1, 0)
        + jnp.where(first_tp, 4, 0)
    )

    depth = width // 2
    half = share // 2

    def piece(j, q, gates, ups, downs, wide_cols):
        c = j % 2
        kind = j // 2
        if kind == 2:
            return downs.at[pl.ds(pl.multiple_of(q * share + c * half, half), half), :]
        span = pl.ds(c * depth, depth)
        ref = gates if kind == 0 else ups
        if wide_cols:
            col = pl.multiple_of(q * (2 * share) + kind * share, share)
        else:
            col = pl.multiple_of(q * share, share)
        return ref.at[span, pl.ds(col, share)]

    def held(j, q):
        return piece(j, q, pgu, pgu, pdown, True)

    pieces = 6
    hop_x = [
        remote(
            piece(j, tp, egate_hbm, eup_hbm, edown_hbm, False),
            held(j, tp), xs.at[j], xr.at[j], z * TOP + 1 - x, tp,
        )
        for j in range(pieces)
    ]
    hop_y = [remote(held(j, tp), held(j, tp), ys.at[j], yr.at[j], ep, y_peer) for j in range(pieces)]
    hop_d = [remote(held(j, tp), held(j, tp), ds.at[j], dr.at[j], ep, core_peer) for j in range(pieces)]
    hop_e = [
        remote(held(j, y_peer), held(j, y_peer), es.at[j], er.at[j], ep, core_peer)
        for j in range(pieces)
    ]

    small[0].wait()
    small[1].wait()
    small[2].wait()
    first = jnp.broadcast_to(experts_ref[0:1, :], (8, rows))
    group_id = lax.broadcasted_iota(jnp.int32, (8, rows), 0)
    member = jnp.logical_and(first >= group_id * TOP, first < (group_id + 1) * TOP)
    before = (
        lax.broadcasted_iota(jnp.int32, (rows, rows), 0)
        < lax.broadcasted_iota(jnp.int32, (rows, rows), 1)
    ).astype(F32).astype(BF16)
    rank = jnp.dot(member.astype(F32).astype(BF16), before, preferred_element_type=F32)
    keep = jnp.logical_and(member, rank < cap)
    slots[...] = jnp.where(keep, rank, -1.0)
    group_gate = sigmoid(scores_ref[0:1, :])
    first_weight = group_gate * sigmoid(scores_ref[1:2, :])
    second_weight = group_gate * sigmoid(-scores_ref[1:2, :])
    in_order = experts_ref[0:1, :] < experts_ref[1:2, :]
    low = jnp.where(in_order, first_weight, second_weight)
    high = jnp.where(in_order, second_weight, first_weight)
    parts = []
    for weight in (low, high):
        for _ in range(3):
            rounded = weight.astype(BF16).astype(F32)
            parts.append(rounded)
            weight = weight - rounded
    nothing = jnp.zeros((2, rows), F32)
    wpieces[...] = jnp.concatenate(parts + [nothing], 0).astype(BF16)

    loads[0].wait()
    strip = 32

    def norm_rows(i, carry):
        span = pl.ds(pl.multiple_of(i * strip, strip), strip)
        wide_rows = tokens[span, :].astype(F32)
        scale = lax.rsqrt(
            jnp.sum(wide_rows * wide_rows, axis=1, keepdims=True) * (1.0 / width) + 1e-06
        )
        normal[span, :] = (wide_rows * scale * mgain_ref[...]).astype(BF16)
        return carry

    lax.fori_loop(0, rows // strip, norm_rows, 0)

    def halo_copy(t, e, c):
        cols = pl.ds(pl.multiple_of(c * chans, LANES), chans)
        return remote(edge.at[2], halo.at[:, cols], hs, hr.at[c], e, t)

    loads[7].wait()
    loads[8].wait()
    edge[2] = (edge[0].astype(F32) * sigmoid(edge[1].astype(F32))).astype(BF16)
    pl.semaphore_wait(barrier, expected)
    for hop in hop_x:
        hop.start()

    @pl.when(ep < last_ep)
    def _():
        halo_copy(0, ep + 1, tp).start()

    zx = z + 1 - 2 * lax.rem(z, 2)
    block = 512

    def dispatch(k, carry):
        d = jnp.where(
            k == 0, jnp.where(lo, 3, 0),
            jnp.where(k == 1, zx, jnp.where(k == 2, jnp.where(lo, 2, 1), z)),
        )
        slot = slots[pl.ds(d, 1), :]
        pick = (
            lax.broadcasted_iota(jnp.int32, (wpad, rows), 0).astype(F32)
            == jnp.broadcast_to(slot, (wpad, rows))
        ).astype(F32).astype(BF16)
        weights = lax.dot_general(
            wpieces[...], pick, (((1,), (1,)), ((), ())), preferred_element_type=F32
        )
        for n in range(width // block):
            cols = pl.ds(n * block, block)
            chosen = jnp.dot(pick[:cap], normal[:, cols], preferred_element_type=F32)
            send[d, :, cols] = chosen.astype(BF16)
        wsend[d] = weights

        @pl.when(k < 3)
        def _():
            remote(
                send.at[d], recv.at[z], zs.at[d], zr.at[z], d * TOP + x, tp
            ).start()
            remote(
                wsend.at[d], wrecv.at[z], us.at[d], ur.at[z], d * TOP + x, tp
            ).start()

        return carry

    lax.fori_loop(0, 4, dispatch, 0)
    recv[z] = send[z]
    wrecv[z] = wsend[z]

    loads[1].wait()
    loads[2].wait()
    gpad[0:HALO, :] = jnp.zeros((HALO, chans), BF16)
    gstrip = 64

    def gate_rows(i, carry):
        span = pl.ds(pl.multiple_of(i * gstrip, gstrip), gstrip)
        out = pl.ds(pl.multiple_of(i * gstrip + HALO, HALO), gstrip)
        gpad[out, :] = (value[span, :].astype(F32) * sigmoid(gate[span, :].astype(F32))).astype(BF16)
        return carry

    lax.fori_loop(0, length // gstrip, gate_rows, 0)
    my_cols = pl.ds(pl.multiple_of(tp * chans, LANES), chans)

    def window(t):
        return pl.ds(pl.multiple_of(t * tile, HALO), tile + HALO)

    gated_copies = [
        remote(gpad.at[window(t)], gin.at[:, my_cols], gs.at[i], gr.at[i], ep, t)
        for i, t in enumerate((core_peer, y_peer, diag))
    ]
    for copy in gated_copies:
        copy.start()

    gin[:, my_cols] = gpad[window(tp), :]

    for g in range(GROUPS):
        ret[g, cap:, :] = jnp.zeros((ret.shape[1] - cap, width), BF16)

    own_wout = wout.at[tp]
    out_y = remote(own_wout, own_wout, cs.at[0], cr.at[0], ep, y_peer)
    out_d = remote(own_wout, own_wout, cs.at[1], cr.at[1], ep, core_peer)
    out_e = remote(wout.at[y_peer], wout.at[y_peer], cs.at[2], cr.at[2], ep, core_peer)

    taps_count = taps_ref.shape[0]
    lane_blocks = gin.shape[1] // LANES
    frows = 64

    def widen():
        for copy in gated_copies:
            copy.wait_recv()

        @pl.when(first_tp)
        def _():
            for c in range(4):
                halo_copy(0, ep, c).wait_recv()
            gin[0:HALO, :] = halo[...]

        for b in range(lane_blocks):
            wide[b] = gin[:, b * LANES : (b + 1) * LANES].astype(F32)

    def filter_block(b, carry):
        for r in range(tile // frows):
            total = jnp.zeros((frows, LANES), F32)
            for k in range(taps_count):
                start = r * frows + HALO - taps_count + 1 + k
                tap = taps_ref[pl.ds(k, 1), pl.ds(pl.multiple_of(b * LANES, LANES), LANES)]
                total = total + tap * wide[b, pl.ds(start, frows), :]
            filt[b, pl.ds(r * frows, frows), :] = total
        return carry

    def activate(i, carry):
        span = pl.ds(pl.multiple_of(i * strip, strip), strip)
        total = filt[0, span, :]
        squares = total * total
        for b in range(1, lane_blocks):
            part = filt[b, span, :]
            total = total + part
            squares = squares + part * part
        count = 1.0 / (lane_blocks * LANES)
        center = jnp.sum(total, axis=1, keepdims=True) * count
        spread = jnp.sum(squares, axis=1, keepdims=True) * count - center * center
        scale = lax.rsqrt(spread + 1e-05)
        for b in range(lane_blocks):
            cols = slice(b * LANES, (b + 1) * LANES)
            normed = (filt[b, span, :] - center) * scale * gain_ref[:, cols] + shift_ref[:, cols]
            act[span, cols] = (normed * sigmoid(normed)).astype(BF16)
        return carry

    for j in range(pieces):
        hop_x[j].wait_recv()
        hop_y[j].start()
        hop_d[j].start()
        if j > 0:
            hop_y[j - 1].wait_recv()
            hop_e[j - 1].start()
        if j == 1:
            for load in small[3:]:
                load.wait()
            widen()
            lax.fori_loop(0, 2, filter_block, 0)
        if 2 <= j < 5:
            lax.fori_loop(2 * j - 2, 2 * j, filter_block, 0)
        if j == 5:
            lax.fori_loop(0, tile // strip, activate, 0)
    loads[6].wait()
    out_y.start()
    out_d.start()
    hop_y[pieces - 1].wait_recv()
    hop_e[pieces - 1].start()
    for load in loads[3:6]:
        load.wait()
    for j in range(pieces):
        hop_d[j].wait_recv()
        hop_e[j].wait_recv()

    ff = ogate.shape[1]
    even = x == 0
    nb = 256

    def expert(i, carry):
        even_z = lax.rem(z, 2) == 0
        s = jnp.where(
            i == 0, jnp.where(even_z, 3, 0),
            jnp.where(
                i == 1, lax.rem(z + 2, GROUPS),
                jnp.where(i == 2, jnp.where(even_z, 1, 2), z),
            ),
        )

        @pl.when(i < 3)
        def _():
            remote(send.at[s], recv.at[s], zs.at[s], zr.at[s], s * TOP + x, tp).wait_recv()
            remote(wsend.at[s], wrecv.at[s], us.at[s], ur.at[s], s * TOP + x, tp).wait_recv()

        w8 = wrecv[s]
        w_low = w8[0:1] + w8[1:2] + w8[2:3]
        w_high = w8[3:4] + w8[4:5] + w8[5:6]
        mine = jnp.where(even, w_low, w_high)
        theirs = jnp.where(even, w_high, w_low)
        mine = jnp.transpose(jnp.broadcast_to(mine, (LANES, wpad)))[:cap]
        theirs = jnp.transpose(jnp.broadcast_to(theirs, (LANES, wpad)))[:cap]
        mine2 = jnp.concatenate([mine] * (nb // LANES), 1)
        theirs1 = jnp.concatenate([theirs] * (share // LANES), 1)
        here = recv[s]
        for n in range(ff // nb):
            cols = pl.ds(n * nb, nb)
            g = jnp.dot(here, ogate[:, cols], preferred_element_type=F32)
            u = jnp.dot(here, oup[:, cols], preferred_element_type=F32)
            inner[:, cols] = (g * sigmoid(g) * u * mine2).astype(BF16)
        for q in range(4):
            gu = jnp.dot(
                here, pgu[:, pl.ds(q * 2 * share, 2 * share)], preferred_element_type=F32
            )
            g = gu[:, :share]
            u = gu[:, share:]
            inner[:, pl.ds(ff + q * share, share)] = (g * sigmoid(g) * u * theirs1).astype(BF16)
        for n in range(width // nb):
            cols = pl.ds(n * nb, nb)
            total = jnp.dot(inner[:, :ff], odown[:, cols], preferred_element_type=F32) + jnp.dot(
                inner[:, ff:], pdown[:, cols], preferred_element_type=F32
            )
            result[s, :, cols] = total.astype(BF16)

        @pl.when(i < 3)
        def _():
            remote(
                result.at[s], ret.at[z, pl.ds(0, cap)], rs.at[s], rr.at[z], s * TOP + x, tp
            ).start()

        return carry

    lax.fori_loop(0, 4, expert, 0)
    ret[z, pl.ds(0, cap), :] = result[z]

    out_y.wait_recv()
    out_e.start()
    out_d.wait_recv()
    out_e.wait_recv()

    def project(n, carry):
        cols = pl.ds(pl.multiple_of(n * nb, nb), nb)
        total = jnp.dot(act[:, 0:chans], wout[0, :, cols], preferred_element_type=F32)
        for t in range(1, 4):
            total = total + jnp.dot(
                act[:, t * chans : (t + 1) * chans], wout[t, :, cols], preferred_element_type=F32
            )
        conv_ref[:, cols] = total.astype(BF16)
        return carry

    lax.fori_loop(0, width // nb, project, 0)

    def put(g):
        slot = jnp.transpose(jnp.broadcast_to(slots[pl.ds(g, 1), :], (LANES, rows)))
        lane = lax.broadcasted_iota(jnp.int32, (rows, LANES), 1).astype(F32)
        return jnp.concatenate(
            [(slot == lane + float(b * LANES)).astype(F32).astype(BF16) for b in range(wpad // LANES)],
            1,
        )

    def returned(g):
        return remote(
            result.at[g], ret.at[g, pl.ds(0, cap)], rs.at[g], rr.at[g], g * TOP + x, tp
        )

    third = jnp.where(lo, 3, 0)
    last = jnp.where(lo, 2, 1)

    def add_back(g, fresh):
        chosen = put(g)
        for n in range(width // nb):
            cols = pl.ds(n * nb, nb)
            rows_back = jnp.dot(chosen, ret[g, :, cols], preferred_element_type=F32)
            if fresh:
                moe_ref[:, cols] = rows_back.astype(BF16)
            else:
                moe_ref[:, cols] = (moe_ref[:, cols].astype(F32) + rows_back).astype(BF16)

    add_back(z, True)

    def rest(i, carry):
        g = jnp.where(i == 0, zx, jnp.where(i == 1, third, last))
        returned(g).wait_recv()
        add_back(g, False)
        return carry

    lax.fori_loop(0, 3, rest, 0)

    for step in range(1, GROUPS):
        s = lax.rem(z + step, GROUPS)
        remote(send.at[s], recv.at[s], zs.at[s], zr.at[s], s * TOP + x, tp).wait_send()
        remote(wsend.at[s], wrecv.at[s], us.at[s], ur.at[s], s * TOP + x, tp).wait_send()
        returned(s).wait_send()
    for j in range(pieces):
        hop_x[j].wait_send()
        hop_y[j].wait_send()
        hop_d[j].wait_send()
        hop_e[j].wait_send()
    for copy in gated_copies:
        copy.wait_send()

    @pl.when(ep < last_ep)
    def _():
        halo_copy(0, ep + 1, tp).wait_send()

    out_y.wait_send()
    out_d.wait_send()
    out_e.wait_send()


def one_kernel(
    conv_value, conv_gate, depth_weight, norm_gain, norm_shift, conv_out_weight,
    moe_input, moe_gain, route_experts, route_scores, expert_gate, expert_up, expert_down,
):
    length, chans = conv_value.shape
    peers = lax.axis_size("tp")
    tile = length // peers
    all_chans = chans * peers
    rows, width = moe_input.shape
    ff = expert_gate.shape[2]
    cap = 2 * (3 * TOP * rows // (4 * lax.axis_size("ep")))
    wpad = -(-cap // LANES) * LANES
    vmem = pl.BlockSpec(memory_space=pltpu.VMEM)
    hbm = pl.BlockSpec(memory_space=pltpu.HBM)
    dma = pltpu.SemaphoreType.DMA
    blocks = all_chans // LANES
    return pl.pallas_call(
        functools.partial(fused, cap),
        out_shape=(
            jax.ShapeDtypeStruct((tile, width), BF16),
            jax.ShapeDtypeStruct((rows, width), BF16),
        ),
        in_specs=[hbm] * 13,
        out_specs=(vmem, vmem),
        scratch_shapes=[
            pltpu.VMEM(depth_weight.shape, F32),
            pltpu.VMEM((1, all_chans), F32),
            pltpu.VMEM((1, all_chans), F32),
            pltpu.VMEM((1, width), F32),
            pltpu.VMEM((TOP, rows), jnp.int32),
            pltpu.VMEM((TOP, rows), F32),
            pltpu.VMEM((length, chans), BF16),
            pltpu.VMEM((length, chans), BF16),
            pltpu.VMEM((length + HALO, chans), BF16),
            pltpu.VMEM((tile + HALO, all_chans), BF16),
            pltpu.VMEM((HALO, all_chans), BF16),
            pltpu.VMEM((3, HALO, chans), BF16),
            pltpu.VMEM((blocks, tile + HALO, LANES), F32),
            pltpu.VMEM((blocks, tile, LANES), F32),
            pltpu.VMEM((tile, all_chans), BF16),
            pltpu.VMEM((peers, chans, width), BF16),
            pltpu.VMEM((rows, width), BF16),
            pltpu.VMEM((rows, width), BF16),
            pltpu.VMEM((8, rows), F32),
            pltpu.VMEM((8, rows), BF16),
            pltpu.VMEM((GROUPS, cap, width), BF16),
            pltpu.VMEM((GROUPS, cap, width), BF16),
            pltpu.VMEM((GROUPS, 8, wpad), F32),
            pltpu.VMEM((GROUPS, 8, wpad), F32),
            pltpu.VMEM((width, ff), BF16),
            pltpu.VMEM((width, ff), BF16),
            pltpu.VMEM((ff, width), BF16),
            pltpu.VMEM((width, 2 * ff), BF16),
            pltpu.VMEM((ff, width), BF16),
            pltpu.VMEM((cap, 2 * ff), BF16),
            pltpu.VMEM((GROUPS, cap, width), BF16),
            pltpu.VMEM((GROUPS, wpad, width), BF16),
            dma((15,)),
            dma((GROUPS,)), dma((GROUPS,)),
            dma((GROUPS,)), dma((GROUPS,)),
            dma((GROUPS,)), dma((GROUPS,)),
            dma((6,)), dma((6,)),
            dma((6,)), dma((6,)),
            dma((6,)), dma((6,)),
            dma((6,)), dma((6,)),
            dma((3,)), dma((3,)),
            dma(()), dma((4,)),
            dma((3,)), dma((3,)),
        ],
        compiler_params=pltpu.CompilerParams(
            collective_id=0, has_side_effects=True, vmem_limit_bytes=46 * 1024 * 1024
        ),
        name="fused",
    )(
        *(
            pltpu.with_memory_space_constraint(a, pltpu.HBM)
            for a in (
                conv_value, conv_gate, depth_weight, norm_gain[None, :], norm_shift[None, :],
                conv_out_weight, moe_input, moe_gain[None, :], route_experts.T, route_scores.T,
                expert_gate[0], expert_up[0], expert_down[0],
            )
        )
    )


def on_device(
    conv_value,
    conv_gate,
    depth_weight,
    norm_gain,
    norm_shift,
    conv_out_weight,
    moe_input,
    moe_gain,
    route_experts,
    route_scores,
    expert_gate,
    expert_up,
    expert_down,
):
    conv_args = (conv_value, conv_gate, depth_weight, norm_gain, norm_shift, conv_out_weight)
    moe_args = (
        moe_input, moe_gain, route_experts, route_scores, expert_gate, expert_up, expert_down
    )
    if lax.axis_size("ep") == GROUPS * TOP and lax.axis_size("tp") == 4:
        return one_kernel(*conv_args, *moe_args)
    last = conv_value.shape[0] - depth_weight.shape[0] + 1
    earlier = passed_along(gated_rows(conv_value[last:], conv_gate[last:]), "ep", 1)
    partial = conv_half(conv_value, conv_gate, earlier, *conv_args[2:])
    return (scattered_sum(partial), moe_half(*moe_args))


def solution(mesh):
    in_specs = (
        P("ep", "tp"),
        P("ep", "tp"),
        P(),
        P(),
        P(),
        P("tp", None),
        P(("ep", "tp"), None),
        P(),
        P(("ep", "tp"), None),
        P(("ep", "tp"), None),
        P("ep", None, None),
        P("ep", None, None),
        P("ep", None, None),
    )
    out_specs = (P(("ep", "tp"), None), P(("ep", "tp"), None))
    return jax.shard_map(
        on_device, mesh=mesh, in_specs=in_specs, out_specs=out_specs, check_vma=False
    )
```

```python
import functools

import jax
import jax.numpy as jnp
from jax import lax
from jax.experimental import pallas as pl
from jax.experimental.pallas import tpu as pltpu
from jax.sharding import PartitionSpec as P

GROUPS = 4
TOP = 2
LANES = 128
HALO = 32
MESH = pl.DeviceIdType.MESH
OUTWARD = ((1, 3), (2, 0), (3, 2))
HOMEWARD = ((3, 3), (1, 0), (2, 2))
F32 = jnp.float32
BF16 = jnp.bfloat16


def passed_along(x, axis, by):
    peers = lax.axis_size(axis)
    pairs = [(i, i + by) for i in range(peers) if 0 <= i + by < peers]
    return lax.ppermute(x, axis, pairs)


def gated_rows(value, gate):
    return (value.astype(jnp.float32) * jax.nn.sigmoid(gate.astype(jnp.float32))).astype(
        jnp.bfloat16
    )


def conv_half(conv_value, conv_gate, earlier, depth_weight, norm_gain, norm_shift, conv_out_weight):
    channels = conv_value.shape[1]
    length = conv_value.shape[0]
    first_col = lax.axis_index("tp") * channels
    taps = lax.dynamic_slice_in_dim(depth_weight, first_col, channels, 1)
    gains = lax.dynamic_slice_in_dim(norm_gain, first_col, channels, 0)
    shifts = lax.dynamic_slice_in_dim(norm_shift, first_col, channels, 0)
    reach = taps.shape[0] - 1
    gated = gated_rows(conv_value, conv_gate)
    padded = jnp.concatenate([earlier, gated], 0).astype(jnp.float32)
    filtered = taps[0] * padded[0:length]
    for offset in range(1, reach + 1):
        filtered = filtered + taps[offset] * padded[offset : offset + length]
    sums, squares = lax.psum(
        (jnp.sum(filtered, axis=1), jnp.sum(filtered * filtered, axis=1)), "tp"
    )
    all_channels = channels * lax.axis_size("tp")
    center = (sums / all_channels)[:, None]
    spread = (squares / all_channels)[:, None] - center * center
    normed = (filtered - center) * lax.rsqrt(spread + 1e-05) * gains + shifts
    activated = jax.nn.silu(normed).astype(jnp.bfloat16)
    partial_value = jnp.dot(activated, conv_out_weight, preferred_element_type=jnp.float32)
    return partial_value.astype(jnp.bfloat16)


def swapped(x, axis, mask):
    peers = lax.axis_size(axis)
    return lax.ppermute(x, axis, [(i, i ^ mask) for i in range(peers)])


def scattered_sum(partial):
    peers = lax.axis_size("tp")
    me = lax.axis_index("tp")
    size = partial.shape[0] // peers
    total = lax.dynamic_slice_in_dim(partial, me * size, size, 0).astype(jnp.float32)
    for mask in range(peers - 1, 0, -1):
        block = lax.dynamic_slice_in_dim(partial, (me ^ mask) * size, size, 0)
        total = total + swapped(block, "tp", mask).astype(jnp.float32)
    return total.astype(jnp.bfloat16)


def moe_half(moe_input, moe_gain, route_experts, route_scores, expert_gate, expert_up, expert_down):
    rows = moe_input.shape[0]
    model_width = moe_input.shape[1]
    experts_all = lax.axis_size("ep")
    capacity = 2 * (3 * TOP * rows // (4 * experts_all))
    widened = moe_input.astype(jnp.float32)
    normal_in = (
        widened * lax.rsqrt(jnp.mean(widened * widened, axis=-1, keepdims=True) + 1e-06) * moe_gain
    ).astype(jnp.bfloat16)
    chosen = route_experts.reshape(-1)
    onehot = (chosen[:, None] == jnp.arange(experts_all, dtype=jnp.int32)[None, :]).astype(
        jnp.int32
    )
    slot_rank = jnp.sum(jnp.cumsum(onehot, axis=0) * onehot, axis=-1) - 1
    slot_index = jnp.where(
        slot_rank < capacity, chosen * capacity + slot_rank, experts_all * capacity
    )
    source_row = jnp.arange(rows * TOP, dtype=jnp.int32) // TOP
    slot_token = (
        jnp.full((experts_all * capacity,), rows, jnp.int32)
        .at[slot_index]
        .set(source_row, mode="drop")
    )
    padded_in = jnp.concatenate([normal_in, jnp.zeros((1, model_width), jnp.bfloat16)], 0)
    send_buffer = padded_in[slot_token].reshape(experts_all, capacity, model_width)
    arrived = lax.all_to_all(send_buffer, "ep", split_axis=0, concat_axis=0, tiled=True)
    flat_rows = arrived.reshape(-1, model_width)
    gate_act = jnp.dot(flat_rows, expert_gate[0], preferred_element_type=jnp.float32)
    up_act = jnp.dot(flat_rows, expert_up[0], preferred_element_type=jnp.float32)
    inner = (jax.nn.silu(gate_act) * up_act).astype(jnp.bfloat16)
    result = jnp.dot(inner, expert_down[0], preferred_element_type=jnp.float32).astype(jnp.bfloat16)
    returned = lax.all_to_all(
        result.reshape(arrived.shape), "ep", split_axis=0, concat_axis=0, tiled=True
    )
    returned_flat = jnp.concatenate(
        [
            returned.reshape(experts_all * capacity, model_width),
            jnp.zeros((1, model_width), jnp.bfloat16),
        ],
        0,
    )
    picked = returned_flat[slot_index].reshape(rows, TOP, model_width)
    group_gate = jax.nn.sigmoid(route_scores[:, 0])
    first_weight = (group_gate * jax.nn.sigmoid(route_scores[:, 1]))[:, None]
    second_weight = (group_gate * jax.nn.sigmoid(-route_scores[:, 1]))[:, None]
    combined = first_weight * picked[:, 0].astype(jnp.float32) + second_weight * picked[
        :, 1
    ].astype(jnp.float32)
    return combined.astype(jnp.bfloat16)


def sigmoid(v):
    return 1.0 / (1.0 + jnp.exp(-v))


def fused(
    cap,
    value_hbm,
    gate_hbm,
    taps_hbm,
    gain_hbm,
    shift_hbm,
    wout_hbm,
    moe_hbm,
    mgain_hbm,
    experts_hbm,
    scores_hbm,
    egate_hbm,
    eup_hbm,
    edown_hbm,
    conv_ref,
    moe_ref,
    taps_ref,
    gain_ref,
    shift_ref,
    mgain_ref,
    experts_ref,
    scores_ref,
    value,
    gate,
    gpad,
    gin,
    halo,
    edge,
    wide,
    filt,
    act,
    wout,
    tokens,
    raw,
    slots,
    wpieces,
    send,
    recv,
    wsend,
    wrecv,
    ogate,
    oup,
    odown,
    pgu,
    pdown,
    inner,
    result,
    ret,
    local_sem,
    zs,
    zr,
    us,
    ur,
    rs,
    rr,
    xs,
    xr,
    ys,
    yr,
    ds,
    dr,
    es,
    er,
    gs,
    gr,
    hs,
    hr,
    cs,
    cr,
):
    ep = lax.axis_index("ep")
    tp = lax.axis_index("tp")
    last_ep = lax.axis_size("ep") - 1
    z = ep // TOP
    x = lax.rem(ep, TOP)
    core = lax.rem(tp, 2)
    y = tp // 2
    core_peer = y * 2 + (1 - core)
    y_peer = (1 - y) * 2 + core
    diag = (1 - y) * 2 + (1 - core)
    rows, width = tokens.shape
    length, chans = value.shape
    tile = gin.shape[0] - HALO
    share = pgu.shape[1] // 8
    wpad = wsend.shape[2]

    def at(e, t):
        return {"ep": e, "tp": t}

    def remote(src, dst, ssem, rsem, e, t):
        return pltpu.make_async_remote_copy(
            src_ref=src, dst_ref=dst, send_sem=ssem, recv_sem=rsem,
            device_id=at(e, t), device_id_type=MESH,
        )

    def there(s):
        return remote(send.at[s], recv.at[z], zs.at[s], zr.at[z], s * TOP + x, tp)

    def here_from(s):
        return remote(send.at[s], recv.at[s], zs.at[s], zr.at[s], s * TOP + x, tp)

    def weights_there(s):
        return remote(wsend.at[s], wrecv.at[z], us.at[s], ur.at[z], s * TOP + x, tp)

    def weights_here(s):
        return remote(wsend.at[s], wrecv.at[s], us.at[s], ur.at[s], s * TOP + x, tp)

    def back(s):
        return remote(
            result.at[s], ret.at[z, pl.ds(0, cap)], rs.at[s], rr.at[z], s * TOP + x, tp
        )

    def returned(g):
        return remote(
            result.at[g], ret.at[g, pl.ds(0, cap)], rs.at[g], rr.at[g], g * TOP + x, tp
        )

    small = [
        pltpu.make_async_copy(experts_hbm, experts_ref, local_sem.at[9]),
        pltpu.make_async_copy(scores_hbm, scores_ref, local_sem.at[10]),
        pltpu.make_async_copy(mgain_hbm, mgain_ref, local_sem.at[11]),
        pltpu.make_async_copy(taps_hbm, taps_ref, local_sem.at[12]),
        pltpu.make_async_copy(gain_hbm, gain_ref, local_sem.at[13]),
        pltpu.make_async_copy(shift_hbm, shift_ref, local_sem.at[14]),
    ]
    for load in small[:3]:
        load.start()
    loads = [
        pltpu.make_async_copy(moe_hbm, tokens, local_sem.at[0]),
        pltpu.make_async_copy(value_hbm, value, local_sem.at[1]),
        pltpu.make_async_copy(gate_hbm, gate, local_sem.at[2]),
        pltpu.make_async_copy(egate_hbm, ogate, local_sem.at[3]),
        pltpu.make_async_copy(eup_hbm, oup, local_sem.at[4]),
        pltpu.make_async_copy(edown_hbm, odown, local_sem.at[5]),
        pltpu.make_async_copy(wout_hbm, wout.at[tp], local_sem.at[6]),
        pltpu.make_async_copy(value_hbm.at[pl.ds(length - HALO, HALO)], edge.at[0], local_sem.at[7]),
        pltpu.make_async_copy(gate_hbm.at[pl.ds(length - HALO, HALO)], edge.at[1], local_sem.at[8]),
    ]
    for load in loads[:1] + loads[7:] + loads[1:7] + small[3:]:
        load.start()

    barrier = pltpu.get_barrier_semaphore()

    def greet(e, t):
        pl.semaphore_signal(barrier, inc=1, device_id=at(e, t), device_id_type=MESH)

    for step in range(1, GROUPS):
        greet(lax.rem(z + step, GROUPS) * TOP + x, tp)
    greet(z * TOP + 1 - x, tp)
    greet(ep, core_peer)
    greet(ep, y_peer)
    greet(ep, diag)

    @pl.when(ep < last_ep)
    def _():
        greet(ep + 1, 0)

    first_tp = jnp.logical_and(ep > 0, tp == 0)

    @pl.when(first_tp)
    def _():
        for t in range(4):
            greet(ep - 1, t)

    expected = (
        GROUPS + 3
        + jnp.where(ep < last_ep, 1, 0)
        + jnp.where(first_tp, 4, 0)
    )

    depth = width // 2
    half = share // 2

    def piece(j, q, gates, ups, downs, wide_cols):
        c = j % 2
        kind = j // 2
        if kind == 2:
            return downs.at[pl.ds(pl.multiple_of(q * share + c * half, half), half), :]
        span = pl.ds(c * depth, depth)
        ref = gates if kind == 0 else ups
        if wide_cols:
            col = pl.multiple_of(q * (2 * share) + kind * share, share)
        else:
            col = pl.multiple_of(q * share, share)
        return ref.at[span, pl.ds(col, share)]

    def held(j, q):
        return piece(j, q, pgu, pgu, pdown, True)

    pieces = 6
    hop_x = [
        remote(
            piece(j, tp, egate_hbm, eup_hbm, edown_hbm, False),
            held(j, tp), xs.at[j], xr.at[j], z * TOP + 1 - x, tp,
        )
        for j in range(pieces)
    ]
    hop_y = [remote(held(j, tp), held(j, tp), ys.at[j], yr.at[j], ep, y_peer) for j in range(pieces)]
    hop_d = [remote(held(j, tp), held(j, tp), ds.at[j], dr.at[j], ep, core_peer) for j in range(pieces)]
    hop_e = [
        remote(held(j, y_peer), held(j, y_peer), es.at[j], er.at[j], ep, core_peer)
        for j in range(pieces)
    ]

    small[0].wait()
    small[1].wait()
    small[2].wait()
    first = jnp.broadcast_to(experts_ref[0:1, :], (8, rows))
    group_id = lax.broadcasted_iota(jnp.int32, (8, rows), 0)
    member = jnp.logical_and(first >= group_id * TOP, first < (group_id + 1) * TOP)
    before = (
        lax.broadcasted_iota(jnp.int32, (rows, rows), 0)
        < lax.broadcasted_iota(jnp.int32, (rows, rows), 1)
    ).astype(F32).astype(BF16)
    rank = jnp.dot(member.astype(F32).astype(BF16), before, preferred_element_type=F32)
    keep = jnp.logical_and(member, rank < cap)
    slots[...] = jnp.where(keep, rank, -1.0)
    group_gate = sigmoid(scores_ref[0:1, :])
    first_weight = group_gate * sigmoid(scores_ref[1:2, :])
    second_weight = group_gate * sigmoid(-scores_ref[1:2, :])
    in_order = experts_ref[0:1, :] < experts_ref[1:2, :]
    low = jnp.where(in_order, first_weight, second_weight)
    high = jnp.where(in_order, second_weight, first_weight)
    parts = []
    for weight in (low, high):
        for _ in range(3):
            rounded = weight.astype(BF16).astype(F32)
            parts.append(rounded)
            weight = weight - rounded
    nothing = jnp.zeros((2, rows), F32)
    wpieces[...] = jnp.concatenate(parts + [nothing], 0).astype(BF16)

    strip = 32

    def halo_copy(t, e, c):
        cols = pl.ds(pl.multiple_of(c * chans, LANES), chans)
        return remote(edge.at[2], halo.at[:, cols], hs, hr.at[c], e, t)

    loads[7].wait()
    loads[8].wait()
    edge[2] = (edge[0].astype(F32) * sigmoid(edge[1].astype(F32))).astype(BF16)
    zx = z + 1 - 2 * lax.rem(z, 2)
    lo = z < 2
    outer = jnp.logical_or(z == 0, z == 3)
    across = jnp.where(lo, 2, 1)
    far = jnp.where(lo, 3, 0)

    def turn(k, table):
        out = z
        for place, (edge_peer, inner_peer) in enumerate(table):
            for spot in range(GROUPS):
                peer = (edge_peer, inner_peer, 3 - inner_peer, 3 - edge_peer)[spot]
                out = jnp.where(jnp.logical_and(k == place, z == spot), peer, out)
        return out

    block = 512

    def fill(d):
        slot = slots[pl.ds(d, 1), :]
        pick = (
            lax.broadcasted_iota(jnp.int32, (wpad, rows), 0).astype(F32)
            == jnp.broadcast_to(slot, (wpad, rows))
        ).astype(F32).astype(BF16)
        squares = jnp.zeros((cap, 1), F32)
        for n in range(width // block):
            cols = pl.ds(n * block, block)
            chosen = jnp.dot(pick[:cap], tokens[:, cols], preferred_element_type=F32)
            raw[:, cols] = chosen
            squares = squares + jnp.sum(chosen * chosen, axis=1, keepdims=True)
        weights = lax.dot_general(
            wpieces[...], pick, (((1,), (1,)), ((), ())), preferred_element_type=F32
        )
        wsend[d, 0:1, :] = weights[0:1] + weights[1:2] + weights[2:3]
        wsend[d, 1:2, :] = weights[3:4] + weights[4:5] + weights[5:6]
        scale = lax.rsqrt(squares * (1.0 / width) + 1e-06)
        for n in range(width // block):
            cols = pl.ds(n * block, block)
            send[d, :, cols] = (raw[:, cols] * scale * mgain_ref[:, cols]).astype(BF16)

    loads[0].wait()
    start = turn(0, OUTWARD)
    fill(start)
    pl.semaphore_wait(barrier, expected)

    @pl.when(ep < last_ep)
    def _():
        halo_copy(0, ep + 1, tp).start()

    there(start).start()
    weights_there(start).start()
    for hop in hop_x:
        hop.start()

    def dispatch(k, carry):
        d = turn(k, OUTWARD)
        fill(d)

        @pl.when(k < 3)
        def _():
            there(d).start()
            weights_there(d).start()

        return carry

    lax.fori_loop(1, 4, dispatch, 0)
    recv[z] = send[z]
    wrecv[z] = wsend[z]

    loads[1].wait()
    loads[2].wait()
    gpad[0:HALO, :] = jnp.zeros((HALO, chans), BF16)
    gstrip = 64

    def gate_rows(i, carry):
        span = pl.ds(pl.multiple_of(i * gstrip, gstrip), gstrip)
        out = pl.ds(pl.multiple_of(i * gstrip + HALO, HALO), gstrip)
        gpad[out, :] = (value[span, :].astype(F32) * sigmoid(gate[span, :].astype(F32))).astype(BF16)
        return carry

    lax.fori_loop(0, length // gstrip, gate_rows, 0)
    my_cols = pl.ds(pl.multiple_of(tp * chans, LANES), chans)

    def window(t):
        return pl.ds(pl.multiple_of(t * tile, HALO), tile + HALO)

    gated_copies = [
        remote(gpad.at[window(t)], gin.at[:, my_cols], gs.at[i], gr.at[i], ep, t)
        for i, t in enumerate((core_peer, y_peer, diag))
    ]
    for copy in gated_copies:
        copy.start()

    gin[:, my_cols] = gpad[window(tp), :]

    for g in range(GROUPS):
        ret[g, cap:, :] = jnp.zeros((ret.shape[1] - cap, width), BF16)

    own_wout = wout.at[tp]
    out_y = remote(own_wout, own_wout, cs.at[0], cr.at[0], ep, y_peer)
    out_d = remote(own_wout, own_wout, cs.at[1], cr.at[1], ep, core_peer)
    out_e = remote(wout.at[y_peer], wout.at[y_peer], cs.at[2], cr.at[2], ep, core_peer)

    taps_count = taps_ref.shape[0]
    lane_blocks = gin.shape[1] // LANES
    frows = 64

    def widen():
        for copy in gated_copies:
            copy.wait_recv()

        @pl.when(first_tp)
        def _():
            for c in range(4):
                halo_copy(0, ep, c).wait_recv()
            gin[0:HALO, :] = halo[...]

        for b in range(lane_blocks):
            wide[b] = gin[:, b * LANES : (b + 1) * LANES].astype(F32)

    def filter_block(b, carry):
        for r in range(tile // frows):
            total = jnp.zeros((frows, LANES), F32)
            for k in range(taps_count):
                start = r * frows + HALO - taps_count + 1 + k
                tap = taps_ref[pl.ds(k, 1), pl.ds(pl.multiple_of(b * LANES, LANES), LANES)]
                total = total + tap * wide[b, pl.ds(start, frows), :]
            filt[b, pl.ds(r * frows, frows), :] = total
        return carry

    def activate(i, carry):
        span = pl.ds(pl.multiple_of(i * strip, strip), strip)
        total = filt[0, span, :]
        squares = total * total
        for b in range(1, lane_blocks):
            part = filt[b, span, :]
            total = total + part
            squares = squares + part * part
        count = 1.0 / (lane_blocks * LANES)
        center = jnp.sum(total, axis=1, keepdims=True) * count
        spread = jnp.sum(squares, axis=1, keepdims=True) * count - center * center
        scale = lax.rsqrt(spread + 1e-05)
        for b in range(lane_blocks):
            cols = slice(b * LANES, (b + 1) * LANES)
            normed = (filt[b, span, :] - center) * scale * gain_ref[:, cols] + shift_ref[:, cols]
            act[span, cols] = (normed * sigmoid(normed)).astype(BF16)
        return carry

    for j in range(pieces):
        hop_x[j].wait_recv()
        hop_y[j].start()
        hop_d[j].start()
        if j > 0:
            hop_y[j - 1].wait_recv()
            hop_e[j - 1].start()
        if j == 1:
            for load in small[3:]:
                load.wait()
            widen()
            lax.fori_loop(0, 2, filter_block, 0)
        if 2 <= j < 5:
            lax.fori_loop(2 * j - 2, 2 * j, filter_block, 0)
        if j == 5:
            lax.fori_loop(0, tile // strip, activate, 0)
    loads[6].wait()
    out_y.start()
    out_d.start()
    hop_y[pieces - 1].wait_recv()
    hop_e[pieces - 1].start()
    for load in loads[3:6]:
        load.wait()
    for j in range(pieces):
        hop_d[j].wait_recv()
        hop_e[j].wait_recv()

    ff = ogate.shape[1]
    even = x == 0
    nb = 256

    def expert(i, carry):
        s = turn(i, HOMEWARD)

        @pl.when(i < 3)
        def _():
            here_from(s).wait_recv()
            weights_here(s).wait_recv()

        w8 = wrecv[s]
        w_low = w8[0:1]
        w_high = w8[1:2]
        mine = jnp.where(even, w_low, w_high)
        theirs = jnp.where(even, w_high, w_low)
        mine = jnp.transpose(jnp.broadcast_to(mine, (LANES, wpad)))[:cap]
        theirs = jnp.transpose(jnp.broadcast_to(theirs, (LANES, wpad)))[:cap]
        mine2 = jnp.concatenate([mine] * (nb // LANES), 1)
        theirs1 = jnp.concatenate([theirs] * (share // LANES), 1)
        here = recv[s]
        for n in range(ff // nb):
            cols = pl.ds(n * nb, nb)
            g = jnp.dot(here, ogate[:, cols], preferred_element_type=F32)
            u = jnp.dot(here, oup[:, cols], preferred_element_type=F32)
            inner[:, cols] = (g * sigmoid(g) * u * mine2).astype(BF16)
        for q in range(4):
            gu = jnp.dot(
                here, pgu[:, pl.ds(q * 2 * share, 2 * share)], preferred_element_type=F32
            )
            g = gu[:, :share]
            u = gu[:, share:]
            inner[:, pl.ds(ff + q * share, share)] = (g * sigmoid(g) * u * theirs1).astype(BF16)
        for n in range(width // nb):
            cols = pl.ds(n * nb, nb)
            total = jnp.dot(inner[:, :ff], odown[:, cols], preferred_element_type=F32) + jnp.dot(
                inner[:, ff:], pdown[:, cols], preferred_element_type=F32
            )
            result[s, :, cols] = total.astype(BF16)

        @pl.when(i < 3)
        def _():
            back(s).start()

        return carry

    lax.fori_loop(0, 4, expert, 0)
    ret[z, pl.ds(0, cap), :] = result[z]

    out_y.wait_recv()
    out_e.start()
    out_d.wait_recv()
    out_e.wait_recv()

    def project(n, carry):
        cols = pl.ds(pl.multiple_of(n * nb, nb), nb)
        total = jnp.dot(act[:, 0:chans], wout[0, :, cols], preferred_element_type=F32)
        for t in range(1, 4):
            total = total + jnp.dot(
                act[:, t * chans : (t + 1) * chans], wout[t, :, cols], preferred_element_type=F32
            )
        conv_ref[:, cols] = total.astype(BF16)
        return carry

    lax.fori_loop(0, width // nb, project, 0)

    def put(g):
        slot = jnp.transpose(jnp.broadcast_to(slots[pl.ds(g, 1), :], (LANES, rows)))
        lane = lax.broadcasted_iota(jnp.int32, (rows, LANES), 1).astype(F32)
        return jnp.concatenate(
            [(slot == lane + float(b * LANES)).astype(F32).astype(BF16) for b in range(wpad // LANES)],
            1,
        )

    def add_back(g, fresh):
        chosen = put(g)
        for n in range(width // nb):
            cols = pl.ds(n * nb, nb)
            rows_back = jnp.dot(chosen, ret[g, :, cols], preferred_element_type=F32)
            if fresh:
                moe_ref[:, cols] = rows_back.astype(BF16)
            else:
                moe_ref[:, cols] = (moe_ref[:, cols].astype(F32) + rows_back).astype(BF16)

    add_back(z, True)

    def rest(i, carry):
        g = jnp.where(
            i == 0, zx, jnp.where(jnp.logical_xor(outer, i == 1), far, across)
        )
        returned(g).wait_recv()
        add_back(g, False)
        return carry

    lax.fori_loop(0, 3, rest, 0)

    for step in range(1, GROUPS):
        s = lax.rem(z + step, GROUPS)
        there(s).wait_send()
        weights_there(s).wait_send()
        back(s).wait_send()
    for j in range(pieces):
        hop_x[j].wait_send()
        hop_y[j].wait_send()
        hop_d[j].wait_send()
        hop_e[j].wait_send()
    for copy in gated_copies:
        copy.wait_send()

    @pl.when(ep < last_ep)
    def _():
        halo_copy(0, ep + 1, tp).wait_send()

    out_y.wait_send()
    out_d.wait_send()
    out_e.wait_send()


def one_kernel(
    conv_value, conv_gate, depth_weight, norm_gain, norm_shift, conv_out_weight,
    moe_input, moe_gain, route_experts, route_scores, expert_gate, expert_up, expert_down,
):
    length, chans = conv_value.shape
    peers = lax.axis_size("tp")
    tile = length // peers
    all_chans = chans * peers
    rows, width = moe_input.shape
    ff = expert_gate.shape[2]
    cap = 2 * (3 * TOP * rows // (4 * lax.axis_size("ep")))
    wpad = -(-cap // LANES) * LANES
    vmem = pl.BlockSpec(memory_space=pltpu.VMEM)
    hbm = pl.BlockSpec(memory_space=pltpu.HBM)
    dma = pltpu.SemaphoreType.DMA
    blocks = all_chans // LANES
    return pl.pallas_call(
        functools.partial(fused, cap),
        out_shape=(
            jax.ShapeDtypeStruct((tile, width), BF16),
            jax.ShapeDtypeStruct((rows, width), BF16),
        ),
        in_specs=[hbm] * 13,
        out_specs=(vmem, vmem),
        scratch_shapes=[
            pltpu.VMEM(depth_weight.shape, F32),
            pltpu.VMEM((1, all_chans), F32),
            pltpu.VMEM((1, all_chans), F32),
            pltpu.VMEM((1, width), F32),
            pltpu.VMEM((TOP, rows), jnp.int32),
            pltpu.VMEM((TOP, rows), F32),
            pltpu.VMEM((length, chans), BF16),
            pltpu.VMEM((length, chans), BF16),
            pltpu.VMEM((length + HALO, chans), BF16),
            pltpu.VMEM((tile + HALO, all_chans), BF16),
            pltpu.VMEM((HALO, all_chans), BF16),
            pltpu.VMEM((3, HALO, chans), BF16),
            pltpu.VMEM((blocks, tile + HALO, LANES), F32),
            pltpu.VMEM((blocks, tile, LANES), F32),
            pltpu.VMEM((tile, all_chans), BF16),
            pltpu.VMEM((peers, chans, width), BF16),
            pltpu.VMEM((rows, width), BF16),
            pltpu.VMEM((cap, width), F32),
            pltpu.VMEM((8, rows), F32),
            pltpu.VMEM((8, rows), BF16),
            pltpu.VMEM((GROUPS, cap, width), BF16),
            pltpu.VMEM((GROUPS, cap, width), BF16),
            pltpu.VMEM((GROUPS, TOP, wpad), F32),
            pltpu.VMEM((GROUPS, TOP, wpad), F32),
            pltpu.VMEM((width, ff), BF16),
            pltpu.VMEM((width, ff), BF16),
            pltpu.VMEM((ff, width), BF16),
            pltpu.VMEM((width, 2 * ff), BF16),
            pltpu.VMEM((ff, width), BF16),
            pltpu.VMEM((cap, 2 * ff), BF16),
            pltpu.VMEM((GROUPS, cap, width), BF16),
            pltpu.VMEM((GROUPS, wpad, width), BF16),
            dma((15,)),
            dma((GROUPS,)), dma((GROUPS,)),
            dma((GROUPS,)), dma((GROUPS,)),
            dma((GROUPS,)), dma((GROUPS,)),
            dma((6,)), dma((6,)),
            dma((6,)), dma((6,)),
            dma((6,)), dma((6,)),
            dma((6,)), dma((6,)),
            dma((3,)), dma((3,)),
            dma(()), dma((4,)),
            dma((3,)), dma((3,)),
        ],
        compiler_params=pltpu.CompilerParams(
            collective_id=0, has_side_effects=True, vmem_limit_bytes=46 * 1024 * 1024
        ),
        name="fused",
    )(
        *(
            pltpu.with_memory_space_constraint(a, pltpu.HBM)
            for a in (
                conv_value, conv_gate, depth_weight, norm_gain[None, :], norm_shift[None, :],
                conv_out_weight, moe_input, moe_gain[None, :], route_experts.T, route_scores.T,
                expert_gate[0], expert_up[0], expert_down[0],
            )
        )
    )


def on_device(
    conv_value,
    conv_gate,
    depth_weight,
    norm_gain,
    norm_shift,
    conv_out_weight,
    moe_input,
    moe_gain,
    route_experts,
    route_scores,
    expert_gate,
    expert_up,
    expert_down,
):
    conv_args = (conv_value, conv_gate, depth_weight, norm_gain, norm_shift, conv_out_weight)
    moe_args = (
        moe_input, moe_gain, route_experts, route_scores, expert_gate, expert_up, expert_down
    )
    if lax.axis_size("ep") == GROUPS * TOP and lax.axis_size("tp") == 4:
        return one_kernel(*conv_args, *moe_args)
    last = conv_value.shape[0] - depth_weight.shape[0] + 1
    earlier = passed_along(gated_rows(conv_value[last:], conv_gate[last:]), "ep", 1)
    partial = conv_half(conv_value, conv_gate, earlier, *conv_args[2:])
    return (scattered_sum(partial), moe_half(*moe_args))


def solution(mesh):
    in_specs = (
        P("ep", "tp"),
        P("ep", "tp"),
        P(),
        P(),
        P(),
        P("tp", None),
        P(("ep", "tp"), None),
        P(),
        P(("ep", "tp"), None),
        P(("ep", "tp"), None),
        P("ep", None, None),
        P("ep", None, None),
        P("ep", None, None),
    )
    out_specs = (P(("ep", "tp"), None), P(("ep", "tp"), None))
    return jax.shard_map(
        on_device, mesh=mesh, in_specs=in_specs, out_specs=out_specs, check_vma=False
    )
```

```python
import functools

import jax
import jax.numpy as jnp
from jax import lax
from jax.experimental import pallas as pl
from jax.experimental.pallas import tpu as pltpu
from jax.sharding import PartitionSpec as P

GROUPS = 4
TOP = 2
LANES = 128
HALO = 32
MESH = pl.DeviceIdType.MESH
OUTWARD = ((1, 3), (2, 0), (3, 2))
HOMEWARD = ((3, 3), (1, 0), (2, 2))
F32 = jnp.float32
BF16 = jnp.bfloat16


def passed_along(x, axis, by):
    peers = lax.axis_size(axis)
    pairs = [(i, i + by) for i in range(peers) if 0 <= i + by < peers]
    return lax.ppermute(x, axis, pairs)


def gated_rows(value, gate):
    return (value.astype(jnp.float32) * jax.nn.sigmoid(gate.astype(jnp.float32))).astype(
        jnp.bfloat16
    )


def conv_half(conv_value, conv_gate, earlier, depth_weight, norm_gain, norm_shift, conv_out_weight):
    channels = conv_value.shape[1]
    length = conv_value.shape[0]
    first_col = lax.axis_index("tp") * channels
    taps = lax.dynamic_slice_in_dim(depth_weight, first_col, channels, 1)
    gains = lax.dynamic_slice_in_dim(norm_gain, first_col, channels, 0)
    shifts = lax.dynamic_slice_in_dim(norm_shift, first_col, channels, 0)
    reach = taps.shape[0] - 1
    gated = gated_rows(conv_value, conv_gate)
    padded = jnp.concatenate([earlier, gated], 0).astype(jnp.float32)
    filtered = taps[0] * padded[0:length]
    for offset in range(1, reach + 1):
        filtered = filtered + taps[offset] * padded[offset : offset + length]
    sums, squares = lax.psum(
        (jnp.sum(filtered, axis=1), jnp.sum(filtered * filtered, axis=1)), "tp"
    )
    all_channels = channels * lax.axis_size("tp")
    center = (sums / all_channels)[:, None]
    spread = (squares / all_channels)[:, None] - center * center
    normed = (filtered - center) * lax.rsqrt(spread + 1e-05) * gains + shifts
    activated = jax.nn.silu(normed).astype(jnp.bfloat16)
    partial_value = jnp.dot(activated, conv_out_weight, preferred_element_type=jnp.float32)
    return partial_value.astype(jnp.bfloat16)


def swapped(x, axis, mask):
    peers = lax.axis_size(axis)
    return lax.ppermute(x, axis, [(i, i ^ mask) for i in range(peers)])


def scattered_sum(partial):
    peers = lax.axis_size("tp")
    me = lax.axis_index("tp")
    size = partial.shape[0] // peers
    total = lax.dynamic_slice_in_dim(partial, me * size, size, 0).astype(jnp.float32)
    for mask in range(peers - 1, 0, -1):
        block = lax.dynamic_slice_in_dim(partial, (me ^ mask) * size, size, 0)
        total = total + swapped(block, "tp", mask).astype(jnp.float32)
    return total.astype(jnp.bfloat16)


def moe_half(moe_input, moe_gain, route_experts, route_scores, expert_gate, expert_up, expert_down):
    rows = moe_input.shape[0]
    model_width = moe_input.shape[1]
    experts_all = lax.axis_size("ep")
    capacity = 2 * (3 * TOP * rows // (4 * experts_all))
    widened = moe_input.astype(jnp.float32)
    normal_in = (
        widened * lax.rsqrt(jnp.mean(widened * widened, axis=-1, keepdims=True) + 1e-06) * moe_gain
    ).astype(jnp.bfloat16)
    chosen = route_experts.reshape(-1)
    onehot = (chosen[:, None] == jnp.arange(experts_all, dtype=jnp.int32)[None, :]).astype(
        jnp.int32
    )
    slot_rank = jnp.sum(jnp.cumsum(onehot, axis=0) * onehot, axis=-1) - 1
    slot_index = jnp.where(
        slot_rank < capacity, chosen * capacity + slot_rank, experts_all * capacity
    )
    source_row = jnp.arange(rows * TOP, dtype=jnp.int32) // TOP
    slot_token = (
        jnp.full((experts_all * capacity,), rows, jnp.int32)
        .at[slot_index]
        .set(source_row, mode="drop")
    )
    padded_in = jnp.concatenate([normal_in, jnp.zeros((1, model_width), jnp.bfloat16)], 0)
    send_buffer = padded_in[slot_token].reshape(experts_all, capacity, model_width)
    arrived = lax.all_to_all(send_buffer, "ep", split_axis=0, concat_axis=0, tiled=True)
    flat_rows = arrived.reshape(-1, model_width)
    gate_act = jnp.dot(flat_rows, expert_gate[0], preferred_element_type=jnp.float32)
    up_act = jnp.dot(flat_rows, expert_up[0], preferred_element_type=jnp.float32)
    inner = (jax.nn.silu(gate_act) * up_act).astype(jnp.bfloat16)
    result = jnp.dot(inner, expert_down[0], preferred_element_type=jnp.float32).astype(jnp.bfloat16)
    returned = lax.all_to_all(
        result.reshape(arrived.shape), "ep", split_axis=0, concat_axis=0, tiled=True
    )
    returned_flat = jnp.concatenate(
        [
            returned.reshape(experts_all * capacity, model_width),
            jnp.zeros((1, model_width), jnp.bfloat16),
        ],
        0,
    )
    picked = returned_flat[slot_index].reshape(rows, TOP, model_width)
    group_gate = jax.nn.sigmoid(route_scores[:, 0])
    first_weight = (group_gate * jax.nn.sigmoid(route_scores[:, 1]))[:, None]
    second_weight = (group_gate * jax.nn.sigmoid(-route_scores[:, 1]))[:, None]
    combined = first_weight * picked[:, 0].astype(jnp.float32) + second_weight * picked[
        :, 1
    ].astype(jnp.float32)
    return combined.astype(jnp.bfloat16)


def sigmoid(v):
    return 1.0 / (1.0 + jnp.exp(-v))


def fused(
    cap,
    value_hbm,
    gate_hbm,
    taps_hbm,
    gain_hbm,
    shift_hbm,
    wout_hbm,
    moe_hbm,
    mgain_hbm,
    experts_hbm,
    scores_hbm,
    egate_hbm,
    eup_hbm,
    edown_hbm,
    conv_ref,
    moe_ref,
    taps_ref,
    gain_ref,
    shift_ref,
    mgain_ref,
    experts_ref,
    scores_ref,
    value,
    gate,
    gpad,
    gin,
    halo,
    edge,
    wide,
    filt,
    act,
    wout,
    tokens,
    raw,
    slots,
    wpieces,
    send,
    recv,
    wsend,
    wrecv,
    ogate,
    oup,
    odown,
    pgu,
    pdown,
    inner,
    result,
    ret,
    local_sem,
    zs,
    zr,
    us,
    ur,
    rs,
    rr,
    xs,
    xr,
    ys,
    yr,
    ds,
    dr,
    es,
    er,
    gs,
    gr,
    hs,
    hr,
    cs,
    cr,
):
    ep = lax.axis_index("ep")
    tp = lax.axis_index("tp")
    last_ep = lax.axis_size("ep") - 1
    z = ep // TOP
    x = lax.rem(ep, TOP)
    core = lax.rem(tp, 2)
    y = tp // 2
    core_peer = y * 2 + (1 - core)
    y_peer = (1 - y) * 2 + core
    diag = (1 - y) * 2 + (1 - core)
    rows, width = tokens.shape
    length, chans = value.shape
    tile = gin.shape[0] - HALO
    share = pgu.shape[1] // 8
    wpad = wsend.shape[2]

    def at(e, t):
        return {"ep": e, "tp": t}

    def remote(src, dst, ssem, rsem, e, t):
        return pltpu.make_async_remote_copy(
            src_ref=src, dst_ref=dst, send_sem=ssem, recv_sem=rsem,
            device_id=at(e, t), device_id_type=MESH,
        )

    def there(s):
        return remote(send.at[s], recv.at[z], zs, zr.at[z], s * TOP + x, tp)

    def here_from(s):
        return remote(send.at[s], recv.at[s], zs, zr.at[s], s * TOP + x, tp)

    def weights_there(s):
        return remote(wsend.at[s], wrecv.at[z], us, ur.at[z], s * TOP + x, tp)

    def weights_here(s):
        return remote(wsend.at[s], wrecv.at[s], us, ur.at[s], s * TOP + x, tp)

    def back(s):
        return remote(
            result.at[s], ret.at[z, pl.ds(0, cap)], rs, rr.at[z], s * TOP + x, tp
        )

    def returned(g):
        return remote(
            result.at[g], ret.at[g, pl.ds(0, cap)], rs, rr.at[g], g * TOP + x, tp
        )

    small = [
        pltpu.make_async_copy(experts_hbm, experts_ref, local_sem.at[9]),
        pltpu.make_async_copy(scores_hbm, scores_ref, local_sem.at[10]),
        pltpu.make_async_copy(mgain_hbm, mgain_ref, local_sem.at[11]),
        pltpu.make_async_copy(taps_hbm, taps_ref, local_sem.at[12]),
        pltpu.make_async_copy(gain_hbm, gain_ref, local_sem.at[13]),
        pltpu.make_async_copy(shift_hbm, shift_ref, local_sem.at[14]),
    ]
    for load in small[:3]:
        load.start()
    loads = [
        pltpu.make_async_copy(moe_hbm, tokens, local_sem.at[0]),
        pltpu.make_async_copy(value_hbm, value, local_sem.at[1]),
        pltpu.make_async_copy(gate_hbm, gate, local_sem.at[2]),
        pltpu.make_async_copy(egate_hbm, ogate, local_sem.at[3]),
        pltpu.make_async_copy(eup_hbm, oup, local_sem.at[4]),
        pltpu.make_async_copy(edown_hbm, odown, local_sem.at[5]),
        pltpu.make_async_copy(wout_hbm, wout.at[tp], local_sem.at[6]),
        pltpu.make_async_copy(value_hbm.at[pl.ds(length - HALO, HALO)], edge.at[0], local_sem.at[7]),
        pltpu.make_async_copy(gate_hbm.at[pl.ds(length - HALO, HALO)], edge.at[1], local_sem.at[8]),
    ]
    for load in loads[:1] + loads[7:] + loads[1:7] + small[3:]:
        load.start()

    barrier = pltpu.get_barrier_semaphore()

    def greet(e, t):
        pl.semaphore_signal(barrier, inc=1, device_id=at(e, t), device_id_type=MESH)

    for step in range(1, GROUPS):
        greet(lax.rem(z + step, GROUPS) * TOP + x, tp)
    greet(z * TOP + 1 - x, tp)
    greet(ep, core_peer)
    greet(ep, y_peer)
    greet(ep, diag)

    @pl.when(ep < last_ep)
    def _():
        greet(ep + 1, 0)

    first_tp = jnp.logical_and(ep > 0, tp == 0)

    @pl.when(first_tp)
    def _():
        for t in range(4):
            greet(ep - 1, t)

    expected = (
        GROUPS + 3
        + jnp.where(ep < last_ep, 1, 0)
        + jnp.where(first_tp, 4, 0)
    )

    depth = width // 2
    half = share // 2

    def piece(j, q, gates, ups, downs, wide_cols):
        c = j % 2
        kind = j // 2
        if kind == 2:
            return downs.at[pl.ds(pl.multiple_of(q * share + c * half, half), half), :]
        span = pl.ds(c * depth, depth)
        ref = gates if kind == 0 else ups
        if wide_cols:
            col = pl.multiple_of(q * (2 * share) + kind * share, share)
        else:
            col = pl.multiple_of(q * share, share)
        return ref.at[span, pl.ds(col, share)]

    def held(j, q):
        return piece(j, q, pgu, pgu, pdown, True)

    pieces = 6
    hop_x = [
        remote(
            piece(j, tp, egate_hbm, eup_hbm, edown_hbm, False),
            held(j, tp), xs, xr.at[j], z * TOP + 1 - x, tp,
        )
        for j in range(pieces)
    ]
    hop_y = [remote(held(j, tp), held(j, tp), ys, yr.at[j], ep, y_peer) for j in range(pieces)]
    hop_d = [remote(held(j, tp), held(j, tp), ds, dr, ep, core_peer) for j in range(pieces)]
    hop_e = [
        remote(held(j, y_peer), held(j, y_peer), es, er, ep, core_peer)
        for j in range(pieces)
    ]
    quarter = pdown.at[pl.ds(0, 3 * share)]
    whole_d = remote(quarter, quarter, ds, dr, ep, core_peer)
    whole_e = remote(quarter, quarter, es, er, ep, core_peer)

    small[0].wait()
    small[1].wait()
    small[2].wait()
    first = jnp.broadcast_to(experts_ref[0:1, :], (8, rows))
    group_id = lax.broadcasted_iota(jnp.int32, (8, rows), 0)
    member = jnp.logical_and(first >= group_id * TOP, first < (group_id + 1) * TOP)
    before = (
        lax.broadcasted_iota(jnp.int32, (rows, rows), 0)
        < lax.broadcasted_iota(jnp.int32, (rows, rows), 1)
    ).astype(F32).astype(BF16)
    rank = jnp.dot(member.astype(F32).astype(BF16), before, preferred_element_type=F32)
    keep = jnp.logical_and(member, rank < cap)
    slots[...] = jnp.where(keep, rank, -1.0)
    group_gate = sigmoid(scores_ref[0:1, :])
    first_weight = group_gate * sigmoid(scores_ref[1:2, :])
    second_weight = group_gate * sigmoid(-scores_ref[1:2, :])
    in_order = experts_ref[0:1, :] < experts_ref[1:2, :]
    low = jnp.where(in_order, first_weight, second_weight)
    high = jnp.where(in_order, second_weight, first_weight)
    parts = []
    for weight in (low, high):
        for _ in range(3):
            rounded = weight.astype(BF16).astype(F32)
            parts.append(rounded)
            weight = weight - rounded
    nothing = jnp.zeros((2, rows), F32)
    wpieces[...] = jnp.concatenate(parts + [nothing], 0).astype(BF16)

    strip = 32

    def halo_copy(t, e, c):
        cols = pl.ds(pl.multiple_of(c * chans, LANES), chans)
        return remote(edge.at[2], halo.at[:, cols], hs, hr, e, t)

    loads[7].wait()
    loads[8].wait()
    edge[2] = (edge[0].astype(F32) * sigmoid(edge[1].astype(F32))).astype(BF16)
    zx = z + 1 - 2 * lax.rem(z, 2)
    lo = z < 2
    outer = jnp.logical_or(z == 0, z == 3)
    across = jnp.where(lo, 2, 1)
    far = jnp.where(lo, 3, 0)

    def turn(k, table):
        out = z
        for place, (edge_peer, inner_peer) in enumerate(table):
            for spot in range(GROUPS):
                peer = (edge_peer, inner_peer, 3 - inner_peer, 3 - edge_peer)[spot]
                out = jnp.where(jnp.logical_and(k == place, z == spot), peer, out)
        return out

    block = 512

    def fill(d):
        slot = slots[pl.ds(d, 1), :]
        pick = (
            lax.broadcasted_iota(jnp.int32, (wpad, rows), 0).astype(F32)
            == jnp.broadcast_to(slot, (wpad, rows))
        ).astype(F32).astype(BF16)
        squares = jnp.zeros((cap, 1), F32)
        for n in range(width // block):
            cols = pl.ds(n * block, block)
            chosen = jnp.dot(pick[:cap], tokens[:, cols], preferred_element_type=F32)
            raw[:, cols] = chosen
            squares = squares + jnp.sum(chosen * chosen, axis=1, keepdims=True)
        weights = lax.dot_general(
            wpieces[...], pick, (((1,), (1,)), ((), ())), preferred_element_type=F32
        )
        wsend[d, 0:1, :] = weights[0:1] + weights[1:2] + weights[2:3]
        wsend[d, 1:2, :] = weights[3:4] + weights[4:5] + weights[5:6]
        scale = lax.rsqrt(squares * (1.0 / width) + 1e-06)
        for n in range(width // block):
            cols = pl.ds(n * block, block)
            send[d, :, cols] = (raw[:, cols] * scale * mgain_ref[:, cols]).astype(BF16)

    loads[0].wait()
    start = turn(0, OUTWARD)
    fill(start)
    pl.semaphore_wait(barrier, expected)

    @pl.when(ep < last_ep)
    def _():
        halo_copy(0, ep + 1, tp).start()

    there(start).start()
    weights_there(start).start()
    for hop in hop_x:
        hop.start()

    def dispatch(k, carry):
        d = turn(k, OUTWARD)
        fill(d)

        @pl.when(k < 3)
        def _():
            there(d).start()
            weights_there(d).start()

        return carry

    lax.fori_loop(1, 4, dispatch, 0)
    recv[z] = send[z]
    wrecv[z] = wsend[z]

    loads[1].wait()
    loads[2].wait()
    gpad[0:HALO, :] = jnp.zeros((HALO, chans), BF16)
    gstrip = 64

    def gate_rows(i, carry):
        span = pl.ds(pl.multiple_of(i * gstrip, gstrip), gstrip)
        out = pl.ds(pl.multiple_of(i * gstrip + HALO, HALO), gstrip)
        gpad[out, :] = (value[span, :].astype(F32) * sigmoid(gate[span, :].astype(F32))).astype(BF16)
        return carry

    lax.fori_loop(0, length // gstrip, gate_rows, 0)
    my_cols = pl.ds(pl.multiple_of(tp * chans, LANES), chans)

    def window(t):
        return pl.ds(pl.multiple_of(t * tile, HALO), tile + HALO)

    gated_copies = [
        remote(gpad.at[window(t)], gin.at[:, my_cols], gs, gr, ep, t)
        for t in (core_peer, y_peer, diag)
    ]
    three = gpad.at[pl.ds(0, 3 * (tile + HALO))]
    whole_gated = remote(three, three, gs, gr, ep, core_peer)
    for copy in gated_copies:
        copy.start()

    gin[:, my_cols] = gpad[window(tp), :]

    for g in range(GROUPS):
        ret[g, cap:, :] = jnp.zeros((ret.shape[1] - cap, width), BF16)

    own_wout = wout.at[tp]
    out_y = remote(own_wout, own_wout, cs, cr.at[0], ep, y_peer)
    out_d = remote(own_wout, own_wout, cs, cr.at[1], ep, core_peer)
    out_e = remote(wout.at[y_peer], wout.at[y_peer], cs, cr.at[1], ep, core_peer)

    taps_count = taps_ref.shape[0]
    lane_blocks = gin.shape[1] // LANES
    frows = 64

    def widen():
        whole_gated.wait_recv()

        @pl.when(first_tp)
        def _():
            remote(halo, halo, hs, hr, ep, core_peer).wait_recv()
            gin[0:HALO, :] = halo[...]

        for b in range(lane_blocks):
            wide[b] = gin[:, b * LANES : (b + 1) * LANES].astype(F32)

    def filter_block(b, carry):
        for r in range(tile // frows):
            total = jnp.zeros((frows, LANES), F32)
            for k in range(taps_count):
                start = r * frows + HALO - taps_count + 1 + k
                tap = taps_ref[pl.ds(k, 1), pl.ds(pl.multiple_of(b * LANES, LANES), LANES)]
                total = total + tap * wide[b, pl.ds(start, frows), :]
            filt[b, pl.ds(r * frows, frows), :] = total
        return carry

    def activate(i, carry):
        span = pl.ds(pl.multiple_of(i * strip, strip), strip)
        total = filt[0, span, :]
        squares = total * total
        for b in range(1, lane_blocks):
            part = filt[b, span, :]
            total = total + part
            squares = squares + part * part
        count = 1.0 / (lane_blocks * LANES)
        center = jnp.sum(total, axis=1, keepdims=True) * count
        spread = jnp.sum(squares, axis=1, keepdims=True) * count - center * center
        scale = lax.rsqrt(spread + 1e-05)
        for b in range(lane_blocks):
            cols = slice(b * LANES, (b + 1) * LANES)
            normed = (filt[b, span, :] - center) * scale * gain_ref[:, cols] + shift_ref[:, cols]
            act[span, cols] = (normed * sigmoid(normed)).astype(BF16)
        return carry

    for j in range(pieces):
        hop_x[j].wait_recv()
        hop_y[j].start()
        hop_d[j].start()
        if j > 0:
            hop_y[j - 1].wait_recv()
            hop_e[j - 1].start()
        if j == 1:
            for load in small[3:]:
                load.wait()
            widen()
            lax.fori_loop(0, 2, filter_block, 0)
        if 2 <= j < 5:
            lax.fori_loop(2 * j - 2, 2 * j, filter_block, 0)
        if j == 5:
            lax.fori_loop(0, tile // strip, activate, 0)
    loads[6].wait()
    out_y.start()
    out_d.start()
    hop_y[pieces - 1].wait_recv()
    hop_e[pieces - 1].start()
    for load in loads[3:6]:
        load.wait()
    whole_d.wait_recv()
    whole_e.wait_recv()

    ff = ogate.shape[1]
    even = x == 0
    nb = 256

    def expert(i, carry):
        s = turn(i, HOMEWARD)

        @pl.when(i < 3)
        def _():
            here_from(s).wait_recv()
            weights_here(s).wait_recv()

        w8 = wrecv[s]
        w_low = w8[0:1]
        w_high = w8[1:2]
        mine = jnp.where(even, w_low, w_high)
        theirs = jnp.where(even, w_high, w_low)
        mine = jnp.transpose(jnp.broadcast_to(mine, (LANES, wpad)))[:cap]
        theirs = jnp.transpose(jnp.broadcast_to(theirs, (LANES, wpad)))[:cap]
        mine2 = jnp.concatenate([mine] * (nb // LANES), 1)
        theirs1 = jnp.concatenate([theirs] * (share // LANES), 1)
        here = recv[s]
        for n in range(ff // nb):
            cols = pl.ds(n * nb, nb)
            g = jnp.dot(here, ogate[:, cols], preferred_element_type=F32)
            u = jnp.dot(here, oup[:, cols], preferred_element_type=F32)
            inner[:, cols] = (g * sigmoid(g) * u * mine2).astype(BF16)
        for q in range(4):
            gu = jnp.dot(
                here, pgu[:, pl.ds(q * 2 * share, 2 * share)], preferred_element_type=F32
            )
            g = gu[:, :share]
            u = gu[:, share:]
            inner[:, pl.ds(ff + q * share, share)] = (g * sigmoid(g) * u * theirs1).astype(BF16)
        for n in range(width // nb):
            cols = pl.ds(n * nb, nb)
            total = jnp.dot(inner[:, :ff], odown[:, cols], preferred_element_type=F32) + jnp.dot(
                inner[:, ff:], pdown[:, cols], preferred_element_type=F32
            )
            result[s, :, cols] = total.astype(BF16)

        @pl.when(i < 3)
        def _():
            back(s).start()

        return carry

    lax.fori_loop(0, 4, expert, 0)
    ret[z, pl.ds(0, cap), :] = result[z]

    out_y.wait_recv()
    out_e.start()
    pair = wout.at[pl.ds(0, 2)]
    remote(pair, pair, cs, cr.at[1], ep, core_peer).wait_recv()

    def project(n, carry):
        cols = pl.ds(pl.multiple_of(n * nb, nb), nb)
        total = jnp.dot(act[:, 0:chans], wout[0, :, cols], preferred_element_type=F32)
        for t in range(1, 4):
            total = total + jnp.dot(
                act[:, t * chans : (t + 1) * chans], wout[t, :, cols], preferred_element_type=F32
            )
        conv_ref[:, cols] = total.astype(BF16)
        return carry

    lax.fori_loop(0, width // nb, project, 0)

    def put(g):
        slot = jnp.transpose(jnp.broadcast_to(slots[pl.ds(g, 1), :], (LANES, rows)))
        lane = lax.broadcasted_iota(jnp.int32, (rows, LANES), 1).astype(F32)
        return jnp.concatenate(
            [(slot == lane + float(b * LANES)).astype(F32).astype(BF16) for b in range(wpad // LANES)],
            1,
        )

    def add_back(g, fresh):
        chosen = put(g)
        for n in range(width // nb):
            cols = pl.ds(n * nb, nb)
            rows_back = jnp.dot(chosen, ret[g, :, cols], preferred_element_type=F32)
            if fresh:
                moe_ref[:, cols] = rows_back.astype(BF16)
            else:
                moe_ref[:, cols] = (moe_ref[:, cols].astype(F32) + rows_back).astype(BF16)

    add_back(z, True)

    def rest(i, carry):
        g = jnp.where(
            i == 0, zx, jnp.where(jnp.logical_xor(outer, i == 1), far, across)
        )
        returned(g).wait_recv()
        add_back(g, False)
        return carry

    lax.fori_loop(0, 3, rest, 0)

    most = pl.ds(0, GROUPS - 1)
    remote(send.at[most], recv.at[most], zs, zr.at[z], ep, core_peer).wait_send()
    remote(wsend.at[most], wrecv.at[most], us, ur.at[z], ep, core_peer).wait_send()
    remote(result.at[most], recv.at[most], rs, rr.at[z], ep, core_peer).wait_send()
    remote(quarter, quarter, xs, xr.at[0], ep, core_peer).wait_send()
    remote(quarter, quarter, ys, yr.at[0], ep, core_peer).wait_send()
    whole_d.wait_send()
    whole_e.wait_send()
    whole_gated.wait_send()

    @pl.when(ep < last_ep)
    def _():
        halo_copy(0, ep + 1, tp).wait_send()

    triple = wout.at[pl.ds(0, 3)]
    remote(triple, triple, cs, cr.at[0], ep, core_peer).wait_send()


def put_out(conv_ref, moe_ref, conv_hbm, moe_hbm, sems):
    copies = (
        pltpu.make_async_copy(conv_ref, conv_hbm, sems.at[0]),
        pltpu.make_async_copy(moe_ref, moe_hbm, sems.at[1]),
    )
    for copy in copies:
        copy.start()
    for copy in copies:
        copy.wait()


def one_kernel(
    conv_value, conv_gate, depth_weight, norm_gain, norm_shift, conv_out_weight,
    moe_input, moe_gain, route_experts, route_scores, expert_gate, expert_up, expert_down,
):
    length, chans = conv_value.shape
    peers = lax.axis_size("tp")
    tile = length // peers
    all_chans = chans * peers
    rows, width = moe_input.shape
    ff = expert_gate.shape[2]
    cap = 2 * (3 * TOP * rows // (4 * lax.axis_size("ep")))
    wpad = -(-cap // LANES) * LANES
    vmem = pl.BlockSpec(memory_space=pltpu.VMEM)
    hbm = pl.BlockSpec(memory_space=pltpu.HBM)
    dma = pltpu.SemaphoreType.DMA
    blocks = all_chans // LANES
    outputs = pl.pallas_call(
        functools.partial(fused, cap),
        out_shape=(
            jax.ShapeDtypeStruct((tile, width), BF16),
            jax.ShapeDtypeStruct((rows, width), BF16),
        ),
        in_specs=[hbm] * 13,
        out_specs=(vmem, vmem),
        scratch_shapes=[
            pltpu.VMEM(depth_weight.shape, F32),
            pltpu.VMEM((1, all_chans), F32),
            pltpu.VMEM((1, all_chans), F32),
            pltpu.VMEM((1, width), F32),
            pltpu.VMEM((TOP, rows), jnp.int32),
            pltpu.VMEM((TOP, rows), F32),
            pltpu.VMEM((length, chans), BF16),
            pltpu.VMEM((length, chans), BF16),
            pltpu.VMEM((length + HALO, chans), BF16),
            pltpu.VMEM((tile + HALO, all_chans), BF16),
            pltpu.VMEM((HALO, all_chans), BF16),
            pltpu.VMEM((3, HALO, chans), BF16),
            pltpu.VMEM((blocks, tile + HALO, LANES), F32),
            pltpu.VMEM((blocks, tile, LANES), F32),
            pltpu.VMEM((tile, all_chans), BF16),
            pltpu.VMEM((peers, chans, width), BF16),
            pltpu.VMEM((rows, width), BF16),
            pltpu.VMEM((cap, width), F32),
            pltpu.VMEM((8, rows), F32),
            pltpu.VMEM((8, rows), BF16),
            pltpu.VMEM((GROUPS, cap, width), BF16),
            pltpu.VMEM((GROUPS, cap, width), BF16),
            pltpu.VMEM((GROUPS, TOP, wpad), F32),
            pltpu.VMEM((GROUPS, TOP, wpad), F32),
            pltpu.VMEM((width, ff), BF16),
            pltpu.VMEM((width, ff), BF16),
            pltpu.VMEM((ff, width), BF16),
            pltpu.VMEM((width, 2 * ff), BF16),
            pltpu.VMEM((ff, width), BF16),
            pltpu.VMEM((cap, 2 * ff), BF16),
            pltpu.VMEM((GROUPS, cap, width), BF16),
            pltpu.VMEM((GROUPS, wpad, width), BF16),
            dma((15,)),
            dma(()), dma((GROUPS,)),
            dma(()), dma((GROUPS,)),
            dma(()), dma((GROUPS,)),
            dma(()), dma((6,)),
            dma(()), dma((6,)),
            dma(()), dma(()),
            dma(()), dma(()),
            dma(()), dma(()),
            dma(()), dma(()),
            dma(()), dma((2,)),
        ],
        compiler_params=pltpu.CompilerParams(
            collective_id=0, has_side_effects=True, vmem_limit_bytes=46 * 1024 * 1024
        ),
        name="fused",
    )(
        *(
            pltpu.with_memory_space_constraint(a, pltpu.HBM)
            for a in (
                conv_value, conv_gate, depth_weight, norm_gain[None, :], norm_shift[None, :],
                conv_out_weight, moe_input, moe_gain[None, :], route_experts.T, route_scores.T,
                expert_gate[0], expert_up[0], expert_down[0],
            )
        )
    )
    return pl.pallas_call(
        put_out,
        out_shape=(
            jax.ShapeDtypeStruct((tile, width), BF16),
            jax.ShapeDtypeStruct((rows, width), BF16),
        ),
        in_specs=[vmem, vmem],
        out_specs=(hbm, hbm),
        scratch_shapes=[dma((2,))],
        compiler_params=pltpu.CompilerParams(vmem_limit_bytes=8 * 1024 * 1024),
        name="put_out",
    )(*outputs)


def on_device(
    conv_value,
    conv_gate,
    depth_weight,
    norm_gain,
    norm_shift,
    conv_out_weight,
    moe_input,
    moe_gain,
    route_experts,
    route_scores,
    expert_gate,
    expert_up,
    expert_down,
):
    conv_args = (conv_value, conv_gate, depth_weight, norm_gain, norm_shift, conv_out_weight)
    moe_args = (
        moe_input, moe_gain, route_experts, route_scores, expert_gate, expert_up, expert_down
    )
    if lax.axis_size("ep") == GROUPS * TOP and lax.axis_size("tp") == 4:
        return one_kernel(*conv_args, *moe_args)
    last = conv_value.shape[0] - depth_weight.shape[0] + 1
    earlier = passed_along(gated_rows(conv_value[last:], conv_gate[last:]), "ep", 1)
    partial = conv_half(conv_value, conv_gate, earlier, *conv_args[2:])
    return (scattered_sum(partial), moe_half(*moe_args))


def solution(mesh):
    in_specs = (
        P("ep", "tp"),
        P("ep", "tp"),
        P(),
        P(),
        P(),
        P("tp", None),
        P(("ep", "tp"), None),
        P(),
        P(("ep", "tp"), None),
        P(("ep", "tp"), None),
        P("ep", None, None),
        P("ep", None, None),
        P("ep", None, None),
    )
    out_specs = (P(("ep", "tp"), None), P(("ep", "tp"), None))
    return jax.shard_map(
        on_device, mesh=mesh, in_specs=in_specs, out_specs=out_specs, check_vma=False
    )
```

```python
import functools

import jax
import jax.numpy as jnp
from jax import lax
from jax.experimental import pallas as pl
from jax.experimental.pallas import tpu as pltpu
from jax.sharding import PartitionSpec as P

GROUPS = 4
TOP = 2
LANES = 128
HALO = 32
MESH = pl.DeviceIdType.MESH
OUTWARD = ((1, 3), (2, 0), (3, 2))
HOMEWARD = ((3, 3), (1, 0), (2, 2))
F32 = jnp.float32
BF16 = jnp.bfloat16


def passed_along(x, axis, by):
    peers = lax.axis_size(axis)
    pairs = [(i, i + by) for i in range(peers) if 0 <= i + by < peers]
    return lax.ppermute(x, axis, pairs)


def gated_rows(value, gate):
    return (value.astype(jnp.float32) * jax.nn.sigmoid(gate.astype(jnp.float32))).astype(
        jnp.bfloat16
    )


def conv_half(conv_value, conv_gate, earlier, depth_weight, norm_gain, norm_shift, conv_out_weight):
    channels = conv_value.shape[1]
    length = conv_value.shape[0]
    first_col = lax.axis_index("tp") * channels
    taps = lax.dynamic_slice_in_dim(depth_weight, first_col, channels, 1)
    gains = lax.dynamic_slice_in_dim(norm_gain, first_col, channels, 0)
    shifts = lax.dynamic_slice_in_dim(norm_shift, first_col, channels, 0)
    reach = taps.shape[0] - 1
    gated = gated_rows(conv_value, conv_gate)
    padded = jnp.concatenate([earlier, gated], 0).astype(jnp.float32)
    filtered = taps[0] * padded[0:length]
    for offset in range(1, reach + 1):
        filtered = filtered + taps[offset] * padded[offset : offset + length]
    sums, squares = lax.psum(
        (jnp.sum(filtered, axis=1), jnp.sum(filtered * filtered, axis=1)), "tp"
    )
    all_channels = channels * lax.axis_size("tp")
    center = (sums / all_channels)[:, None]
    spread = (squares / all_channels)[:, None] - center * center
    normed = (filtered - center) * lax.rsqrt(spread + 1e-05) * gains + shifts
    activated = jax.nn.silu(normed).astype(jnp.bfloat16)
    partial_value = jnp.dot(activated, conv_out_weight, preferred_element_type=jnp.float32)
    return partial_value.astype(jnp.bfloat16)


def swapped(x, axis, mask):
    peers = lax.axis_size(axis)
    return lax.ppermute(x, axis, [(i, i ^ mask) for i in range(peers)])


def scattered_sum(partial):
    peers = lax.axis_size("tp")
    me = lax.axis_index("tp")
    size = partial.shape[0] // peers
    total = lax.dynamic_slice_in_dim(partial, me * size, size, 0).astype(jnp.float32)
    for mask in range(peers - 1, 0, -1):
        block = lax.dynamic_slice_in_dim(partial, (me ^ mask) * size, size, 0)
        total = total + swapped(block, "tp", mask).astype(jnp.float32)
    return total.astype(jnp.bfloat16)


def moe_half(moe_input, moe_gain, route_experts, route_scores, expert_gate, expert_up, expert_down):
    rows = moe_input.shape[0]
    model_width = moe_input.shape[1]
    experts_all = lax.axis_size("ep")
    capacity = 2 * (3 * TOP * rows // (4 * experts_all))
    widened = moe_input.astype(jnp.float32)
    normal_in = (
        widened * lax.rsqrt(jnp.mean(widened * widened, axis=-1, keepdims=True) + 1e-06) * moe_gain
    ).astype(jnp.bfloat16)
    chosen = route_experts.reshape(-1)
    onehot = (chosen[:, None] == jnp.arange(experts_all, dtype=jnp.int32)[None, :]).astype(
        jnp.int32
    )
    slot_rank = jnp.sum(jnp.cumsum(onehot, axis=0) * onehot, axis=-1) - 1
    slot_index = jnp.where(
        slot_rank < capacity, chosen * capacity + slot_rank, experts_all * capacity
    )
    source_row = jnp.arange(rows * TOP, dtype=jnp.int32) // TOP
    slot_token = (
        jnp.full((experts_all * capacity,), rows, jnp.int32)
        .at[slot_index]
        .set(source_row, mode="drop")
    )
    padded_in = jnp.concatenate([normal_in, jnp.zeros((1, model_width), jnp.bfloat16)], 0)
    send_buffer = padded_in[slot_token].reshape(experts_all, capacity, model_width)
    arrived = lax.all_to_all(send_buffer, "ep", split_axis=0, concat_axis=0, tiled=True)
    flat_rows = arrived.reshape(-1, model_width)
    gate_act = jnp.dot(flat_rows, expert_gate[0], preferred_element_type=jnp.float32)
    up_act = jnp.dot(flat_rows, expert_up[0], preferred_element_type=jnp.float32)
    inner = (jax.nn.silu(gate_act) * up_act).astype(jnp.bfloat16)
    result = jnp.dot(inner, expert_down[0], preferred_element_type=jnp.float32).astype(jnp.bfloat16)
    returned = lax.all_to_all(
        result.reshape(arrived.shape), "ep", split_axis=0, concat_axis=0, tiled=True
    )
    returned_flat = jnp.concatenate(
        [
            returned.reshape(experts_all * capacity, model_width),
            jnp.zeros((1, model_width), jnp.bfloat16),
        ],
        0,
    )
    picked = returned_flat[slot_index].reshape(rows, TOP, model_width)
    group_gate = jax.nn.sigmoid(route_scores[:, 0])
    first_weight = (group_gate * jax.nn.sigmoid(route_scores[:, 1]))[:, None]
    second_weight = (group_gate * jax.nn.sigmoid(-route_scores[:, 1]))[:, None]
    combined = first_weight * picked[:, 0].astype(jnp.float32) + second_weight * picked[
        :, 1
    ].astype(jnp.float32)
    return combined.astype(jnp.bfloat16)


def sigmoid(v):
    return 1.0 / (1.0 + jnp.exp(-v))


def fused(
    cap,
    value_hbm,
    gate_hbm,
    taps_hbm,
    gain_hbm,
    shift_hbm,
    wout_hbm,
    moe_hbm,
    mgain_hbm,
    experts_hbm,
    scores_hbm,
    egate_hbm,
    eup_hbm,
    edown_hbm,
    conv_ref,
    moe_ref,
    late_ref,
    where_ref,
    taps_ref,
    gain_ref,
    shift_ref,
    mgain_ref,
    experts_ref,
    scores_ref,
    value,
    gate,
    gpad,
    gin,
    halo,
    edge,
    wide,
    filt,
    act,
    wout,
    tokens,
    raw,
    slots,
    wpieces,
    send,
    recv,
    wsend,
    wrecv,
    ogate,
    oup,
    odown,
    pgu,
    pdown,
    inner,
    result,
    ret,
    local_sem,
    zs,
    zr,
    us,
    ur,
    rs,
    rr,
    xs,
    xr,
    ys,
    yr,
    ds,
    dr,
    es,
    er,
    gs,
    gr,
    hs,
    hr,
    cs,
    cr,
):
    ep = lax.axis_index("ep")
    tp = lax.axis_index("tp")
    last_ep = lax.axis_size("ep") - 1
    z = ep // TOP
    x = lax.rem(ep, TOP)
    core = lax.rem(tp, 2)
    y = tp // 2
    core_peer = y * 2 + (1 - core)
    y_peer = (1 - y) * 2 + core
    diag = (1 - y) * 2 + (1 - core)
    rows, width = tokens.shape
    length, chans = value.shape
    tile = gin.shape[0] - HALO
    share = pgu.shape[1] // 8
    wpad = wsend.shape[2]

    def at(e, t):
        return {"ep": e, "tp": t}

    def remote(src, dst, ssem, rsem, e, t):
        return pltpu.make_async_remote_copy(
            src_ref=src, dst_ref=dst, send_sem=ssem, recv_sem=rsem,
            device_id=at(e, t), device_id_type=MESH,
        )

    def there(s):
        return remote(send.at[s], recv.at[z], zs, zr.at[z], s * TOP + x, tp)

    def here_from(s):
        return remote(send.at[s], recv.at[s], zs, zr.at[s], s * TOP + x, tp)

    def weights_there(s):
        return remote(wsend.at[s], wrecv.at[z], us, ur.at[z], s * TOP + x, tp)

    def weights_here(s):
        return remote(wsend.at[s], wrecv.at[s], us, ur.at[s], s * TOP + x, tp)

    def back(s):
        return remote(
            result.at[s], ret.at[z, pl.ds(0, cap)], rs, rr.at[z], s * TOP + x, tp
        )

    def returned(g):
        return remote(
            result.at[g], ret.at[g, pl.ds(0, cap)], rs, rr.at[g], g * TOP + x, tp
        )

    small = [
        pltpu.make_async_copy(experts_hbm, experts_ref, local_sem.at[9]),
        pltpu.make_async_copy(scores_hbm, scores_ref, local_sem.at[10]),
        pltpu.make_async_copy(mgain_hbm, mgain_ref, local_sem.at[11]),
        pltpu.make_async_copy(taps_hbm, taps_ref, local_sem.at[12]),
        pltpu.make_async_copy(gain_hbm, gain_ref, local_sem.at[13]),
        pltpu.make_async_copy(shift_hbm, shift_ref, local_sem.at[14]),
    ]
    for load in small[:3]:
        load.start()
    loads = [
        pltpu.make_async_copy(moe_hbm, tokens, local_sem.at[0]),
        pltpu.make_async_copy(value_hbm, value, local_sem.at[1]),
        pltpu.make_async_copy(gate_hbm, gate, local_sem.at[2]),
        pltpu.make_async_copy(egate_hbm, ogate, local_sem.at[3]),
        pltpu.make_async_copy(eup_hbm, oup, local_sem.at[4]),
        pltpu.make_async_copy(edown_hbm, odown, local_sem.at[5]),
        pltpu.make_async_copy(wout_hbm, wout.at[tp], local_sem.at[6]),
        pltpu.make_async_copy(value_hbm.at[pl.ds(length - HALO, HALO)], edge.at[0], local_sem.at[7]),
        pltpu.make_async_copy(gate_hbm.at[pl.ds(length - HALO, HALO)], edge.at[1], local_sem.at[8]),
    ]
    for load in loads[:1] + loads[7:] + loads[1:7] + small[3:]:
        load.start()

    barrier = pltpu.get_barrier_semaphore()

    def greet(e, t):
        pl.semaphore_signal(barrier, inc=1, device_id=at(e, t), device_id_type=MESH)

    for step in range(1, GROUPS):
        greet(lax.rem(z + step, GROUPS) * TOP + x, tp)
    greet(z * TOP + 1 - x, tp)
    greet(ep, core_peer)
    greet(ep, y_peer)
    greet(ep, diag)

    @pl.when(ep < last_ep)
    def _():
        greet(ep + 1, 0)

    first_tp = jnp.logical_and(ep > 0, tp == 0)

    @pl.when(first_tp)
    def _():
        for t in range(4):
            greet(ep - 1, t)

    expected = (
        GROUPS + 3
        + jnp.where(ep < last_ep, 1, 0)
        + jnp.where(first_tp, 4, 0)
    )

    depth = width // 2
    half = share // 2

    def piece(j, q, gates, ups, downs, wide_cols):
        c = j % 2
        kind = j // 2
        if kind == 2:
            return downs.at[pl.ds(pl.multiple_of(q * share + c * half, half), half), :]
        span = pl.ds(c * depth, depth)
        ref = gates if kind == 0 else ups
        if wide_cols:
            col = pl.multiple_of(q * (2 * share) + kind * share, share)
        else:
            col = pl.multiple_of(q * share, share)
        return ref.at[span, pl.ds(col, share)]

    def held(j, q):
        return piece(j, q, pgu, pgu, pdown, True)

    pieces = 6
    hop_x = [
        remote(
            piece(j, tp, egate_hbm, eup_hbm, edown_hbm, False),
            held(j, tp), xs, xr.at[j], z * TOP + 1 - x, tp,
        )
        for j in range(pieces)
    ]
    hop_y = [remote(held(j, tp), held(j, tp), ys, yr.at[j], ep, y_peer) for j in range(pieces)]
    hop_d = [remote(held(j, tp), held(j, tp), ds, dr, ep, core_peer) for j in range(pieces)]
    hop_e = [
        remote(held(j, y_peer), held(j, y_peer), es, er, ep, core_peer)
        for j in range(pieces)
    ]
    quarter = pdown.at[pl.ds(0, 3 * share)]
    whole_d = remote(quarter, quarter, ds, dr, ep, core_peer)
    whole_e = remote(quarter, quarter, es, er, ep, core_peer)

    small[0].wait()
    small[1].wait()
    small[2].wait()
    first = jnp.broadcast_to(experts_ref[0:1, :], (8, rows))
    group_id = lax.broadcasted_iota(jnp.int32, (8, rows), 0)
    member = jnp.logical_and(first >= group_id * TOP, first < (group_id + 1) * TOP)
    before = (
        lax.broadcasted_iota(jnp.int32, (rows, rows), 0)
        < lax.broadcasted_iota(jnp.int32, (rows, rows), 1)
    ).astype(F32).astype(BF16)
    rank = jnp.dot(member.astype(F32).astype(BF16), before, preferred_element_type=F32)
    keep = jnp.logical_and(member, rank < cap)
    slots[...] = jnp.where(keep, rank, -1.0)
    group_gate = sigmoid(scores_ref[0:1, :])
    first_weight = group_gate * sigmoid(scores_ref[1:2, :])
    second_weight = group_gate * sigmoid(-scores_ref[1:2, :])
    in_order = experts_ref[0:1, :] < experts_ref[1:2, :]
    low = jnp.where(in_order, first_weight, second_weight)
    high = jnp.where(in_order, second_weight, first_weight)
    parts = []
    for weight in (low, high):
        for _ in range(3):
            rounded = weight.astype(BF16).astype(F32)
            parts.append(rounded)
            weight = weight - rounded
    nothing = jnp.zeros((2, rows), F32)
    wpieces[...] = jnp.concatenate(parts + [nothing], 0).astype(BF16)

    strip = 32

    def halo_copy(t, e, c):
        cols = pl.ds(pl.multiple_of(c * chans, LANES), chans)
        return remote(edge.at[2], halo.at[:, cols], hs, hr, e, t)

    loads[7].wait()
    loads[8].wait()
    edge[2] = (edge[0].astype(F32) * sigmoid(edge[1].astype(F32))).astype(BF16)
    zx = z + 1 - 2 * lax.rem(z, 2)
    lo = z < 2
    outer = jnp.logical_or(z == 0, z == 3)
    across = jnp.where(lo, 2, 1)
    far = jnp.where(lo, 3, 0)

    def turn(k, table):
        out = z
        for place, (edge_peer, inner_peer) in enumerate(table):
            for spot in range(GROUPS):
                peer = (edge_peer, inner_peer, 3 - inner_peer, 3 - edge_peer)[spot]
                out = jnp.where(jnp.logical_and(k == place, z == spot), peer, out)
        return out

    block = 512

    def fill(d):
        slot = slots[pl.ds(d, 1), :]
        pick = (
            lax.broadcasted_iota(jnp.int32, (wpad, rows), 0).astype(F32)
            == jnp.broadcast_to(slot, (wpad, rows))
        ).astype(F32).astype(BF16)
        squares = jnp.zeros((cap, 1), F32)
        for n in range(width // block):
            cols = pl.ds(n * block, block)
            chosen = jnp.dot(pick[:cap], tokens[:, cols], preferred_element_type=F32)
            raw[:, cols] = chosen
            squares = squares + jnp.sum(chosen * chosen, axis=1, keepdims=True)
        weights = lax.dot_general(
            wpieces[...], pick, (((1,), (1,)), ((), ())), preferred_element_type=F32
        )
        wsend[d, 0:1, :] = weights[0:1] + weights[1:2] + weights[2:3]
        wsend[d, 1:2, :] = weights[3:4] + weights[4:5] + weights[5:6]
        scale = lax.rsqrt(squares * (1.0 / width) + 1e-06)
        for n in range(width // block):
            cols = pl.ds(n * block, block)
            send[d, :, cols] = (raw[:, cols] * scale * mgain_ref[:, cols]).astype(BF16)

    loads[0].wait()
    start = turn(0, OUTWARD)
    fill(start)
    pl.semaphore_wait(barrier, expected)

    @pl.when(ep < last_ep)
    def _():
        halo_copy(0, ep + 1, tp).start()

    there(start).start()
    weights_there(start).start()
    for hop in hop_x:
        hop.start()

    def dispatch(k, carry):
        d = turn(k, OUTWARD)
        fill(d)

        @pl.when(k < 3)
        def _():
            there(d).start()
            weights_there(d).start()

        return carry

    lax.fori_loop(1, 4, dispatch, 0)
    recv[z] = send[z]
    wrecv[z] = wsend[z]

    loads[1].wait()
    loads[2].wait()
    gpad[0:HALO, :] = jnp.zeros((HALO, chans), BF16)
    gstrip = 64

    def gate_rows(i, carry):
        span = pl.ds(pl.multiple_of(i * gstrip, gstrip), gstrip)
        out = pl.ds(pl.multiple_of(i * gstrip + HALO, HALO), gstrip)
        gpad[out, :] = (value[span, :].astype(F32) * sigmoid(gate[span, :].astype(F32))).astype(BF16)
        return carry

    lax.fori_loop(0, length // gstrip, gate_rows, 0)
    my_cols = pl.ds(pl.multiple_of(tp * chans, LANES), chans)

    def window(t):
        return pl.ds(pl.multiple_of(t * tile, HALO), tile + HALO)

    gated_copies = [
        remote(gpad.at[window(t)], gin.at[:, my_cols], gs, gr, ep, t)
        for t in (core_peer, y_peer, diag)
    ]
    three = gpad.at[pl.ds(0, 3 * (tile + HALO))]
    whole_gated = remote(three, three, gs, gr, ep, core_peer)
    for copy in gated_copies:
        copy.start()

    gin[:, my_cols] = gpad[window(tp), :]

    for g in range(GROUPS):
        ret[g, cap:, :] = jnp.zeros((ret.shape[1] - cap, width), BF16)

    own_wout = wout.at[tp]
    out_y = remote(own_wout, own_wout, cs, cr.at[0], ep, y_peer)
    out_d = remote(own_wout, own_wout, cs, cr.at[1], ep, core_peer)
    out_e = remote(wout.at[y_peer], wout.at[y_peer], cs, cr.at[1], ep, core_peer)

    taps_count = taps_ref.shape[0]
    lane_blocks = gin.shape[1] // LANES
    frows = 64

    def widen():
        whole_gated.wait_recv()

        @pl.when(first_tp)
        def _():
            remote(halo, halo, hs, hr, ep, core_peer).wait_recv()
            gin[0:HALO, :] = halo[...]

        for b in range(lane_blocks):
            wide[b] = gin[:, b * LANES : (b + 1) * LANES].astype(F32)

    def filter_block(b, carry):
        for r in range(tile // frows):
            total = jnp.zeros((frows, LANES), F32)
            for k in range(taps_count):
                start = r * frows + HALO - taps_count + 1 + k
                tap = taps_ref[pl.ds(k, 1), pl.ds(pl.multiple_of(b * LANES, LANES), LANES)]
                total = total + tap * wide[b, pl.ds(start, frows), :]
            filt[b, pl.ds(r * frows, frows), :] = total
        return carry

    def activate(i, carry):
        span = pl.ds(pl.multiple_of(i * strip, strip), strip)
        total = filt[0, span, :]
        squares = total * total
        for b in range(1, lane_blocks):
            part = filt[b, span, :]
            total = total + part
            squares = squares + part * part
        count = 1.0 / (lane_blocks * LANES)
        center = jnp.sum(total, axis=1, keepdims=True) * count
        spread = jnp.sum(squares, axis=1, keepdims=True) * count - center * center
        scale = lax.rsqrt(spread + 1e-05)
        for b in range(lane_blocks):
            cols = slice(b * LANES, (b + 1) * LANES)
            normed = (filt[b, span, :] - center) * scale * gain_ref[:, cols] + shift_ref[:, cols]
            act[span, cols] = (normed * sigmoid(normed)).astype(BF16)
        return carry

    for j in range(pieces):
        hop_x[j].wait_recv()
        hop_y[j].start()
        hop_d[j].start()
        if j > 0:
            hop_y[j - 1].wait_recv()
            hop_e[j - 1].start()
        if j == 1:
            for load in small[3:]:
                load.wait()
            widen()
            lax.fori_loop(0, 2, filter_block, 0)
        if 2 <= j < 5:
            lax.fori_loop(2 * j - 2, 2 * j, filter_block, 0)
        if j == 5:
            lax.fori_loop(0, tile // strip, activate, 0)
    loads[6].wait()
    out_y.start()
    out_d.start()
    hop_y[pieces - 1].wait_recv()
    hop_e[pieces - 1].start()
    for load in loads[3:6]:
        load.wait()
    whole_d.wait_recv()
    whole_e.wait_recv()

    ff = ogate.shape[1]
    even = x == 0
    nb = 256

    def expert(i, carry):
        s = turn(i, HOMEWARD)

        @pl.when(i < 3)
        def _():
            here_from(s).wait_recv()
            weights_here(s).wait_recv()

        w8 = wrecv[s]
        w_low = w8[0:1]
        w_high = w8[1:2]
        mine = jnp.where(even, w_low, w_high)
        theirs = jnp.where(even, w_high, w_low)
        mine = jnp.transpose(jnp.broadcast_to(mine, (LANES, wpad)))[:cap]
        theirs = jnp.transpose(jnp.broadcast_to(theirs, (LANES, wpad)))[:cap]
        mine2 = jnp.concatenate([mine] * (nb // LANES), 1)
        theirs1 = jnp.concatenate([theirs] * (share // LANES), 1)
        here = recv[s]
        for n in range(ff // nb):
            cols = pl.ds(n * nb, nb)
            g = jnp.dot(here, ogate[:, cols], preferred_element_type=F32)
            u = jnp.dot(here, oup[:, cols], preferred_element_type=F32)
            inner[:, cols] = (g * sigmoid(g) * u * mine2).astype(BF16)
        for q in range(4):
            gu = jnp.dot(
                here, pgu[:, pl.ds(q * 2 * share, 2 * share)], preferred_element_type=F32
            )
            g = gu[:, :share]
            u = gu[:, share:]
            inner[:, pl.ds(ff + q * share, share)] = (g * sigmoid(g) * u * theirs1).astype(BF16)
        for n in range(width // nb):
            cols = pl.ds(n * nb, nb)
            total = jnp.dot(inner[:, :ff], odown[:, cols], preferred_element_type=F32) + jnp.dot(
                inner[:, ff:], pdown[:, cols], preferred_element_type=F32
            )
            result[s, :, cols] = total.astype(BF16)

        @pl.when(i < 3)
        def _():
            back(s).start()

        return carry

    lax.fori_loop(0, 4, expert, 0)
    ret[z, pl.ds(0, cap), :] = result[z]

    out_y.wait_recv()
    out_e.start()
    pair = wout.at[pl.ds(0, 2)]
    remote(pair, pair, cs, cr.at[1], ep, core_peer).wait_recv()

    def project(n, carry):
        cols = pl.ds(pl.multiple_of(n * nb, nb), nb)
        total = jnp.dot(act[:, 0:chans], wout[0, :, cols], preferred_element_type=F32)
        for t in range(1, 4):
            total = total + jnp.dot(
                act[:, t * chans : (t + 1) * chans], wout[t, :, cols], preferred_element_type=F32
            )
        conv_ref[:, cols] = total.astype(BF16)
        return carry

    lax.fori_loop(0, width // nb, project, 0)

    def put(g):
        slot = jnp.transpose(jnp.broadcast_to(slots[pl.ds(g, 1), :], (LANES, rows)))
        lane = lax.broadcasted_iota(jnp.int32, (rows, LANES), 1).astype(F32)
        return jnp.concatenate(
            [(slot == lane + float(b * LANES)).astype(F32).astype(BF16) for b in range(wpad // LANES)],
            1,
        )

    def add_back(g, fresh):
        chosen = put(g)
        for n in range(width // nb):
            cols = pl.ds(n * nb, nb)
            rows_back = jnp.dot(chosen, ret[g, :, cols], preferred_element_type=F32)
            if fresh:
                moe_ref[:, cols] = rows_back.astype(BF16)
            else:
                moe_ref[:, cols] = (moe_ref[:, cols].astype(F32) + rows_back).astype(BF16)

    add_back(z, True)

    early = jnp.where(outer, across, far)
    late = jnp.where(outer, far, across)
    where_ref[...] = put(late)

    def rest(i, carry):
        g = jnp.where(i == 0, zx, early)
        returned(g).wait_recv()
        add_back(g, False)
        return carry

    lax.fori_loop(0, 2, rest, 0)
    returned(late).wait_recv()
    late_ref[...] = ret[late]

    most = pl.ds(0, GROUPS - 1)
    remote(send.at[most], recv.at[most], zs, zr.at[z], ep, core_peer).wait_send()
    remote(wsend.at[most], wrecv.at[most], us, ur.at[z], ep, core_peer).wait_send()
    remote(result.at[most], recv.at[most], rs, rr.at[z], ep, core_peer).wait_send()
    remote(quarter, quarter, xs, xr.at[0], ep, core_peer).wait_send()
    remote(quarter, quarter, ys, yr.at[0], ep, core_peer).wait_send()
    whole_d.wait_send()
    whole_e.wait_send()
    whole_gated.wait_send()

    @pl.when(ep < last_ep)
    def _():
        halo_copy(0, ep + 1, tp).wait_send()

    triple = wout.at[pl.ds(0, 3)]
    remote(triple, triple, cs, cr.at[0], ep, core_peer).wait_send()


def put_out(conv_ref, moe_ref, late_ref, where_ref, conv_hbm, moe_hbm, stage, sems):
    block = 512
    blocks = stage.shape[1] // block
    conv_copy = pltpu.make_async_copy(conv_ref, conv_hbm, sems.at[blocks])
    conv_copy.start()

    def columns(n):
        return pl.ds(n * block, block)

    copies = [
        pltpu.make_async_copy(stage.at[:, columns(n)], moe_hbm.at[:, columns(n)], sems.at[n])
        for n in range(blocks)
    ]
    for n in range(blocks):
        late = jnp.dot(where_ref[...], late_ref[:, columns(n)], preferred_element_type=F32)
        stage[:, columns(n)] = (moe_ref[:, columns(n)].astype(F32) + late).astype(BF16)
        if n > 0:
            copies[n - 1].start()
    copies[blocks - 1].start()
    conv_copy.wait()
    for copy in copies:
        copy.wait()


def one_kernel(
    conv_value, conv_gate, depth_weight, norm_gain, norm_shift, conv_out_weight,
    moe_input, moe_gain, route_experts, route_scores, expert_gate, expert_up, expert_down,
):
    length, chans = conv_value.shape
    peers = lax.axis_size("tp")
    tile = length // peers
    all_chans = chans * peers
    rows, width = moe_input.shape
    ff = expert_gate.shape[2]
    cap = 2 * (3 * TOP * rows // (4 * lax.axis_size("ep")))
    wpad = -(-cap // LANES) * LANES
    vmem = pl.BlockSpec(memory_space=pltpu.VMEM)
    hbm = pl.BlockSpec(memory_space=pltpu.HBM)
    dma = pltpu.SemaphoreType.DMA
    blocks = all_chans // LANES
    outputs = pl.pallas_call(
        functools.partial(fused, cap),
        out_shape=(
            jax.ShapeDtypeStruct((tile, width), BF16),
            jax.ShapeDtypeStruct((rows, width), BF16),
            jax.ShapeDtypeStruct((wpad, width), BF16),
            jax.ShapeDtypeStruct((rows, wpad), BF16),
        ),
        in_specs=[hbm] * 13,
        out_specs=(vmem,) * 4,
        scratch_shapes=[
            pltpu.VMEM(depth_weight.shape, F32),
            pltpu.VMEM((1, all_chans), F32),
            pltpu.VMEM((1, all_chans), F32),
            pltpu.VMEM((1, width), F32),
            pltpu.VMEM((TOP, rows), jnp.int32),
            pltpu.VMEM((TOP, rows), F32),
            pltpu.VMEM((length, chans), BF16),
            pltpu.VMEM((length, chans), BF16),
            pltpu.VMEM((length + HALO, chans), BF16),
            pltpu.VMEM((tile + HALO, all_chans), BF16),
            pltpu.VMEM((HALO, all_chans), BF16),
            pltpu.VMEM((3, HALO, chans), BF16),
            pltpu.VMEM((blocks, tile + HALO, LANES), F32),
            pltpu.VMEM((blocks, tile, LANES), F32),
            pltpu.VMEM((tile, all_chans), BF16),
            pltpu.VMEM((peers, chans, width), BF16),
            pltpu.VMEM((rows, width), BF16),
            pltpu.VMEM((cap, width), F32),
            pltpu.VMEM((8, rows), F32),
            pltpu.VMEM((8, rows), BF16),
            pltpu.VMEM((GROUPS, cap, width), BF16),
            pltpu.VMEM((GROUPS, cap, width), BF16),
            pltpu.VMEM((GROUPS, TOP, wpad), F32),
            pltpu.VMEM((GROUPS, TOP, wpad), F32),
            pltpu.VMEM((width, ff), BF16),
            pltpu.VMEM((width, ff), BF16),
            pltpu.VMEM((ff, width), BF16),
            pltpu.VMEM((width, 2 * ff), BF16),
            pltpu.VMEM((ff, width), BF16),
            pltpu.VMEM((cap, 2 * ff), BF16),
            pltpu.VMEM((GROUPS, cap, width), BF16),
            pltpu.VMEM((GROUPS, wpad, width), BF16),
            dma((15,)),
            dma(()), dma((GROUPS,)),
            dma(()), dma((GROUPS,)),
            dma(()), dma((GROUPS,)),
            dma(()), dma((6,)),
            dma(()), dma((6,)),
            dma(()), dma(()),
            dma(()), dma(()),
            dma(()), dma(()),
            dma(()), dma(()),
            dma(()), dma((2,)),
        ],
        compiler_params=pltpu.CompilerParams(
            collective_id=0, has_side_effects=True, vmem_limit_bytes=46 * 1024 * 1024
        ),
        name="fused",
    )(
        *(
            pltpu.with_memory_space_constraint(a, pltpu.HBM)
            for a in (
                conv_value, conv_gate, depth_weight, norm_gain[None, :], norm_shift[None, :],
                conv_out_weight, moe_input, moe_gain[None, :], route_experts.T, route_scores.T,
                expert_gate[0], expert_up[0], expert_down[0],
            )
        )
    )
    return pl.pallas_call(
        put_out,
        out_shape=(
            jax.ShapeDtypeStruct((tile, width), BF16),
            jax.ShapeDtypeStruct((rows, width), BF16),
        ),
        in_specs=[vmem] * 4,
        out_specs=(hbm, hbm),
        scratch_shapes=[pltpu.VMEM((rows, width), BF16), dma((width // 512 + 1,))],
        compiler_params=pltpu.CompilerParams(vmem_limit_bytes=8 * 1024 * 1024),
        name="put_out",
    )(*outputs)


def on_device(
    conv_value,
    conv_gate,
    depth_weight,
    norm_gain,
    norm_shift,
    conv_out_weight,
    moe_input,
    moe_gain,
    route_experts,
    route_scores,
    expert_gate,
    expert_up,
    expert_down,
):
    conv_args = (conv_value, conv_gate, depth_weight, norm_gain, norm_shift, conv_out_weight)
    moe_args = (
        moe_input, moe_gain, route_experts, route_scores, expert_gate, expert_up, expert_down
    )
    if lax.axis_size("ep") == GROUPS * TOP and lax.axis_size("tp") == 4:
        return one_kernel(*conv_args, *moe_args)
    last = conv_value.shape[0] - depth_weight.shape[0] + 1
    earlier = passed_along(gated_rows(conv_value[last:], conv_gate[last:]), "ep", 1)
    partial = conv_half(conv_value, conv_gate, earlier, *conv_args[2:])
    return (scattered_sum(partial), moe_half(*moe_args))


def solution(mesh):
    in_specs = (
        P("ep", "tp"),
        P("ep", "tp"),
        P(),
        P(),
        P(),
        P("tp", None),
        P(("ep", "tp"), None),
        P(),
        P(("ep", "tp"), None),
        P(("ep", "tp"), None),
        P("ep", None, None),
        P("ep", None, None),
        P("ep", None, None),
    )
    out_specs = (P(("ep", "tp"), None), P(("ep", "tp"), None))
    return jax.shard_map(
        on_device, mesh=mesh, in_specs=in_specs, out_specs=out_specs, check_vma=False
    )
```

```python
import functools

import jax
import jax.numpy as jnp
from jax import lax
from jax.experimental import pallas as pl
from jax.experimental.pallas import tpu as pltpu
from jax.sharding import PartitionSpec as P

GROUPS = 4
TOP = 2
LANES = 128
HALO = 32
MESH = pl.DeviceIdType.MESH
OUTWARD = ((1, 3), (2, 0), (3, 2))
HOMEWARD = ((3, 3), (1, 0), (2, 2))
F32 = jnp.float32
BF16 = jnp.bfloat16


def passed_along(x, axis, by):
    peers = lax.axis_size(axis)
    pairs = [(i, i + by) for i in range(peers) if 0 <= i + by < peers]
    return lax.ppermute(x, axis, pairs)


def gated_rows(value, gate):
    return (value.astype(jnp.float32) * jax.nn.sigmoid(gate.astype(jnp.float32))).astype(
        jnp.bfloat16
    )


def conv_half(conv_value, conv_gate, earlier, depth_weight, norm_gain, norm_shift, conv_out_weight):
    channels = conv_value.shape[1]
    length = conv_value.shape[0]
    first_col = lax.axis_index("tp") * channels
    taps = lax.dynamic_slice_in_dim(depth_weight, first_col, channels, 1)
    gains = lax.dynamic_slice_in_dim(norm_gain, first_col, channels, 0)
    shifts = lax.dynamic_slice_in_dim(norm_shift, first_col, channels, 0)
    reach = taps.shape[0] - 1
    gated = gated_rows(conv_value, conv_gate)
    padded = jnp.concatenate([earlier, gated], 0).astype(jnp.float32)
    filtered = taps[0] * padded[0:length]
    for offset in range(1, reach + 1):
        filtered = filtered + taps[offset] * padded[offset : offset + length]
    sums, squares = lax.psum(
        (jnp.sum(filtered, axis=1), jnp.sum(filtered * filtered, axis=1)), "tp"
    )
    all_channels = channels * lax.axis_size("tp")
    center = (sums / all_channels)[:, None]
    spread = (squares / all_channels)[:, None] - center * center
    normed = (filtered - center) * lax.rsqrt(spread + 1e-05) * gains + shifts
    activated = jax.nn.silu(normed).astype(jnp.bfloat16)
    partial_value = jnp.dot(activated, conv_out_weight, preferred_element_type=jnp.float32)
    return partial_value.astype(jnp.bfloat16)


def swapped(x, axis, mask):
    peers = lax.axis_size(axis)
    return lax.ppermute(x, axis, [(i, i ^ mask) for i in range(peers)])


def scattered_sum(partial):
    peers = lax.axis_size("tp")
    me = lax.axis_index("tp")
    size = partial.shape[0] // peers
    total = lax.dynamic_slice_in_dim(partial, me * size, size, 0).astype(jnp.float32)
    for mask in range(peers - 1, 0, -1):
        block = lax.dynamic_slice_in_dim(partial, (me ^ mask) * size, size, 0)
        total = total + swapped(block, "tp", mask).astype(jnp.float32)
    return total.astype(jnp.bfloat16)


def moe_half(moe_input, moe_gain, route_experts, route_scores, expert_gate, expert_up, expert_down):
    rows = moe_input.shape[0]
    model_width = moe_input.shape[1]
    experts_all = lax.axis_size("ep")
    capacity = 2 * (3 * TOP * rows // (4 * experts_all))
    widened = moe_input.astype(jnp.float32)
    normal_in = (
        widened * lax.rsqrt(jnp.mean(widened * widened, axis=-1, keepdims=True) + 1e-06) * moe_gain
    ).astype(jnp.bfloat16)
    chosen = route_experts.reshape(-1)
    onehot = (chosen[:, None] == jnp.arange(experts_all, dtype=jnp.int32)[None, :]).astype(
        jnp.int32
    )
    slot_rank = jnp.sum(jnp.cumsum(onehot, axis=0) * onehot, axis=-1) - 1
    slot_index = jnp.where(
        slot_rank < capacity, chosen * capacity + slot_rank, experts_all * capacity
    )
    source_row = jnp.arange(rows * TOP, dtype=jnp.int32) // TOP
    slot_token = (
        jnp.full((experts_all * capacity,), rows, jnp.int32)
        .at[slot_index]
        .set(source_row, mode="drop")
    )
    padded_in = jnp.concatenate([normal_in, jnp.zeros((1, model_width), jnp.bfloat16)], 0)
    send_buffer = padded_in[slot_token].reshape(experts_all, capacity, model_width)
    arrived = lax.all_to_all(send_buffer, "ep", split_axis=0, concat_axis=0, tiled=True)
    flat_rows = arrived.reshape(-1, model_width)
    gate_act = jnp.dot(flat_rows, expert_gate[0], preferred_element_type=jnp.float32)
    up_act = jnp.dot(flat_rows, expert_up[0], preferred_element_type=jnp.float32)
    inner = (jax.nn.silu(gate_act) * up_act).astype(jnp.bfloat16)
    result = jnp.dot(inner, expert_down[0], preferred_element_type=jnp.float32).astype(jnp.bfloat16)
    returned = lax.all_to_all(
        result.reshape(arrived.shape), "ep", split_axis=0, concat_axis=0, tiled=True
    )
    returned_flat = jnp.concatenate(
        [
            returned.reshape(experts_all * capacity, model_width),
            jnp.zeros((1, model_width), jnp.bfloat16),
        ],
        0,
    )
    picked = returned_flat[slot_index].reshape(rows, TOP, model_width)
    group_gate = jax.nn.sigmoid(route_scores[:, 0])
    first_weight = (group_gate * jax.nn.sigmoid(route_scores[:, 1]))[:, None]
    second_weight = (group_gate * jax.nn.sigmoid(-route_scores[:, 1]))[:, None]
    combined = first_weight * picked[:, 0].astype(jnp.float32) + second_weight * picked[
        :, 1
    ].astype(jnp.float32)
    return combined.astype(jnp.bfloat16)


def sigmoid(v):
    return 1.0 / (1.0 + jnp.exp(-v))


def fused(
    cap,
    value_hbm,
    gate_hbm,
    taps_hbm,
    gain_hbm,
    shift_hbm,
    wout_hbm,
    moe_hbm,
    mgain_hbm,
    experts_hbm,
    scores_hbm,
    egate_hbm,
    eup_hbm,
    edown_hbm,
    conv_ref,
    moe_ref,
    late_ref,
    where_ref,
    taps_ref,
    gain_ref,
    shift_ref,
    mgain_ref,
    experts_ref,
    scores_ref,
    value,
    gate,
    gpad,
    gin,
    halo,
    edge,
    wide,
    filt,
    act,
    wout,
    tokens,
    raw,
    slots,
    wpieces,
    send,
    recv,
    wsend,
    wrecv,
    ogate,
    oup,
    odown,
    pgu,
    pdown,
    inner,
    result,
    ret,
    local_sem,
    zs,
    zr,
    us,
    ur,
    rs,
    rr,
    xs,
    xr,
    ys,
    yr,
    ds,
    dr,
    es,
    er,
    gs,
    gr,
    hs,
    hr,
    cs,
    cr,
):
    ep = lax.axis_index("ep")
    tp = lax.axis_index("tp")
    last_ep = lax.axis_size("ep") - 1
    z = ep // TOP
    x = lax.rem(ep, TOP)
    core = lax.rem(tp, 2)
    y = tp // 2
    core_peer = y * 2 + (1 - core)
    y_peer = (1 - y) * 2 + core
    diag = (1 - y) * 2 + (1 - core)
    rows, width = tokens.shape
    length, chans = value.shape
    tile = gin.shape[0] - HALO
    share = pgu.shape[1] // 8
    wpad = wsend.shape[2]

    def at(e, t):
        return {"ep": e, "tp": t}

    def remote(src, dst, ssem, rsem, e, t):
        return pltpu.make_async_remote_copy(
            src_ref=src, dst_ref=dst, send_sem=ssem, recv_sem=rsem,
            device_id=at(e, t), device_id_type=MESH,
        )

    def there(s):
        return remote(send.at[s], recv.at[z], zs, zr.at[z], s * TOP + x, tp)

    def here_from(s):
        return remote(send.at[s], recv.at[s], zs, zr.at[s], s * TOP + x, tp)

    def weights_there(s):
        return remote(wsend.at[s], wrecv.at[z], us, ur.at[z], s * TOP + x, tp)

    def weights_here(s):
        return remote(wsend.at[s], wrecv.at[s], us, ur.at[s], s * TOP + x, tp)

    def back(s):
        return remote(
            result.at[s], ret.at[z, pl.ds(0, cap)], rs, rr.at[z], s * TOP + x, tp
        )

    def returned(g):
        return remote(
            result.at[g], ret.at[g, pl.ds(0, cap)], rs, rr.at[g], g * TOP + x, tp
        )

    small = [
        pltpu.make_async_copy(experts_hbm, experts_ref, local_sem.at[9]),
        pltpu.make_async_copy(scores_hbm, scores_ref, local_sem.at[10]),
        pltpu.make_async_copy(mgain_hbm, mgain_ref, local_sem.at[11]),
        pltpu.make_async_copy(taps_hbm, taps_ref, local_sem.at[12]),
        pltpu.make_async_copy(gain_hbm, gain_ref, local_sem.at[13]),
        pltpu.make_async_copy(shift_hbm, shift_ref, local_sem.at[14]),
    ]
    for load in small[:3]:
        load.start()
    loads = [
        pltpu.make_async_copy(moe_hbm, tokens, local_sem.at[0]),
        pltpu.make_async_copy(value_hbm, value, local_sem.at[1]),
        pltpu.make_async_copy(gate_hbm, gate, local_sem.at[2]),
        pltpu.make_async_copy(egate_hbm, ogate, local_sem.at[3]),
        pltpu.make_async_copy(eup_hbm, oup, local_sem.at[4]),
        pltpu.make_async_copy(edown_hbm, odown, local_sem.at[5]),
        pltpu.make_async_copy(wout_hbm, wout.at[tp], local_sem.at[6]),
        pltpu.make_async_copy(value_hbm.at[pl.ds(length - HALO, HALO)], edge.at[0], local_sem.at[7]),
        pltpu.make_async_copy(gate_hbm.at[pl.ds(length - HALO, HALO)], edge.at[1], local_sem.at[8]),
    ]
    for load in loads[:1] + loads[7:] + loads[1:7] + small[3:]:
        load.start()

    barrier = pltpu.get_barrier_semaphore()

    def greet(e, t):
        pl.semaphore_signal(barrier, inc=1, device_id=at(e, t), device_id_type=MESH)

    for step in range(1, GROUPS):
        greet(lax.rem(z + step, GROUPS) * TOP + x, tp)
    greet(z * TOP + 1 - x, tp)
    greet(ep, core_peer)
    greet(ep, y_peer)
    greet(ep, diag)

    @pl.when(ep < last_ep)
    def _():
        greet(ep + 1, 0)

    first_tp = jnp.logical_and(ep > 0, tp == 0)

    @pl.when(first_tp)
    def _():
        for t in range(4):
            greet(ep - 1, t)

    expected = (
        GROUPS + 3
        + jnp.where(ep < last_ep, 1, 0)
        + jnp.where(first_tp, 4, 0)
    )

    depth = width // 2
    half = share // 2

    def piece(j, q, gates, ups, downs, wide_cols):
        c = j % 2
        kind = j // 2
        if kind == 2:
            return downs.at[pl.ds(pl.multiple_of(q * share + c * half, half), half), :]
        span = pl.ds(c * depth, depth)
        ref = gates if kind == 0 else ups
        if wide_cols:
            col = pl.multiple_of(q * (2 * share) + kind * share, share)
        else:
            col = pl.multiple_of(q * share, share)
        return ref.at[span, pl.ds(col, share)]

    def held(j, q):
        return piece(j, q, pgu, pgu, pdown, True)

    pieces = 6
    hop_x = [
        remote(
            piece(j, tp, egate_hbm, eup_hbm, edown_hbm, False),
            held(j, tp), xs, xr.at[j], z * TOP + 1 - x, tp,
        )
        for j in range(pieces)
    ]
    hop_y = [remote(held(j, tp), held(j, tp), ys, yr.at[j], ep, y_peer) for j in range(pieces)]
    hop_d = [remote(held(j, tp), held(j, tp), ds, dr, ep, core_peer) for j in range(pieces)]
    hop_e = [
        remote(held(j, y_peer), held(j, y_peer), es, er, ep, core_peer)
        for j in range(pieces)
    ]
    quarter = pdown.at[pl.ds(0, 3 * share)]
    whole_d = remote(quarter, quarter, ds, dr, ep, core_peer)
    whole_e = remote(quarter, quarter, es, er, ep, core_peer)

    small[0].wait()
    small[1].wait()
    small[2].wait()
    first = jnp.broadcast_to(experts_ref[0:1, :], (8, rows))
    group_id = lax.broadcasted_iota(jnp.int32, (8, rows), 0)
    member = jnp.logical_and(first >= group_id * TOP, first < (group_id + 1) * TOP)
    before = (
        lax.broadcasted_iota(jnp.int32, (rows, rows), 0)
        < lax.broadcasted_iota(jnp.int32, (rows, rows), 1)
    ).astype(F32).astype(BF16)
    rank = jnp.dot(member.astype(F32).astype(BF16), before, preferred_element_type=F32)
    keep = jnp.logical_and(member, rank < cap)
    slots[...] = jnp.where(keep, rank, -1.0)
    group_gate = sigmoid(scores_ref[0:1, :])
    first_weight = group_gate * sigmoid(scores_ref[1:2, :])
    second_weight = group_gate * sigmoid(-scores_ref[1:2, :])
    in_order = experts_ref[0:1, :] < experts_ref[1:2, :]
    low = jnp.where(in_order, first_weight, second_weight)
    high = jnp.where(in_order, second_weight, first_weight)
    parts = []
    for weight in (low, high):
        for _ in range(3):
            rounded = weight.astype(BF16).astype(F32)
            parts.append(rounded)
            weight = weight - rounded
    nothing = jnp.zeros((2, rows), F32)
    wpieces[...] = jnp.concatenate(parts + [nothing], 0).astype(BF16)

    strip = 32

    def halo_copy(t, e, c):
        cols = pl.ds(pl.multiple_of(c * chans, LANES), chans)
        return remote(edge.at[2], halo.at[:, cols], hs, hr, e, t)

    loads[7].wait()
    loads[8].wait()
    edge[2] = (edge[0].astype(F32) * sigmoid(edge[1].astype(F32))).astype(BF16)
    zx = z + 1 - 2 * lax.rem(z, 2)
    lo = z < 2
    outer = jnp.logical_or(z == 0, z == 3)
    across = jnp.where(lo, 2, 1)
    far = jnp.where(lo, 3, 0)

    def turn(k, table):
        out = z
        for place, (edge_peer, inner_peer) in enumerate(table):
            for spot in range(GROUPS):
                peer = (edge_peer, inner_peer, 3 - inner_peer, 3 - edge_peer)[spot]
                out = jnp.where(jnp.logical_and(k == place, z == spot), peer, out)
        return out

    block = 512

    def fill(d):
        slot = slots[pl.ds(d, 1), :]
        pick = (
            lax.broadcasted_iota(jnp.int32, (wpad, rows), 0).astype(F32)
            == jnp.broadcast_to(slot, (wpad, rows))
        ).astype(F32).astype(BF16)
        squares = jnp.zeros((cap, 1), F32)
        for n in range(width // block):
            cols = pl.ds(n * block, block)
            chosen = jnp.dot(pick[:cap], tokens[:, cols], preferred_element_type=F32)
            raw[:, cols] = chosen
            squares = squares + jnp.sum(chosen * chosen, axis=1, keepdims=True)
        weights = lax.dot_general(
            wpieces[...], pick, (((1,), (1,)), ((), ())), preferred_element_type=F32
        )
        wsend[d, 0:1, :] = weights[0:1] + weights[1:2] + weights[2:3]
        wsend[d, 1:2, :] = weights[3:4] + weights[4:5] + weights[5:6]
        scale = lax.rsqrt(squares * (1.0 / width) + 1e-06)
        for n in range(width // block):
            cols = pl.ds(n * block, block)
            send[d, :, cols] = (raw[:, cols] * scale * mgain_ref[:, cols]).astype(BF16)

    loads[0].wait()
    start = turn(0, OUTWARD)
    fill(start)
    pl.semaphore_wait(barrier, expected)

    @pl.when(ep < last_ep)
    def _():
        halo_copy(0, ep + 1, tp).start()

    there(start).start()
    weights_there(start).start()
    for hop in hop_x:
        hop.start()

    def dispatch(k, carry):
        d = turn(k, OUTWARD)
        fill(d)

        @pl.when(k < 3)
        def _():
            there(d).start()
            weights_there(d).start()

        return carry

    lax.fori_loop(1, 4, dispatch, 0)
    recv[z] = send[z]
    wrecv[z] = wsend[z]

    loads[1].wait()
    loads[2].wait()
    gpad[0:HALO, :] = jnp.zeros((HALO, chans), BF16)
    gstrip = 64

    def gate_rows(i, carry):
        span = pl.ds(pl.multiple_of(i * gstrip, gstrip), gstrip)
        out = pl.ds(pl.multiple_of(i * gstrip + HALO, HALO), gstrip)
        gpad[out, :] = (value[span, :].astype(F32) * sigmoid(gate[span, :].astype(F32))).astype(BF16)
        return carry

    lax.fori_loop(0, length // gstrip, gate_rows, 0)
    my_cols = pl.ds(pl.multiple_of(tp * chans, LANES), chans)

    def window(t):
        return pl.ds(pl.multiple_of(t * tile, HALO), tile + HALO)

    gated_copies = [
        remote(gpad.at[window(t)], gin.at[:, my_cols], gs, gr, ep, t)
        for t in (core_peer, y_peer, diag)
    ]
    three = gpad.at[pl.ds(0, 3 * (tile + HALO))]
    whole_gated = remote(three, three, gs, gr, ep, core_peer)
    for copy in gated_copies:
        copy.start()

    gin[:, my_cols] = gpad[window(tp), :]

    for g in range(GROUPS):
        ret[g, cap:, :] = jnp.zeros((ret.shape[1] - cap, width), BF16)

    own_wout = wout.at[tp]
    out_y = remote(own_wout, own_wout, cs, cr.at[0], ep, y_peer)
    out_d = remote(own_wout, own_wout, cs, cr.at[1], ep, core_peer)
    out_e = remote(wout.at[y_peer], wout.at[y_peer], cs, cr.at[1], ep, core_peer)

    taps_count = taps_ref.shape[0]
    lane_blocks = gin.shape[1] // LANES
    frows = 64

    def widen():
        whole_gated.wait_recv()

        @pl.when(first_tp)
        def _():
            remote(halo, halo, hs, hr, ep, core_peer).wait_recv()
            gin[0:HALO, :] = halo[...]

        for b in range(lane_blocks):
            wide[b] = gin[:, b * LANES : (b + 1) * LANES].astype(F32)

    def filter_block(b, carry):
        for r in range(tile // frows):
            total = jnp.zeros((frows, LANES), F32)
            for k in range(taps_count):
                start = r * frows + HALO - taps_count + 1 + k
                tap = taps_ref[pl.ds(k, 1), pl.ds(pl.multiple_of(b * LANES, LANES), LANES)]
                total = total + tap * wide[b, pl.ds(start, frows), :]
            filt[b, pl.ds(r * frows, frows), :] = total
        return carry

    def activate(i, carry):
        span = pl.ds(pl.multiple_of(i * strip, strip), strip)
        total = filt[0, span, :]
        squares = total * total
        for b in range(1, lane_blocks):
            part = filt[b, span, :]
            total = total + part
            squares = squares + part * part
        count = 1.0 / (lane_blocks * LANES)
        center = jnp.sum(total, axis=1, keepdims=True) * count
        spread = jnp.sum(squares, axis=1, keepdims=True) * count - center * center
        scale = lax.rsqrt(spread + 1e-05)
        for b in range(lane_blocks):
            cols = slice(b * LANES, (b + 1) * LANES)
            normed = (filt[b, span, :] - center) * scale * gain_ref[:, cols] + shift_ref[:, cols]
            act[span, cols] = (normed * sigmoid(normed)).astype(BF16)
        return carry

    for j in range(pieces):
        hop_x[j].wait_recv()
        hop_y[j].start()
        hop_d[j].start()
        if j > 0:
            hop_y[j - 1].wait_recv()
            hop_e[j - 1].start()
        if j == 1:
            for load in small[3:]:
                load.wait()
            widen()
            lax.fori_loop(0, 2, filter_block, 0)
        if 2 <= j < 5:
            lax.fori_loop(2 * j - 2, 2 * j, filter_block, 0)
        if j == 5:
            lax.fori_loop(0, tile // strip, activate, 0)
    loads[6].wait()
    out_y.start()
    out_d.start()
    hop_y[pieces - 1].wait_recv()
    hop_e[pieces - 1].start()
    for load in loads[3:6]:
        load.wait()
    whole_d.wait_recv()
    whole_e.wait_recv()

    ff = ogate.shape[1]
    even = x == 0
    nb = 256

    def expert(i, carry):
        s = turn(i, HOMEWARD)

        @pl.when(i < 3)
        def _():
            here_from(s).wait_recv()
            weights_here(s).wait_recv()

        w8 = wrecv[s]
        w_low = w8[0:1]
        w_high = w8[1:2]
        mine = jnp.where(even, w_low, w_high)
        theirs = jnp.where(even, w_high, w_low)
        mine = jnp.transpose(jnp.broadcast_to(mine, (LANES, wpad)))[:cap]
        theirs = jnp.transpose(jnp.broadcast_to(theirs, (LANES, wpad)))[:cap]
        mine2 = jnp.concatenate([mine] * (nb // LANES), 1)
        theirs1 = jnp.concatenate([theirs] * (share // LANES), 1)
        here = recv[s]
        for n in range(ff // nb):
            cols = pl.ds(n * nb, nb)
            g = jnp.dot(here, ogate[:, cols], preferred_element_type=F32)
            u = jnp.dot(here, oup[:, cols], preferred_element_type=F32)
            inner[:, cols] = (g * sigmoid(g) * u * mine2).astype(BF16)
        for q in range(4):
            gu = jnp.dot(
                here, pgu[:, pl.ds(q * 2 * share, 2 * share)], preferred_element_type=F32
            )
            g = gu[:, :share]
            u = gu[:, share:]
            inner[:, pl.ds(ff + q * share, share)] = (g * sigmoid(g) * u * theirs1).astype(BF16)
        for n in range(width // nb):
            cols = pl.ds(n * nb, nb)
            total = jnp.dot(inner[:, :ff], odown[:, cols], preferred_element_type=F32) + jnp.dot(
                inner[:, ff:], pdown[:, cols], preferred_element_type=F32
            )
            result[s, :, cols] = total.astype(BF16)

        @pl.when(i < 3)
        def _():
            back(s).start()

        return carry

    lax.fori_loop(0, 4, expert, 0)
    ret[z, pl.ds(0, cap), :] = result[z]

    out_y.wait_recv()
    out_e.start()
    pair = wout.at[pl.ds(0, 2)]
    remote(pair, pair, cs, cr.at[1], ep, core_peer).wait_recv()

    def project(n, carry):
        cols = pl.ds(pl.multiple_of(n * nb, nb), nb)
        total = jnp.dot(act[:, 0:chans], wout[0, :, cols], preferred_element_type=F32)
        for t in range(1, 4):
            total = total + jnp.dot(
                act[:, t * chans : (t + 1) * chans], wout[t, :, cols], preferred_element_type=F32
            )
        conv_ref[:, cols] = total.astype(BF16)
        return carry

    lax.fori_loop(0, width // nb, project, 0)

    def put(g):
        slot = jnp.transpose(jnp.broadcast_to(slots[pl.ds(g, 1), :], (LANES, rows)))
        lane = lax.broadcasted_iota(jnp.int32, (rows, LANES), 1).astype(F32)
        return jnp.concatenate(
            [(slot == lane + float(b * LANES)).astype(F32).astype(BF16) for b in range(wpad // LANES)],
            1,
        )

    def add_back(g, fresh):
        chosen = put(g)
        for n in range(width // nb):
            cols = pl.ds(n * nb, nb)
            rows_back = jnp.dot(chosen, ret[g, :, cols], preferred_element_type=F32)
            if fresh:
                moe_ref[:, cols] = rows_back.astype(BF16)
            else:
                moe_ref[:, cols] = (moe_ref[:, cols].astype(F32) + rows_back).astype(BF16)

    add_back(z, True)

    early = jnp.where(outer, across, far)
    late = jnp.where(outer, far, across)
    where_ref[...] = put(late)
    late_ref[cap:, :] = jnp.zeros((ret.shape[1] - cap, width), BF16)

    def rest(i, carry):
        g = jnp.where(i == 0, zx, early)
        returned(g).wait_recv()
        add_back(g, False)
        return carry

    lax.fori_loop(0, 2, rest, 0)
    returned(late).wait_recv()
    late_ref[0:cap, :] = ret[late, 0:cap, :]

    most = pl.ds(0, GROUPS - 1)
    remote(send.at[most], recv.at[most], zs, zr.at[z], ep, core_peer).wait_send()
    remote(wsend.at[most], wrecv.at[most], us, ur.at[z], ep, core_peer).wait_send()
    remote(result.at[most], recv.at[most], rs, rr.at[z], ep, core_peer).wait_send()
    remote(quarter, quarter, xs, xr.at[0], ep, core_peer).wait_send()
    remote(quarter, quarter, ys, yr.at[0], ep, core_peer).wait_send()
    whole_d.wait_send()
    whole_e.wait_send()
    whole_gated.wait_send()

    @pl.when(ep < last_ep)
    def _():
        halo_copy(0, ep + 1, tp).wait_send()

    triple = wout.at[pl.ds(0, 3)]
    remote(triple, triple, cs, cr.at[0], ep, core_peer).wait_send()


def put_out(conv_ref, moe_ref, late_ref, where_ref, conv_hbm, moe_hbm, stage, sems):
    block = 512
    blocks = stage.shape[1] // block
    conv_copy = pltpu.make_async_copy(conv_ref, conv_hbm, sems.at[blocks])
    conv_copy.start()

    def columns(n):
        return pl.ds(n * block, block)

    copies = [
        pltpu.make_async_copy(stage.at[:, columns(n)], moe_hbm.at[:, columns(n)], sems.at[n])
        for n in range(blocks)
    ]
    for n in range(blocks):
        late = jnp.dot(where_ref[...], late_ref[:, columns(n)], preferred_element_type=F32)
        stage[:, columns(n)] = moe_ref[:, columns(n)] + late.astype(BF16)
        if n > 0:
            copies[n - 1].start()
    copies[blocks - 1].start()
    conv_copy.wait()
    for copy in copies:
        copy.wait()


def one_kernel(
    conv_value, conv_gate, depth_weight, norm_gain, norm_shift, conv_out_weight,
    moe_input, moe_gain, route_experts, route_scores, expert_gate, expert_up, expert_down,
):
    length, chans = conv_value.shape
    peers = lax.axis_size("tp")
    tile = length // peers
    all_chans = chans * peers
    rows, width = moe_input.shape
    ff = expert_gate.shape[2]
    cap = 2 * (3 * TOP * rows // (4 * lax.axis_size("ep")))
    wpad = -(-cap // LANES) * LANES
    vmem = pl.BlockSpec(memory_space=pltpu.VMEM)
    hbm = pl.BlockSpec(memory_space=pltpu.HBM)
    dma = pltpu.SemaphoreType.DMA
    blocks = all_chans // LANES
    outputs = pl.pallas_call(
        functools.partial(fused, cap),
        out_shape=(
            jax.ShapeDtypeStruct((tile, width), BF16),
            jax.ShapeDtypeStruct((rows, width), BF16),
            jax.ShapeDtypeStruct((wpad, width), BF16),
            jax.ShapeDtypeStruct((rows, wpad), BF16),
        ),
        in_specs=[hbm] * 13,
        out_specs=(vmem,) * 4,
        scratch_shapes=[
            pltpu.VMEM(depth_weight.shape, F32),
            pltpu.VMEM((1, all_chans), F32),
            pltpu.VMEM((1, all_chans), F32),
            pltpu.VMEM((1, width), F32),
            pltpu.VMEM((TOP, rows), jnp.int32),
            pltpu.VMEM((TOP, rows), F32),
            pltpu.VMEM((length, chans), BF16),
            pltpu.VMEM((length, chans), BF16),
            pltpu.VMEM((length + HALO, chans), BF16),
            pltpu.VMEM((tile + HALO, all_chans), BF16),
            pltpu.VMEM((HALO, all_chans), BF16),
            pltpu.VMEM((3, HALO, chans), BF16),
            pltpu.VMEM((blocks, tile + HALO, LANES), F32),
            pltpu.VMEM((blocks, tile, LANES), F32),
            pltpu.VMEM((tile, all_chans), BF16),
            pltpu.VMEM((peers, chans, width), BF16),
            pltpu.VMEM((rows, width), BF16),
            pltpu.VMEM((cap, width), F32),
            pltpu.VMEM((8, rows), F32),
            pltpu.VMEM((8, rows), BF16),
            pltpu.VMEM((GROUPS, cap, width), BF16),
            pltpu.VMEM((GROUPS, cap, width), BF16),
            pltpu.VMEM((GROUPS, TOP, wpad), F32),
            pltpu.VMEM((GROUPS, TOP, wpad), F32),
            pltpu.VMEM((width, ff), BF16),
            pltpu.VMEM((width, ff), BF16),
            pltpu.VMEM((ff, width), BF16),
            pltpu.VMEM((width, 2 * ff), BF16),
            pltpu.VMEM((ff, width), BF16),
            pltpu.VMEM((cap, 2 * ff), BF16),
            pltpu.VMEM((GROUPS, cap, width), BF16),
            pltpu.VMEM((GROUPS, wpad, width), BF16),
            dma((15,)),
            dma(()), dma((GROUPS,)),
            dma(()), dma((GROUPS,)),
            dma(()), dma((GROUPS,)),
            dma(()), dma((6,)),
            dma(()), dma((6,)),
            dma(()), dma(()),
            dma(()), dma(()),
            dma(()), dma(()),
            dma(()), dma(()),
            dma(()), dma((2,)),
        ],
        compiler_params=pltpu.CompilerParams(
            collective_id=0, has_side_effects=True, vmem_limit_bytes=46 * 1024 * 1024
        ),
        name="fused",
    )(
        *(
            pltpu.with_memory_space_constraint(a, pltpu.HBM)
            for a in (
                conv_value, conv_gate, depth_weight, norm_gain[None, :], norm_shift[None, :],
                conv_out_weight, moe_input, moe_gain[None, :], route_experts.T, route_scores.T,
                expert_gate[0], expert_up[0], expert_down[0],
            )
        )
    )
    return pl.pallas_call(
        put_out,
        out_shape=(
            jax.ShapeDtypeStruct((tile, width), BF16),
            jax.ShapeDtypeStruct((rows, width), BF16),
        ),
        in_specs=[vmem] * 4,
        out_specs=(hbm, hbm),
        scratch_shapes=[pltpu.VMEM((rows, width), BF16), dma((width // 512 + 1,))],
        compiler_params=pltpu.CompilerParams(vmem_limit_bytes=8 * 1024 * 1024),
        name="put_out",
    )(*outputs)


def on_device(
    conv_value,
    conv_gate,
    depth_weight,
    norm_gain,
    norm_shift,
    conv_out_weight,
    moe_input,
    moe_gain,
    route_experts,
    route_scores,
    expert_gate,
    expert_up,
    expert_down,
):
    conv_args = (conv_value, conv_gate, depth_weight, norm_gain, norm_shift, conv_out_weight)
    moe_args = (
        moe_input, moe_gain, route_experts, route_scores, expert_gate, expert_up, expert_down
    )
    if lax.axis_size("ep") == GROUPS * TOP and lax.axis_size("tp") == 4:
        return one_kernel(*conv_args, *moe_args)
    last = conv_value.shape[0] - depth_weight.shape[0] + 1
    earlier = passed_along(gated_rows(conv_value[last:], conv_gate[last:]), "ep", 1)
    partial = conv_half(conv_value, conv_gate, earlier, *conv_args[2:])
    return (scattered_sum(partial), moe_half(*moe_args))


def solution(mesh):
    in_specs = (
        P("ep", "tp"),
        P("ep", "tp"),
        P(),
        P(),
        P(),
        P("tp", None),
        P(("ep", "tp"), None),
        P(),
        P(("ep", "tp"), None),
        P(("ep", "tp"), None),
        P("ep", None, None),
        P("ep", None, None),
        P("ep", None, None),
    )
    out_specs = (P(("ep", "tp"), None), P(("ep", "tp"), None))
    return jax.shard_map(
        on_device, mesh=mesh, in_specs=in_specs, out_specs=out_specs, check_vma=False
    )
```

```python
import functools

import jax
import jax.numpy as jnp
from jax import lax
from jax.experimental import pallas as pl
from jax.experimental.pallas import tpu as pltpu
from jax.sharding import PartitionSpec as P

GROUPS = 4
TOP = 2
LANES = 128
HALO = 32
MESH = pl.DeviceIdType.MESH
OUTWARD = ((1, 3), (3, 2), (2, 0))
HOMEWARD = ((3, 3), (1, 0), (2, 2))
F32 = jnp.float32
BF16 = jnp.bfloat16


def passed_along(x, axis, by):
    peers = lax.axis_size(axis)
    pairs = [(i, i + by) for i in range(peers) if 0 <= i + by < peers]
    return lax.ppermute(x, axis, pairs)


def gated_rows(value, gate):
    return (value.astype(jnp.float32) * jax.nn.sigmoid(gate.astype(jnp.float32))).astype(
        jnp.bfloat16
    )


def conv_half(conv_value, conv_gate, earlier, depth_weight, norm_gain, norm_shift, conv_out_weight):
    channels = conv_value.shape[1]
    length = conv_value.shape[0]
    first_col = lax.axis_index("tp") * channels
    taps = lax.dynamic_slice_in_dim(depth_weight, first_col, channels, 1)
    gains = lax.dynamic_slice_in_dim(norm_gain, first_col, channels, 0)
    shifts = lax.dynamic_slice_in_dim(norm_shift, first_col, channels, 0)
    reach = taps.shape[0] - 1
    gated = gated_rows(conv_value, conv_gate)
    padded = jnp.concatenate([earlier, gated], 0).astype(jnp.float32)
    filtered = taps[0] * padded[0:length]
    for offset in range(1, reach + 1):
        filtered = filtered + taps[offset] * padded[offset : offset + length]
    sums, squares = lax.psum(
        (jnp.sum(filtered, axis=1), jnp.sum(filtered * filtered, axis=1)), "tp"
    )
    all_channels = channels * lax.axis_size("tp")
    center = (sums / all_channels)[:, None]
    spread = (squares / all_channels)[:, None] - center * center
    normed = (filtered - center) * lax.rsqrt(spread + 1e-05) * gains + shifts
    activated = jax.nn.silu(normed).astype(jnp.bfloat16)
    partial_value = jnp.dot(activated, conv_out_weight, preferred_element_type=jnp.float32)
    return partial_value.astype(jnp.bfloat16)


def swapped(x, axis, mask):
    peers = lax.axis_size(axis)
    return lax.ppermute(x, axis, [(i, i ^ mask) for i in range(peers)])


def scattered_sum(partial):
    peers = lax.axis_size("tp")
    me = lax.axis_index("tp")
    size = partial.shape[0] // peers
    total = lax.dynamic_slice_in_dim(partial, me * size, size, 0).astype(jnp.float32)
    for mask in range(peers - 1, 0, -1):
        block = lax.dynamic_slice_in_dim(partial, (me ^ mask) * size, size, 0)
        total = total + swapped(block, "tp", mask).astype(jnp.float32)
    return total.astype(jnp.bfloat16)


def moe_half(moe_input, moe_gain, route_experts, route_scores, expert_gate, expert_up, expert_down):
    rows = moe_input.shape[0]
    model_width = moe_input.shape[1]
    experts_all = lax.axis_size("ep")
    capacity = 2 * (3 * TOP * rows // (4 * experts_all))
    widened = moe_input.astype(jnp.float32)
    normal_in = (
        widened * lax.rsqrt(jnp.mean(widened * widened, axis=-1, keepdims=True) + 1e-06) * moe_gain
    ).astype(jnp.bfloat16)
    chosen = route_experts.reshape(-1)
    onehot = (chosen[:, None] == jnp.arange(experts_all, dtype=jnp.int32)[None, :]).astype(
        jnp.int32
    )
    slot_rank = jnp.sum(jnp.cumsum(onehot, axis=0) * onehot, axis=-1) - 1
    slot_index = jnp.where(
        slot_rank < capacity, chosen * capacity + slot_rank, experts_all * capacity
    )
    source_row = jnp.arange(rows * TOP, dtype=jnp.int32) // TOP
    slot_token = (
        jnp.full((experts_all * capacity,), rows, jnp.int32)
        .at[slot_index]
        .set(source_row, mode="drop")
    )
    padded_in = jnp.concatenate([normal_in, jnp.zeros((1, model_width), jnp.bfloat16)], 0)
    send_buffer = padded_in[slot_token].reshape(experts_all, capacity, model_width)
    arrived = lax.all_to_all(send_buffer, "ep", split_axis=0, concat_axis=0, tiled=True)
    flat_rows = arrived.reshape(-1, model_width)
    gate_act = jnp.dot(flat_rows, expert_gate[0], preferred_element_type=jnp.float32)
    up_act = jnp.dot(flat_rows, expert_up[0], preferred_element_type=jnp.float32)
    inner = (jax.nn.silu(gate_act) * up_act).astype(jnp.bfloat16)
    result = jnp.dot(inner, expert_down[0], preferred_element_type=jnp.float32).astype(jnp.bfloat16)
    returned = lax.all_to_all(
        result.reshape(arrived.shape), "ep", split_axis=0, concat_axis=0, tiled=True
    )
    returned_flat = jnp.concatenate(
        [
            returned.reshape(experts_all * capacity, model_width),
            jnp.zeros((1, model_width), jnp.bfloat16),
        ],
        0,
    )
    picked = returned_flat[slot_index].reshape(rows, TOP, model_width)
    group_gate = jax.nn.sigmoid(route_scores[:, 0])
    first_weight = (group_gate * jax.nn.sigmoid(route_scores[:, 1]))[:, None]
    second_weight = (group_gate * jax.nn.sigmoid(-route_scores[:, 1]))[:, None]
    combined = first_weight * picked[:, 0].astype(jnp.float32) + second_weight * picked[
        :, 1
    ].astype(jnp.float32)
    return combined.astype(jnp.bfloat16)


def sigmoid(v):
    return 1.0 / (1.0 + jnp.exp(-v))


def fused(
    cap,
    value_hbm,
    gate_hbm,
    taps_hbm,
    gain_hbm,
    shift_hbm,
    wout_hbm,
    moe_hbm,
    mgain_hbm,
    experts_hbm,
    scores_hbm,
    egate_hbm,
    eup_hbm,
    edown_hbm,
    conv_ref,
    moe_ref,
    late_ref,
    where_ref,
    taps_ref,
    gain_ref,
    shift_ref,
    mgain_ref,
    experts_ref,
    scores_ref,
    value,
    gate,
    gpad,
    gin,
    halo,
    edge,
    wide,
    filt,
    act,
    wout,
    tokens,
    raw,
    slots,
    wpieces,
    send,
    recv,
    wsend,
    wrecv,
    ogate,
    oup,
    odown,
    pgu,
    pdown,
    inner,
    result,
    ret,
    local_sem,
    zs,
    zr,
    us,
    ur,
    rs,
    rr,
    xs,
    xr,
    ys,
    yr,
    ds,
    dr,
    es,
    er,
    gs,
    gr,
    hs,
    hr,
    cs,
    cr,
):
    ep = lax.axis_index("ep")
    tp = lax.axis_index("tp")
    last_ep = lax.axis_size("ep") - 1
    z = ep // TOP
    x = lax.rem(ep, TOP)
    core = lax.rem(tp, 2)
    y = tp // 2
    core_peer = y * 2 + (1 - core)
    y_peer = (1 - y) * 2 + core
    diag = (1 - y) * 2 + (1 - core)
    rows, width = tokens.shape
    length, chans = value.shape
    tile = gin.shape[0] - HALO
    share = pgu.shape[1] // 8
    wpad = wsend.shape[2]

    def at(e, t):
        return {"ep": e, "tp": t}

    def remote(src, dst, ssem, rsem, e, t):
        return pltpu.make_async_remote_copy(
            src_ref=src, dst_ref=dst, send_sem=ssem, recv_sem=rsem,
            device_id=at(e, t), device_id_type=MESH,
        )

    def there(s):
        return remote(send.at[s], recv.at[z], zs, zr.at[z], s * TOP + x, tp)

    def here_from(s):
        return remote(send.at[s], recv.at[s], zs, zr.at[s], s * TOP + x, tp)

    def weights_there(s):
        return remote(wsend.at[s], wrecv.at[z], us, ur.at[z], s * TOP + x, tp)

    def weights_here(s):
        return remote(wsend.at[s], wrecv.at[s], us, ur.at[s], s * TOP + x, tp)

    def back(s):
        return remote(
            result.at[s], ret.at[z, pl.ds(0, cap)], rs, rr.at[z], s * TOP + x, tp
        )

    def returned(g):
        return remote(
            result.at[g], ret.at[g, pl.ds(0, cap)], rs, rr.at[g], g * TOP + x, tp
        )

    small = [
        pltpu.make_async_copy(experts_hbm, experts_ref, local_sem.at[9]),
        pltpu.make_async_copy(scores_hbm, scores_ref, local_sem.at[10]),
        pltpu.make_async_copy(mgain_hbm, mgain_ref, local_sem.at[11]),
        pltpu.make_async_copy(taps_hbm, taps_ref, local_sem.at[12]),
        pltpu.make_async_copy(gain_hbm, gain_ref, local_sem.at[13]),
        pltpu.make_async_copy(shift_hbm, shift_ref, local_sem.at[14]),
    ]
    for load in small[:3]:
        load.start()
    loads = [
        pltpu.make_async_copy(moe_hbm, tokens, local_sem.at[0]),
        pltpu.make_async_copy(value_hbm, value, local_sem.at[1]),
        pltpu.make_async_copy(gate_hbm, gate, local_sem.at[2]),
        pltpu.make_async_copy(egate_hbm, ogate, local_sem.at[3]),
        pltpu.make_async_copy(eup_hbm, oup, local_sem.at[4]),
        pltpu.make_async_copy(edown_hbm, odown, local_sem.at[5]),
        pltpu.make_async_copy(wout_hbm, wout.at[tp], local_sem.at[6]),
        pltpu.make_async_copy(value_hbm.at[pl.ds(length - HALO, HALO)], edge.at[0], local_sem.at[7]),
        pltpu.make_async_copy(gate_hbm.at[pl.ds(length - HALO, HALO)], edge.at[1], local_sem.at[8]),
    ]
    for load in loads[:1] + loads[7:] + loads[1:7] + small[3:]:
        load.start()

    barrier = pltpu.get_barrier_semaphore()

    def greet(e, t):
        pl.semaphore_signal(barrier, inc=1, device_id=at(e, t), device_id_type=MESH)

    for step in range(1, GROUPS):
        greet(lax.rem(z + step, GROUPS) * TOP + x, tp)
    greet(z * TOP + 1 - x, tp)
    greet(ep, core_peer)
    greet(ep, y_peer)
    greet(ep, diag)

    @pl.when(ep < last_ep)
    def _():
        greet(ep + 1, 0)

    first_tp = jnp.logical_and(ep > 0, tp == 0)

    @pl.when(first_tp)
    def _():
        for t in range(4):
            greet(ep - 1, t)

    expected = (
        GROUPS + 3
        + jnp.where(ep < last_ep, 1, 0)
        + jnp.where(first_tp, 4, 0)
    )

    depth = width // 2
    half = share // 2

    def piece(j, q, gates, ups, downs, wide_cols):
        c = j % 2
        kind = j // 2
        if kind == 2:
            return downs.at[pl.ds(pl.multiple_of(q * share + c * half, half), half), :]
        span = pl.ds(c * depth, depth)
        ref = gates if kind == 0 else ups
        if wide_cols:
            col = pl.multiple_of(q * (2 * share) + kind * share, share)
        else:
            col = pl.multiple_of(q * share, share)
        return ref.at[span, pl.ds(col, share)]

    def held(j, q):
        return piece(j, q, pgu, pgu, pdown, True)

    pieces = 6
    hop_x = [
        remote(
            piece(j, tp, egate_hbm, eup_hbm, edown_hbm, False),
            held(j, tp), xs, xr.at[j], z * TOP + 1 - x, tp,
        )
        for j in range(pieces)
    ]
    hop_y = [remote(held(j, tp), held(j, tp), ys, yr.at[j], ep, y_peer) for j in range(pieces)]
    hop_d = [remote(held(j, tp), held(j, tp), ds, dr, ep, core_peer) for j in range(pieces)]
    hop_e = [
        remote(held(j, y_peer), held(j, y_peer), es, er, ep, core_peer)
        for j in range(pieces)
    ]
    quarter = pdown.at[pl.ds(0, 3 * share)]
    whole_d = remote(quarter, quarter, ds, dr, ep, core_peer)
    whole_e = remote(quarter, quarter, es, er, ep, core_peer)

    small[0].wait()
    small[1].wait()
    small[2].wait()
    first = jnp.broadcast_to(experts_ref[0:1, :], (8, rows))
    group_id = lax.broadcasted_iota(jnp.int32, (8, rows), 0)
    member = jnp.logical_and(first >= group_id * TOP, first < (group_id + 1) * TOP)
    before = (
        lax.broadcasted_iota(jnp.int32, (rows, rows), 0)
        < lax.broadcasted_iota(jnp.int32, (rows, rows), 1)
    ).astype(F32).astype(BF16)
    rank = jnp.dot(member.astype(F32).astype(BF16), before, preferred_element_type=F32)
    keep = jnp.logical_and(member, rank < cap)
    slots[...] = jnp.where(keep, rank, -1.0)
    group_gate = sigmoid(scores_ref[0:1, :])
    first_weight = group_gate * sigmoid(scores_ref[1:2, :])
    second_weight = group_gate * sigmoid(-scores_ref[1:2, :])
    in_order = experts_ref[0:1, :] < experts_ref[1:2, :]
    low = jnp.where(in_order, first_weight, second_weight)
    high = jnp.where(in_order, second_weight, first_weight)
    parts = []
    for weight in (low, high):
        for _ in range(3):
            rounded = weight.astype(BF16).astype(F32)
            parts.append(rounded)
            weight = weight - rounded
    nothing = jnp.zeros((2, rows), F32)
    wpieces[...] = jnp.concatenate(parts + [nothing], 0).astype(BF16)

    strip = 32

    def halo_copy(t, e, c):
        cols = pl.ds(pl.multiple_of(c * chans, LANES), chans)
        return remote(edge.at[2], halo.at[:, cols], hs, hr, e, t)

    loads[7].wait()
    loads[8].wait()
    edge[2] = (edge[0].astype(F32) * sigmoid(edge[1].astype(F32))).astype(BF16)
    zx = z + 1 - 2 * lax.rem(z, 2)
    lo = z < 2
    outer = jnp.logical_or(z == 0, z == 3)
    across = jnp.where(lo, 2, 1)
    far = jnp.where(lo, 3, 0)

    def turn(k, table):
        out = z
        for place, (edge_peer, inner_peer) in enumerate(table):
            for spot in range(GROUPS):
                peer = (edge_peer, inner_peer, 3 - inner_peer, 3 - edge_peer)[spot]
                out = jnp.where(jnp.logical_and(k == place, z == spot), peer, out)
        return out

    block = 512

    def fill(d):
        slot = slots[pl.ds(d, 1), :]
        pick = (
            lax.broadcasted_iota(jnp.int32, (wpad, rows), 0).astype(F32)
            == jnp.broadcast_to(slot, (wpad, rows))
        ).astype(F32).astype(BF16)
        squares = jnp.zeros((cap, 1), F32)
        for n in range(width // block):
            cols = pl.ds(n * block, block)
            chosen = jnp.dot(pick[:cap], tokens[:, cols], preferred_element_type=F32)
            raw[:, cols] = chosen
            squares = squares + jnp.sum(chosen * chosen, axis=1, keepdims=True)
        weights = lax.dot_general(
            wpieces[...], pick, (((1,), (1,)), ((), ())), preferred_element_type=F32
        )
        wsend[d, 0:1, :] = weights[0:1] + weights[1:2] + weights[2:3]
        wsend[d, 1:2, :] = weights[3:4] + weights[4:5] + weights[5:6]
        scale = lax.rsqrt(squares * (1.0 / width) + 1e-06)
        for n in range(width // block):
            cols = pl.ds(n * block, block)
            send[d, :, cols] = (raw[:, cols] * scale * mgain_ref[:, cols]).astype(BF16)

    loads[0].wait()
    start = turn(0, OUTWARD)
    fill(start)
    pl.semaphore_wait(barrier, expected)

    @pl.when(ep < last_ep)
    def _():
        halo_copy(0, ep + 1, tp).start()

    there(start).start()
    weights_there(start).start()
    for hop in hop_x:
        hop.start()

    def dispatch(k, carry):
        d = turn(k, OUTWARD)
        fill(d)

        @pl.when(k < 3)
        def _():
            there(d).start()
            weights_there(d).start()

        return carry

    lax.fori_loop(1, 4, dispatch, 0)
    recv[z] = send[z]
    wrecv[z] = wsend[z]

    loads[1].wait()
    loads[2].wait()
    gpad[0:HALO, :] = jnp.zeros((HALO, chans), BF16)
    gstrip = 64

    def gate_rows(i, carry):
        span = pl.ds(pl.multiple_of(i * gstrip, gstrip), gstrip)
        out = pl.ds(pl.multiple_of(i * gstrip + HALO, HALO), gstrip)
        gpad[out, :] = (value[span, :].astype(F32) * sigmoid(gate[span, :].astype(F32))).astype(BF16)
        return carry

    lax.fori_loop(0, length // gstrip, gate_rows, 0)
    my_cols = pl.ds(pl.multiple_of(tp * chans, LANES), chans)

    def window(t):
        return pl.ds(pl.multiple_of(t * tile, HALO), tile + HALO)

    gated_copies = [
        remote(gpad.at[window(t)], gin.at[:, my_cols], gs, gr, ep, t)
        for t in (core_peer, y_peer, diag)
    ]
    three = gpad.at[pl.ds(0, 3 * (tile + HALO))]
    whole_gated = remote(three, three, gs, gr, ep, core_peer)
    for copy in gated_copies:
        copy.start()

    gin[:, my_cols] = gpad[window(tp), :]

    for g in range(GROUPS):
        ret[g, cap:, :] = jnp.zeros((ret.shape[1] - cap, width), BF16)

    own_wout = wout.at[tp]
    out_y = remote(own_wout, own_wout, cs, cr.at[0], ep, y_peer)
    out_d = remote(own_wout, own_wout, cs, cr.at[1], ep, core_peer)
    out_e = remote(wout.at[y_peer], wout.at[y_peer], cs, cr.at[1], ep, core_peer)

    taps_count = taps_ref.shape[0]
    lane_blocks = gin.shape[1] // LANES
    frows = 64

    def widen():
        whole_gated.wait_recv()

        @pl.when(first_tp)
        def _():
            remote(halo, halo, hs, hr, ep, core_peer).wait_recv()
            gin[0:HALO, :] = halo[...]

        for b in range(lane_blocks):
            wide[b] = gin[:, b * LANES : (b + 1) * LANES].astype(F32)

    def filter_block(b, carry):
        for r in range(tile // frows):
            total = jnp.zeros((frows, LANES), F32)
            for k in range(taps_count):
                start = r * frows + HALO - taps_count + 1 + k
                tap = taps_ref[pl.ds(k, 1), pl.ds(pl.multiple_of(b * LANES, LANES), LANES)]
                total = total + tap * wide[b, pl.ds(start, frows), :]
            filt[b, pl.ds(r * frows, frows), :] = total
        return carry

    def activate(i, carry):
        span = pl.ds(pl.multiple_of(i * strip, strip), strip)
        total = filt[0, span, :]
        squares = total * total
        for b in range(1, lane_blocks):
            part = filt[b, span, :]
            total = total + part
            squares = squares + part * part
        count = 1.0 / (lane_blocks * LANES)
        center = jnp.sum(total, axis=1, keepdims=True) * count
        spread = jnp.sum(squares, axis=1, keepdims=True) * count - center * center
        scale = lax.rsqrt(spread + 1e-05)
        for b in range(lane_blocks):
            cols = slice(b * LANES, (b + 1) * LANES)
            normed = (filt[b, span, :] - center) * scale * gain_ref[:, cols] + shift_ref[:, cols]
            act[span, cols] = (normed * sigmoid(normed)).astype(BF16)
        return carry

    for j in range(pieces):
        hop_x[j].wait_recv()
        hop_y[j].start()
        hop_d[j].start()
        if j > 0:
            hop_y[j - 1].wait_recv()
            hop_e[j - 1].start()
        if j == 1:
            for load in small[3:]:
                load.wait()
            widen()
            lax.fori_loop(0, 2, filter_block, 0)
        if 2 <= j < 5:
            lax.fori_loop(2 * j - 2, 2 * j, filter_block, 0)
        if j == 5:
            lax.fori_loop(0, tile // strip, activate, 0)
    loads[6].wait()
    out_y.start()
    out_d.start()
    hop_y[pieces - 1].wait_recv()
    hop_e[pieces - 1].start()
    for load in loads[3:6]:
        load.wait()
    whole_d.wait_recv()
    whole_e.wait_recv()

    ff = ogate.shape[1]
    even = x == 0
    nb = 256

    def expert(i, carry):
        s = turn(i, HOMEWARD)

        @pl.when(i < 3)
        def _():
            here_from(s).wait_recv()
            weights_here(s).wait_recv()

        w8 = wrecv[s]
        w_low = w8[0:1]
        w_high = w8[1:2]
        mine = jnp.where(even, w_low, w_high)
        theirs = jnp.where(even, w_high, w_low)
        mine = jnp.transpose(jnp.broadcast_to(mine, (LANES, wpad)))[:cap]
        theirs = jnp.transpose(jnp.broadcast_to(theirs, (LANES, wpad)))[:cap]
        mine2 = jnp.concatenate([mine] * (nb // LANES), 1)
        theirs1 = jnp.concatenate([theirs] * (share // LANES), 1)
        here = recv[s]
        for n in range(ff // nb):
            cols = pl.ds(n * nb, nb)
            g = jnp.dot(here, ogate[:, cols], preferred_element_type=F32)
            u = jnp.dot(here, oup[:, cols], preferred_element_type=F32)
            inner[:, cols] = (g * sigmoid(g) * u * mine2).astype(BF16)
        for q in range(4):
            gu = jnp.dot(
                here, pgu[:, pl.ds(q * 2 * share, 2 * share)], preferred_element_type=F32
            )
            g = gu[:, :share]
            u = gu[:, share:]
            inner[:, pl.ds(ff + q * share, share)] = (g * sigmoid(g) * u * theirs1).astype(BF16)
        for n in range(width // nb):
            cols = pl.ds(n * nb, nb)
            total = jnp.dot(inner[:, :ff], odown[:, cols], preferred_element_type=F32) + jnp.dot(
                inner[:, ff:], pdown[:, cols], preferred_element_type=F32
            )
            result[s, :, cols] = total.astype(BF16)

        @pl.when(i < 3)
        def _():
            back(s).start()

        return carry

    lax.fori_loop(0, 4, expert, 0)
    ret[z, pl.ds(0, cap), :] = result[z]

    out_y.wait_recv()
    out_e.start()
    pair = wout.at[pl.ds(0, 2)]
    remote(pair, pair, cs, cr.at[1], ep, core_peer).wait_recv()

    def project(n, carry):
        cols = pl.ds(pl.multiple_of(n * nb, nb), nb)
        total = jnp.dot(act[:, 0:chans], wout[0, :, cols], preferred_element_type=F32)
        for t in range(1, 4):
            total = total + jnp.dot(
                act[:, t * chans : (t + 1) * chans], wout[t, :, cols], preferred_element_type=F32
            )
        conv_ref[:, cols] = total.astype(BF16)
        return carry

    lax.fori_loop(0, width // nb, project, 0)

    def put(g):
        slot = jnp.transpose(jnp.broadcast_to(slots[pl.ds(g, 1), :], (LANES, rows)))
        lane = lax.broadcasted_iota(jnp.int32, (rows, LANES), 1).astype(F32)
        return jnp.concatenate(
            [(slot == lane + float(b * LANES)).astype(F32).astype(BF16) for b in range(wpad // LANES)],
            1,
        )

    def add_back(g, fresh):
        chosen = put(g)
        for n in range(width // nb):
            cols = pl.ds(n * nb, nb)
            rows_back = jnp.dot(chosen, ret[g, :, cols], preferred_element_type=F32)
            if fresh:
                moe_ref[:, cols] = rows_back.astype(BF16)
            else:
                moe_ref[:, cols] = (moe_ref[:, cols].astype(F32) + rows_back).astype(BF16)

    add_back(z, True)

    early = jnp.where(outer, across, far)
    late = jnp.where(outer, far, across)
    where_ref[...] = put(late)
    late_ref[cap:, :] = jnp.zeros((ret.shape[1] - cap, width), BF16)

    def rest(i, carry):
        g = jnp.where(i == 0, zx, early)
        returned(g).wait_recv()
        add_back(g, False)
        return carry

    lax.fori_loop(0, 2, rest, 0)
    returned(late).wait_recv()
    late_ref[0:cap, :] = ret[late, 0:cap, :]

    most = pl.ds(0, GROUPS - 1)
    remote(send.at[most], recv.at[most], zs, zr.at[z], ep, core_peer).wait_send()
    remote(wsend.at[most], wrecv.at[most], us, ur.at[z], ep, core_peer).wait_send()
    remote(result.at[most], recv.at[most], rs, rr.at[z], ep, core_peer).wait_send()
    remote(quarter, quarter, xs, xr.at[0], ep, core_peer).wait_send()
    remote(quarter, quarter, ys, yr.at[0], ep, core_peer).wait_send()
    whole_d.wait_send()
    whole_e.wait_send()
    whole_gated.wait_send()

    @pl.when(ep < last_ep)
    def _():
        halo_copy(0, ep + 1, tp).wait_send()

    triple = wout.at[pl.ds(0, 3)]
    remote(triple, triple, cs, cr.at[0], ep, core_peer).wait_send()


def put_out(conv_ref, moe_ref, late_ref, where_ref, conv_hbm, moe_hbm, stage, sems):
    block = 512
    blocks = stage.shape[1] // block
    conv_copy = pltpu.make_async_copy(conv_ref, conv_hbm, sems.at[blocks])
    conv_copy.start()

    def columns(n):
        return pl.ds(n * block, block)

    copies = [
        pltpu.make_async_copy(stage.at[:, columns(n)], moe_hbm.at[:, columns(n)], sems.at[n])
        for n in range(blocks)
    ]
    for n in range(blocks):
        late = jnp.dot(where_ref[...], late_ref[:, columns(n)], preferred_element_type=F32)
        stage[:, columns(n)] = moe_ref[:, columns(n)] + late.astype(BF16)
        if n > 0:
            copies[n - 1].start()
    copies[blocks - 1].start()
    conv_copy.wait()
    for copy in copies:
        copy.wait()


def one_kernel(
    conv_value, conv_gate, depth_weight, norm_gain, norm_shift, conv_out_weight,
    moe_input, moe_gain, route_experts, route_scores, expert_gate, expert_up, expert_down,
):
    length, chans = conv_value.shape
    peers = lax.axis_size("tp")
    tile = length // peers
    all_chans = chans * peers
    rows, width = moe_input.shape
    ff = expert_gate.shape[2]
    cap = 2 * (3 * TOP * rows // (4 * lax.axis_size("ep")))
    wpad = -(-cap // LANES) * LANES
    vmem = pl.BlockSpec(memory_space=pltpu.VMEM)
    hbm = pl.BlockSpec(memory_space=pltpu.HBM)
    dma = pltpu.SemaphoreType.DMA
    blocks = all_chans // LANES
    outputs = pl.pallas_call(
        functools.partial(fused, cap),
        out_shape=(
            jax.ShapeDtypeStruct((tile, width), BF16),
            jax.ShapeDtypeStruct((rows, width), BF16),
            jax.ShapeDtypeStruct((wpad, width), BF16),
            jax.ShapeDtypeStruct((rows, wpad), BF16),
        ),
        in_specs=[hbm] * 13,
        out_specs=(vmem,) * 4,
        scratch_shapes=[
            pltpu.VMEM(depth_weight.shape, F32),
            pltpu.VMEM((1, all_chans), F32),
            pltpu.VMEM((1, all_chans), F32),
            pltpu.VMEM((1, width), F32),
            pltpu.VMEM((TOP, rows), jnp.int32),
            pltpu.VMEM((TOP, rows), F32),
            pltpu.VMEM((length, chans), BF16),
            pltpu.VMEM((length, chans), BF16),
            pltpu.VMEM((length + HALO, chans), BF16),
            pltpu.VMEM((tile + HALO, all_chans), BF16),
            pltpu.VMEM((HALO, all_chans), BF16),
            pltpu.VMEM((3, HALO, chans), BF16),
            pltpu.VMEM((blocks, tile + HALO, LANES), F32),
            pltpu.VMEM((blocks, tile, LANES), F32),
            pltpu.VMEM((tile, all_chans), BF16),
            pltpu.VMEM((peers, chans, width), BF16),
            pltpu.VMEM((rows, width), BF16),
            pltpu.VMEM((cap, width), F32),
            pltpu.VMEM((8, rows), F32),
            pltpu.VMEM((8, rows), BF16),
            pltpu.VMEM((GROUPS, cap, width), BF16),
            pltpu.VMEM((GROUPS, cap, width), BF16),
            pltpu.VMEM((GROUPS, TOP, wpad), F32),
            pltpu.VMEM((GROUPS, TOP, wpad), F32),
            pltpu.VMEM((width, ff), BF16),
            pltpu.VMEM((width, ff), BF16),
            pltpu.VMEM((ff, width), BF16),
            pltpu.VMEM((width, 2 * ff), BF16),
            pltpu.VMEM((ff, width), BF16),
            pltpu.VMEM((cap, 2 * ff), BF16),
            pltpu.VMEM((GROUPS, cap, width), BF16),
            pltpu.VMEM((GROUPS, wpad, width), BF16),
            dma((15,)),
            dma(()), dma((GROUPS,)),
            dma(()), dma((GROUPS,)),
            dma(()), dma((GROUPS,)),
            dma(()), dma((6,)),
            dma(()), dma((6,)),
            dma(()), dma(()),
            dma(()), dma(()),
            dma(()), dma(()),
            dma(()), dma(()),
            dma(()), dma((2,)),
        ],
        compiler_params=pltpu.CompilerParams(
            collective_id=0, has_side_effects=True, vmem_limit_bytes=46 * 1024 * 1024
        ),
        name="fused",
    )(
        *(
            pltpu.with_memory_space_constraint(a, pltpu.HBM)
            for a in (
                conv_value, conv_gate, depth_weight, norm_gain[None, :], norm_shift[None, :],
                conv_out_weight, moe_input, moe_gain[None, :], route_experts.T, route_scores.T,
                expert_gate[0], expert_up[0], expert_down[0],
            )
        )
    )
    return pl.pallas_call(
        put_out,
        out_shape=(
            jax.ShapeDtypeStruct((tile, width), BF16),
            jax.ShapeDtypeStruct((rows, width), BF16),
        ),
        in_specs=[vmem] * 4,
        out_specs=(hbm, hbm),
        scratch_shapes=[pltpu.VMEM((rows, width), BF16), dma((width // 512 + 1,))],
        compiler_params=pltpu.CompilerParams(vmem_limit_bytes=8 * 1024 * 1024),
        name="put_out",
    )(*outputs)


def on_device(
    conv_value,
    conv_gate,
    depth_weight,
    norm_gain,
    norm_shift,
    conv_out_weight,
    moe_input,
    moe_gain,
    route_experts,
    route_scores,
    expert_gate,
    expert_up,
    expert_down,
):
    conv_args = (conv_value, conv_gate, depth_weight, norm_gain, norm_shift, conv_out_weight)
    moe_args = (
        moe_input, moe_gain, route_experts, route_scores, expert_gate, expert_up, expert_down
    )
    if lax.axis_size("ep") == GROUPS * TOP and lax.axis_size("tp") == 4:
        return one_kernel(*conv_args, *moe_args)
    last = conv_value.shape[0] - depth_weight.shape[0] + 1
    earlier = passed_along(gated_rows(conv_value[last:], conv_gate[last:]), "ep", 1)
    partial = conv_half(conv_value, conv_gate, earlier, *conv_args[2:])
    return (scattered_sum(partial), moe_half(*moe_args))


def solution(mesh):
    in_specs = (
        P("ep", "tp"),
        P("ep", "tp"),
        P(),
        P(),
        P(),
        P("tp", None),
        P(("ep", "tp"), None),
        P(),
        P(("ep", "tp"), None),
        P(("ep", "tp"), None),
        P("ep", None, None),
        P("ep", None, None),
        P("ep", None, None),
    )
    out_specs = (P(("ep", "tp"), None), P(("ep", "tp"), None))
    return jax.shard_map(
        on_device, mesh=mesh, in_specs=in_specs, out_specs=out_specs, check_vma=False
    )
```
